128 devices in a mesh: kv: 32 (over z, y, core), tp: 4 (over x).
Axes of the slice: x: 4, y: 4, z: 4, core: 2. Of those that a mesh axis runs over, the one named last changes fastest.
Arguments:
- query_rows: bfloat16 [65536, 1536], P('kv', 'tp'), may hold values from -6 to 6
- key_rows: bfloat16 [65536, 1536], P('kv', 'tp'), may hold values from -6 to 6
- value_rows: bfloat16 [65536, 1536], P('kv', 'tp'), may hold values from -6 to 6
- log_sums: float32 [12, 65536], P('tp', 'kv'), may hold values from 5.5 to 7.5
- cotangent: bfloat16 [65536, 1536], P('kv', 'tp'), may hold values from -24 to 24
- layer_input: bfloat16 [65536, 4096], P('kv', 'tp'), may hold values from -0.29882812 to 0.29882812
- chosen: int32 [12, 2048, 12], P('tp'), may hold values from -1 to 1983, as said below
Outputs:
- grad_queries: bfloat16 [65536, 1536], P('kv', 'tp')
- grad_keys: float32 [65536, 1536], P('kv', 'tp')
- grad_values: float32 [65536, 1536], P('kv', 'tp')
- grad_weight: float32 [4096, 1536], P(('tp', 'kv'))
The draws below stay inside these ranges and needn't reach their ends.
Inputs may be any that keep to these rules, and one draw needn't show every extreme that they name: `chosen`: for query block i, write j = i // 64. Every entry other than -1 names a block below j * 64; the entries of a row are distinct, the -1 entries stand last, and a row has exactly min(12, 2 * min(j, 31)) entries other than -1. For one head, the rows with the same j name at most 2 distinct blocks of any one span; for j >= 1 the span j - 1 gives exactly 2 blocks, named by every such row.
All inputs are finite; a program needn't handle non-finite values.
Results may differ from the reference program's by a relative error of at most 0.007.
Values may be sent and summed in bfloat16 or wider, within the bound.
No kernel may reach another device: no remote copies, remote signals or barrier semaphores. Data moves between devices by JAX's collectives and lax.ppermute only.
A program may use at most 192 MiB of HBM per device.

```python
import jax
import jax.numpy as jnp
from jax import lax

D = 4096
HEADS = 12
HEAD_DIM = 128
KEY_BLOCK = 32
SEL = 12
CAP = 2
OWNERS = 31
TOKENS = 65536
BPD = 64
N_KV = 32


def draw_chosen(key, part):
    base_key = jax.random.fold_in(key, 17)
    owner_key, block_key, row_key = jax.random.split(base_key, 3)
    asking_accelerator = jnp.arange(N_KV, dtype=jnp.int32)[:, None]
    proposed_segment = jnp.arange(N_KV, dtype=jnp.int32)[None, :]
    noise_perturbation = jax.random.randint(owner_key, (HEADS, N_KV, N_KV), 0, 1 << 20, dtype=jnp.int32) * 64 + proposed_segment
    merit_increment = jnp.where(proposed_segment == asking_accelerator - 1, 3 << 27, jnp.where(proposed_segment == asking_accelerator - N_KV // 2, 2 << 27, jnp.where(proposed_segment == 0, 1 << 27, 0)))
    possessor_merit = jnp.where(proposed_segment < asking_accelerator, noise_perturbation + merit_increment, -1 - proposed_segment)
    owner_top, owner_pick = lax.top_k(possessor_merit, OWNERS)
    owner_valid = owner_top >= 0
    block_noise = jax.random.randint(block_key, (HEADS, N_KV, OWNERS, BPD), 0, 1 << 20, dtype=jnp.int32) * BPD + jnp.arange(BPD, dtype=jnp.int32)
    block_top, block_pick = lax.top_k(block_noise, CAP)
    pool_ids = (owner_pick[:, :, :, None] * BPD + block_pick).reshape(HEADS, N_KV, OWNERS * CAP)
    pool_valid = jnp.repeat(owner_valid, CAP, axis=2)
    pool_size = OWNERS * CAP
    slot_ids = jnp.arange(pool_size, dtype=jnp.int32)
    row_noise = jax.random.randint(row_key, (HEADS, N_KV, BPD, pool_size), 0, 1 << 20, dtype=jnp.int32) * pool_size + slot_ids
    row_noise = row_noise + jnp.where(slot_ids < 2 * CAP, 1 << 27, 0)
    row_score = jnp.where(pool_valid[:, :, None, :], row_noise, -1 - slot_ids)
    row_top, row_pick = lax.top_k(row_score, SEL)
    picked = jnp.take_along_axis(jnp.broadcast_to(pool_ids[:, :, None, :], row_score.shape), row_pick, axis=3)
    result = jnp.where(row_top >= 0, picked, -1)
    return result.reshape(HEADS, N_KV * BPD, SEL).astype(jnp.int32)


def block_levels(stream_key, shape, shards, smallest, high):
    level, own = 1.0, jax.random.fold_in(stream_key, 6)
    for dim, blocks in shards:
        heights = jnp.exp(jax.random.uniform(jax.random.fold_in(own, dim), (blocks,), jnp.float32, smallest / len(shards), high / len(shards)))
        level = level * jnp.repeat(heights, shape[dim] // blocks).reshape([-1 if axis == dim else 1 for axis in range(len(shape))])
    return level


def gaussian(own_key, shape, deviation, most, cuts=(), kind=jnp.bfloat16):
    entries = deviation * jax.random.normal(own_key, shape, jnp.float32)
    if cuts:
        entries = entries * block_levels(own_key, shape, cuts, -0.22, 0.18)
    return jnp.clip(entries, -most, most).astype(kind)


def setup_inputs(seed: int = 0) -> dict:
    seeds = jax.random.split(jax.random.key(seed), 8)
    return {
        "query_rows": gaussian(seeds[0], (TOKENS, HEADS * HEAD_DIM), 1.0, 6.0, ((0, 32), (1, 4))),
        "key_rows": gaussian(seeds[1], (TOKENS, HEADS * HEAD_DIM), 1.0, 6.0, ((0, 32), (1, 4))),
        "value_rows": gaussian(seeds[2], (TOKENS, HEADS * HEAD_DIM), 1.0, 6.0, ((0, 32), (1, 4))),
        "log_sums": jnp.clip(5.5 + 2.0 * jax.random.uniform(seeds[3], (HEADS, TOKENS), jnp.float32) ** block_levels(seeds[3], (HEADS, TOKENS), ((0, 4), (1, 32)), -0.2, 0.2), 5.5, 7.5),
        "cotangent": gaussian(seeds[4], (TOKENS, HEADS * HEAD_DIM), 4.0, 24.0, ((0, 32), (1, 4))),
        "layer_input": gaussian(seeds[5], (TOKENS, D), 0.05, 0.29882812, ((0, 32), (1, 4))),
        "chosen": draw_chosen(jax.random.fold_in(seeds[7], 71), 0),
    }


def head_grads(inputs):
    query_portion, key_part, value_part, output_gradient, log_sum, picked = inputs
    blocks = query_portion.shape[0] // KEY_BLOCK
    scale_factor = HEAD_DIM ** -0.5
    batch_query = query_portion.reshape(blocks, KEY_BLOCK, HEAD_DIM).astype(jnp.float32)
    key_b = key_part.reshape(blocks, KEY_BLOCK, HEAD_DIM).astype(jnp.float32)
    value_b = value_part.reshape(blocks, KEY_BLOCK, HEAD_DIM).astype(jnp.float32)
    batch_gradient = output_gradient.reshape(blocks, KEY_BLOCK, HEAD_DIM).astype(jnp.float32)
    sums_b = log_sum.reshape(blocks, KEY_BLOCK)
    usable = picked >= 0
    safe_ids = jnp.maximum(picked, 0).astype(jnp.int32)
    far_span = SEL * KEY_BLOCK
    gathered_keys = jnp.concatenate([key_b[safe_ids].reshape(blocks, far_span, HEAD_DIM), key_b], axis=1)
    gathered_values = jnp.concatenate([value_b[safe_ids].reshape(blocks, far_span, HEAD_DIM), value_b], axis=1)
    far_mask = jnp.broadcast_to(jnp.repeat(usable, KEY_BLOCK, axis=1)[:, None, :], (blocks, KEY_BLOCK, far_span))
    lower_triangular = jnp.broadcast_to(jnp.tril(jnp.ones((KEY_BLOCK, KEY_BLOCK), dtype=bool)), (blocks, KEY_BLOCK, KEY_BLOCK))
    attend_mask = jnp.concatenate([far_mask, lower_triangular], axis=2)
    attention_scores = jnp.einsum("cjw,ctw->cjt", batch_query, gathered_keys) * scale_factor
    probs = jnp.where(attend_mask, jnp.exp(attention_scores - sums_b[:, :, None]), 0.0)
    probability_gradient = jnp.einsum("cjw,ctw->cjt", batch_gradient, gathered_values)
    row_dots = jnp.sum(probs * probability_gradient, axis=2)
    score_gradient = lax.optimization_barrier((probs * (probability_gradient - row_dots[:, :, None])).astype(jnp.bfloat16))
    reduced_probabilities = lax.optimization_barrier(probs.astype(jnp.bfloat16))
    query_gradient = (scale_factor * jnp.einsum("lzs,lsa->lza", score_gradient.astype(jnp.float32), gathered_keys)).astype(jnp.bfloat16)
    full_key_gradient = scale_factor * jnp.einsum("slm,slc->smc", score_gradient.astype(jnp.float32), batch_query)
    full_value_gradient = jnp.einsum("slm,slc->smc", reduced_probabilities.astype(jnp.float32), batch_gradient)
    flat_ids = safe_ids.reshape(-1)
    empty = jnp.zeros((blocks, KEY_BLOCK, HEAD_DIM), jnp.float32)
    grad_key = full_key_gradient[:, far_span:] + empty.at[flat_ids].add(full_key_gradient[:, :far_span].reshape(blocks * SEL, KEY_BLOCK, HEAD_DIM))
    grad_value = full_value_gradient[:, far_span:] + empty.at[flat_ids].add(full_value_gradient[:, :far_span].reshape(blocks * SEL, KEY_BLOCK, HEAD_DIM))
    return query_gradient.reshape(-1, HEAD_DIM), grad_key.reshape(-1, HEAD_DIM), grad_value.reshape(-1, HEAD_DIM)


def heads_first(array):
    return array.reshape(TOKENS, HEADS, HEAD_DIM).transpose(1, 0, 2)


def heads_back(array):
    return array.transpose(1, 0, 2).reshape(TOKENS, HEADS * HEAD_DIM)


def reference(query_rows, key_rows, value_rows, log_sums, cotangent, layer_input, chosen):
    query_gradient, grad_key, grad_value = lax.map(head_grads, (heads_first(query_rows), heads_first(key_rows), heads_first(value_rows), heads_first(cotangent), log_sums, chosen))
    grad_queries = heads_back(query_gradient)
    grad_weight = jnp.dot(layer_input.T, grad_queries, preferred_element_type=jnp.float32)
    return grad_queries, heads_back(grad_key), heads_back(grad_value), grad_weight
```

```python
import functools

import jax
import jax.numpy as jnp
from jax import lax
from jax.experimental import pallas as pl
from jax.experimental.pallas import tpu as pltpu
from jax.sharding import PartitionSpec as P

HEAD_DIM = 128
KEY_BLOCK = 32
CAP = 2
BIG = 1 << 20
LOG2E = 1.4426950408889634
NEG = -1.0e30
TQ = 512
KB = 256


def to_lanes(column):
    wide = jnp.broadcast_to(column.astype(jnp.float32), (128, 128))
    return wide.T[0:1, :].astype(jnp.int32)


def pack_kernel(me_ref, chosen_ref, k_ref, v_ref, *rest, heads, spans, blocks, picks):
    sends = rest[:heads]
    tab_ref, bias_ref, lo_s, hi_s, tab_v, tab_s, sem = rest[heads:]
    me = me_ref[0]
    lo_s[...] = jnp.full((128, 128), BIG, jnp.int32)
    hi_s[...] = jnp.full((128, 128), -1, jnp.int32)
    for h in range(heads):

        def one_span(n, carry, h=h):
            ids = chosen_ref[h, pl.ds(n * blocks, blocks), :]
            mine = (ids >> 6) == me
            lo_s[pl.ds(h * spans + n, 1), 0:picks] = jnp.min(
                jnp.where(mine, ids, BIG), axis=0, keepdims=True
            )
            hi_s[pl.ds(h * spans + n, 1), 0:picks] = jnp.max(
                jnp.where(mine, ids, -1), axis=0, keepdims=True
            )
            return carry

        lax.fori_loop(0, spans, one_span, 0, unroll=4)
    lo = to_lanes(jnp.min(lo_s[...], axis=1, keepdims=True))
    hi = to_lanes(jnp.max(hi_s[...], axis=1, keepdims=True))
    tab_v[...] = jnp.zeros((8, 128), jnp.int32)
    tab_v[0:1, :] = lo & (blocks - 1)
    tab_v[1:2, :] = jnp.where(hi >= 0, hi, 0) & (blocks - 1)
    tab_v[2:3, :] = (hi >= 0).astype(jnp.int32)
    tab_v[3:4, :] = (hi > lo).astype(jnp.int32)
    tab_ref[...] = tab_v[...]
    copy = pltpu.make_async_copy(tab_v, tab_s, sem)
    copy.start()
    slot = lax.broadcasted_iota(jnp.int32, (blocks, 128), 1)
    place = lax.broadcasted_iota(jnp.int32, (blocks, blocks * KEY_BLOCK), 1) // KEY_BLOCK
    row = lax.broadcasted_iota(jnp.int32, (blocks, blocks * KEY_BLOCK), 0)
    expand = (place == row).astype(jnp.bfloat16)
    for h in range(heads):
        ids = chosen_ref[h, pl.ds(me * blocks, blocks), :]
        cols = [jnp.broadcast_to(ids[:, c : c + 1], (blocks, 128)) for c in range(picks)]
        least = jnp.full((blocks, 128), BIG, jnp.int32)
        most = jnp.full((blocks, 128), -1, jnp.int32)
        for col in cols:
            hit = (col >> 6) == (slot >> 1)
            least = jnp.minimum(least, jnp.where(hit, col, BIG))
            most = jnp.maximum(most, jnp.where(hit, col, -1))
        least = jnp.min(least, axis=0, keepdims=True)
        most = jnp.max(most, axis=0, keepdims=True)
        name = jnp.where(
            (slot[0:1] & 1) == 0, least, jnp.where(most > least, most, -7)
        )
        named = cols[0] == name
        for col in cols[1:]:
            named = named | (col == name)
        flag = jnp.where(named, 1.0, 0.0).astype(jnp.float32)
        flag = jnp.concatenate([flag, jnp.zeros((128 - blocks, 128), jnp.float32)], axis=0).T
        hot = flag[0 : spans * CAP, 0:blocks].astype(jnp.bfloat16)
        full = jnp.dot(hot, expand, preferred_element_type=jnp.float32)
        bias_ref[h] = jnp.where(full > 0.5, 0.0, NEG)
    copy.wait()
    for h in range(heads):
        lanes = slice(h * HEAD_DIM, (h + 1) * HEAD_DIM)

        def fill(n, carry, h=h, lanes=lanes):
            for c in range(CAP):
                b = tab_s[c, h * spans + n]
                sends[h][n, 0, c] = k_ref[b, :, lanes]
                sends[h][n, 1, c] = v_ref[b, :, lanes]
            return carry

        lax.fori_loop(0, spans, fill, 0, unroll=4)


def attend_kernel(*refs, head, first, tiles, far):
    if first:
        q_ref, g_ref, ko_ref, vo_ref, lse_ref, bias_ref, kv_ref = refs[:7]
        rest = refs[7:]
    else:
        q_ref, g_ref, ko_ref, vo_ref, lse_ref, bias_ref, kv_ref = refs[:7]
        rest = refs[8:]
    gqf_ref, gq_ref, dko_ref, dvo_ref, back_ref = rest[:5]
    p_s, dp_s, ds_s, dk_s, dv_s, kt_s = rest[5:]
    step = pl.program_id(0)
    scale = HEAD_DIM**-0.5
    nkb = far // KB
    per = KB // (CAP * KEY_BLOCK)

    @pl.when(step == 0)
    def _():
        dk_s[...] = jnp.zeros_like(dk_s)
        dv_s[...] = jnp.zeros_like(dv_s)
        for i in range(nkb):
            keys = kv_ref[i * per : (i + 1) * per, 0].reshape(KB, HEAD_DIM)
            kt_s[:, i * KB : (i + 1) * KB] = keys.astype(jnp.float32).T.astype(jnp.bfloat16)

    q = q_ref[...]
    g = g_ref[...]
    lse = lse_ref[head : head + 1, :] * LOG2E
    nt = (((1,), (1,)), ((), ()))

    def ahead(i, dots):
        keys = kv_ref[pl.ds(i * per, per), 0].reshape(KB, HEAD_DIM)
        values = kv_ref[pl.ds(i * per, per), 1].reshape(KB, HEAD_DIM)
        s = lax.dot_general(keys, q, nt, preferred_element_type=jnp.float32)
        dp = lax.dot_general(values, g, nt, preferred_element_type=jnp.float32)
        shift = bias_ref[pl.ds(i * per * CAP, per * CAP), :] - lse
        s = (s * (scale * LOG2E)).reshape(per * CAP, KEY_BLOCK, TQ) + shift[:, None, :]
        p = jnp.exp2(s).reshape(KB, TQ)
        rows = pl.ds(pl.multiple_of(i * KB, KB), KB)
        p_s[rows, :] = p
        dp_s[rows, :] = dp
        dv_s[rows, :] += jnp.dot(
            p.astype(jnp.bfloat16), g, preferred_element_type=jnp.float32
        )
        return dots + (p * dp).reshape(KB // 8, 8, TQ).sum(axis=0)

    dots = lax.fori_loop(0, nkb, ahead, jnp.zeros((8, TQ), jnp.float32))
    dots = jnp.sum(dots, axis=0, keepdims=True)
    key_at = lax.broadcasted_iota(jnp.int32, (128, 128), 0)
    row_at = lax.broadcasted_iota(jnp.int32, (128, 128), 1)
    near = (key_at // KEY_BLOCK == row_at // KEY_BLOCK) & (key_at <= row_at)
    own = []
    own_dots = []
    for t in range(TQ // 128):
        cut = slice(t * 128, (t + 1) * 128)
        s = lax.dot_general(ko_ref[cut, :], q[cut], nt, preferred_element_type=jnp.float32)
        dp = lax.dot_general(vo_ref[cut, :], g[cut], nt, preferred_element_type=jnp.float32)
        p = jnp.exp2(jnp.where(near, s * (scale * LOG2E) - lse[:, cut], NEG))
        own.append((p, dp))
        own_dots.append(jnp.sum(p * dp, axis=0, keepdims=True))
        dvo_ref[cut, :] = jnp.dot(
            p.astype(jnp.bfloat16), g[cut], preferred_element_type=jnp.float32
        )
    dots = dots + jnp.concatenate(own_dots, axis=1)

    def behind(i, carry):
        rows = pl.ds(pl.multiple_of(i * KB, KB), KB)
        ds = (p_s[rows, :] * (dp_s[rows, :] - dots)).astype(jnp.bfloat16)
        ds_s[rows, :] = ds
        dk_s[rows, :] += jnp.dot(ds, q, preferred_element_type=jnp.float32)
        return carry

    lax.fori_loop(0, nkb, behind, 0)
    total = jnp.dot(kt_s[...], ds_s[...], preferred_element_type=jnp.float32)
    for t in range(TQ // 128):
        cut = slice(t * 128, (t + 1) * 128)
        p, dp = own[t]
        ds = (p * (dp - dots[:, cut])).astype(jnp.bfloat16)
        dko_ref[cut, :] = scale * jnp.dot(ds, q[cut], preferred_element_type=jnp.float32)
        kt = ko_ref[cut, :].astype(jnp.float32).T.astype(jnp.bfloat16)
        part = total[:, cut] + jnp.dot(kt, ds, preferred_element_type=jnp.float32)
        out = (scale * part).T.astype(jnp.bfloat16)
        gq_ref[cut, :] = out
        gqf_ref[cut, :] = out

    @pl.when(step == tiles - 1)
    def _():
        back_ref[:, 0] = (scale * dk_s[...]).astype(jnp.bfloat16).reshape(back_ref[:, 0].shape)
        back_ref[:, 1] = dv_s[...].astype(jnp.bfloat16).reshape(back_ref[:, 1].shape)


def land_kernel(me_ref, tab_ref, back_ref, dko_ref, dvo_ref, *rest, head, spans):
    gk_ref, gv_ref = rest[-2:]
    gk_ref[...] = dko_ref[...]
    gv_ref[...] = dvo_ref[...]
    me = me_ref[0]

    def one(n, carry):
        for c in range(CAP):
            at = head * spans + n

            @pl.when(tab_ref[2 + c, at] > 0)
            def _(c=c, at=at):
                rows = pl.ds(pl.multiple_of(tab_ref[c, at] * KEY_BLOCK, KEY_BLOCK), KEY_BLOCK)
                gk_ref[rows, :] += back_ref[n, 0, c].astype(jnp.float32)
                gv_ref[rows, :] += back_ref[n, 1, c].astype(jnp.float32)

        return carry

    lax.fori_loop(me + 1, spans, one, 0)


def pack(me, chosen, key_rows, value_rows, heads, spans, blocks):
    picks = chosen.shape[2]
    rows = key_rows.shape[0]
    shape = (spans, 2, CAP, KEY_BLOCK, HEAD_DIM)
    vmem = pl.BlockSpec(memory_space=pltpu.VMEM)
    return pl.pallas_call(
        functools.partial(pack_kernel, heads=heads, spans=spans, blocks=blocks, picks=picks),
        out_shape=[jax.ShapeDtypeStruct(shape, jnp.bfloat16)] * heads
        + [
            jax.ShapeDtypeStruct((8, 128), jnp.int32),
            jax.ShapeDtypeStruct((heads, spans * CAP, rows), jnp.float32),
        ],
        in_specs=[pl.BlockSpec(memory_space=pltpu.SMEM), vmem, vmem, vmem],
        out_specs=[vmem] * (heads + 2),
        scratch_shapes=[
            pltpu.VMEM((128, 128), jnp.int32),
            pltpu.VMEM((128, 128), jnp.int32),
            pltpu.VMEM((8, 128), jnp.int32),
            pltpu.SMEM((8, 128), jnp.int32),
            pltpu.SemaphoreType.DMA,
        ],
        compiler_params=pltpu.CompilerParams(vmem_limit_bytes=40 * 1024 * 1024),
        name="pack",
    )(
        me,
        chosen,
        key_rows.reshape(blocks, KEY_BLOCK, -1),
        value_rows.reshape(blocks, KEY_BLOCK, -1),
    )


def attend(head, q, g, k, v, lse, bias, far_kv, gq_full):
    rows, width = q.shape
    heads = lse.shape[0]
    tiles = rows // TQ
    spans = far_kv.shape[0]
    far = spans * CAP * KEY_BLOCK
    first = gq_full is None
    column = pl.BlockSpec((TQ, HEAD_DIM), lambda i: (i, head))
    alone = pl.BlockSpec((TQ, HEAD_DIM), lambda i: (i, 0))
    whole = pl.BlockSpec(far_kv.shape, lambda i: (0, 0, 0, 0, 0))
    in_specs = [
        column,
        column,
        column,
        column,
        pl.BlockSpec((heads, TQ), lambda i: (0, i)),
        pl.BlockSpec((None, spans * CAP, TQ), lambda i: (head, 0, i)),
        whole,
    ]
    args = [q, g, k, v, lse, bias, far_kv]
    aliases = {}
    if not first:
        in_specs.append(pl.BlockSpec(memory_space=pl.ANY))
        args.append(gq_full)
        aliases = {7: 0}
    flops = 10 * rows * far * HEAD_DIM
    return pl.pallas_call(
        functools.partial(attend_kernel, head=head, first=first, tiles=tiles, far=far),
        grid=(tiles,),
        in_specs=in_specs,
        out_specs=[column, alone, alone, alone, whole],
        out_shape=[
            jax.ShapeDtypeStruct((rows, width), jnp.bfloat16),
            jax.ShapeDtypeStruct((rows, HEAD_DIM), jnp.bfloat16),
            jax.ShapeDtypeStruct((rows, HEAD_DIM), jnp.float32),
            jax.ShapeDtypeStruct((rows, HEAD_DIM), jnp.float32),
            jax.ShapeDtypeStruct(far_kv.shape, jnp.bfloat16),
        ],
        scratch_shapes=[
            pltpu.VMEM((far, TQ), jnp.float32),
            pltpu.VMEM((far, TQ), jnp.float32),
            pltpu.VMEM((far, TQ), jnp.bfloat16),
            pltpu.VMEM((far, HEAD_DIM), jnp.float32),
            pltpu.VMEM((far, HEAD_DIM), jnp.float32),
            pltpu.VMEM((HEAD_DIM, far), jnp.bfloat16),
        ],
        input_output_aliases=aliases,
        cost_estimate=pl.CostEstimate(
            flops=flops, transcendentals=rows * far, bytes_accessed=8 * 1024 * 1024
        ),
        compiler_params=pltpu.CompilerParams(
            dimension_semantics=("arbitrary",), vmem_limit_bytes=40 * 1024 * 1024
        ),
        name=f"attend{head}",
    )(*args)


def land(head, me, tab, home, dko, dvo, full, rows, width):
    spans = home.shape[0]
    smem = pl.BlockSpec(memory_space=pltpu.SMEM)
    column = pl.BlockSpec((rows, HEAD_DIM), lambda i: (0, head))
    alone = pl.BlockSpec((rows, HEAD_DIM), lambda i: (0, 0))
    in_specs = [smem, smem, pl.BlockSpec(home.shape, lambda i: (0, 0, 0, 0, 0)), alone, alone]
    args = [me, tab, home, dko, dvo]
    aliases = {}
    if full is not None:
        in_specs += [pl.BlockSpec(memory_space=pl.ANY)] * 2
        args += list(full)
        aliases = {5: 0, 6: 1}
    return pl.pallas_call(
        functools.partial(land_kernel, head=head, spans=spans),
        grid=(1,),
        in_specs=in_specs,
        out_specs=[column, column],
        out_shape=[jax.ShapeDtypeStruct((rows, width), jnp.float32)] * 2,
        input_output_aliases=aliases,
        compiler_params=pltpu.CompilerParams(vmem_limit_bytes=40 * 1024 * 1024),
        name=f"land{head}",
    )(*args)


def exchange(x):
    return lax.all_to_all(x, "kv", split_axis=0, concat_axis=0, tiled=True)


def local(query_rows, key_rows, value_rows, log_sums, cotangent, layer_input, chosen):
    spans = lax.axis_size("kv")
    heads = log_sums.shape[0]
    rows, width = query_rows.shape
    blocks = rows // KEY_BLOCK
    me = lax.axis_index("kv").astype(jnp.int32).reshape(1)
    packed = pack(me, chosen, key_rows, value_rows, heads, spans, blocks)
    sends, tab, bias = packed[:heads], packed[heads], packed[heads + 1]
    fars = [exchange(s) for s in sends]
    gq_full = None
    full = None
    weights = []
    for h in range(heads):
        gq_full, gq, dko, dvo, back = attend(
            h, query_rows, cotangent, key_rows, value_rows, log_sums, bias, fars[h], gq_full
        )
        home = exchange(back)
        everyone = lax.all_gather(gq, "tp", axis=0)
        part = lax.dot_general(
            layer_input,
            everyone,
            (((0,), (1,)), ((), ())),
            preferred_element_type=jnp.float32,
        ).astype(jnp.bfloat16)
        mine = exchange(part.reshape(spans, -1, part.shape[1] * HEAD_DIM))
        weights.append(mine.astype(jnp.float32).sum(axis=0))
        full = land(h, me, tab, home, dko, dvo, full, rows, width)
    tp = lax.axis_size("tp")
    stacked = jnp.stack([w.reshape(-1, tp, HEAD_DIM) for w in weights], axis=2)
    grad_weight = stacked.reshape(stacked.shape[0], -1)
    return gq_full, full[0], full[1], grad_weight


def solution(mesh):
    placed = (
        P("kv", "tp"),
        P("kv", "tp"),
        P("kv", "tp"),
        P("tp", "kv"),
        P("kv", "tp"),
        P("kv", "tp"),
        P("tp", None, None),
    )
    return jax.shard_map(
        local,
        mesh=mesh,
        in_specs=placed,
        out_specs=(P("kv", "tp"), P("kv", "tp"), P("kv", "tp"), P(("tp", "kv"), None)),
        check_vma=False,
    )
```

```python
import functools

import jax
import jax.numpy as jnp
from jax import lax
from jax.experimental import pallas as pl
from jax.experimental.pallas import tpu as pltpu
from jax.sharding import PartitionSpec as P


HEAD_DIM = 128
KEY_BLOCK = 32
CAP = 2
BIG = 1 << 20
LOG2E = 1.4426950408889634
NEG = -1.0e30
TQ = 512
KB = 256


def spread(column):
    wide = jnp.broadcast_to(column.astype(jnp.float32), (column.shape[0], 128))
    wide = jnp.concatenate([wide, jnp.zeros((128 - column.shape[0], 128), jnp.float32)], axis=0)
    return wide.T[0:1, :].astype(jnp.int32)


def copy_blocks(tab_s, k_ref, v_ref, send, h, half, lanes):
    def fill(m, carry):
        for odd in range(2):
            for c in range(CAP):
                b = tab_s[2 * c + odd, h * half + m]
                send[2 * m + odd, c] = k_ref[b, :, lanes]
                send[2 * m + odd, CAP + c] = v_ref[b, :, lanes]
        return carry

    lax.fori_loop(0, half, fill, 0, unroll=2)


def first_kernel(me_ref, chosen_ref, k_ref, v_ref, send, tab_ref, lo_s, hi_s, tab_v, tab_s, sem,
                 *, heads, spans, blocks):
    me = me_ref[0]
    half = spans // 2
    for h in range(heads):
        ids = chosen_ref[h]
        mine = (ids >> 6) == me
        lo = jnp.min(jnp.where(mine, ids, BIG), axis=0, keepdims=True)
        hi = jnp.max(jnp.where(mine, ids, -1), axis=0, keepdims=True)
        for m in range(half):
            lo_s[h * half + m : h * half + m + 1, :] = lo[:, m * 128 : (m + 1) * 128]
            hi_s[h * half + m : h * half + m + 1, :] = hi[:, m * 128 : (m + 1) * 128]
    lane = lax.broadcasted_iota(jnp.int32, (heads * half, 128), 1)
    tab_v[...] = jnp.zeros((8, 128), jnp.int32)
    for odd in range(2):
        ours = (lane // blocks) == odd
        lo = spread(jnp.min(jnp.where(ours, lo_s[...], BIG), axis=1, keepdims=True))
        hi = spread(jnp.max(jnp.where(ours, hi_s[...], -1), axis=1, keepdims=True))
        tab_v[odd : odd + 1, :] = lo & (blocks - 1)
        tab_v[2 + odd : 3 + odd, :] = jnp.maximum(hi, 0) & (blocks - 1)
        tab_v[4 + odd : 5 + odd, :] = (hi >= 0).astype(jnp.int32)
        tab_v[6 + odd : 7 + odd, :] = (hi > lo).astype(jnp.int32)
    tab_ref[...] = tab_v[...]
    copy = pltpu.make_async_copy(tab_v, tab_s, sem)
    copy.start()
    copy.wait()
    copy_blocks(tab_s, k_ref, v_ref, send, 0, half, slice(0, HEAD_DIM))


def pack_kernel(tab_ref, k_ref, v_ref, *sends, spans):
    for n, send in enumerate(sends):
        h = n + 1
        lanes = slice(h * HEAD_DIM, (h + 1) * HEAD_DIM)
        copy_blocks(tab_ref, k_ref, v_ref, send, h, spans // 2, lanes)


def mask_kernel(me_ref, chosen_ref, bias_ref, *, heads, spans, blocks, picks):
    me = me_ref[0]
    slots = spans * CAP
    slot = lax.broadcasted_iota(jnp.int32, (slots, 128), 0)
    lane = lax.broadcasted_iota(jnp.int32, (slots, 128), 1)
    ours = (lane // blocks) == (me % 2)
    place = lax.broadcasted_iota(jnp.int32, (128, blocks * KEY_BLOCK), 1) // KEY_BLOCK
    row = lax.broadcasted_iota(jnp.int32, (128, blocks * KEY_BLOCK), 0)
    expand = ((place + (me % 2) * blocks) == row).astype(jnp.bfloat16)
    start = pl.multiple_of((me // 2) * 128, 128)
    for h in range(heads):
        ids = chosen_ref[h, :, pl.ds(start, 128)]
        cols = [jnp.broadcast_to(ids[c : c + 1, :], (slots, 128)) for c in range(picks)]
        least = jnp.full((slots, 128), BIG, jnp.int32)
        most = jnp.full((slots, 128), -1, jnp.int32)
        for col in cols:
            hit = ((col >> 6) == (slot >> 1)) & ours
            least = jnp.minimum(least, jnp.where(hit, col, BIG))
            most = jnp.maximum(most, jnp.where(hit, col, -1))
        least = jnp.min(least, axis=1, keepdims=True)
        most = jnp.max(most, axis=1, keepdims=True)
        name = jnp.where(
            (slot & 1) == 0, least, jnp.where(most > least, most, -7)
        )
        named = cols[0] == name
        for col in cols[1:]:
            named = named | (col == name)
        hot = jnp.where(named, 1.0, 0.0).astype(jnp.bfloat16)
        full = jnp.dot(hot, expand, preferred_element_type=jnp.float32)
        bias_ref[h] = jnp.where(full > 0.5, 0.0, NEG)


def turn_kernel(x_ref, out_ref):
    rows = x_ref.shape[0]
    for i in range(rows // 256):
        cut = slice(i * 256, (i + 1) * 256)
        out_ref[:, cut] = x_ref[cut, :].T


def weight_kernel(xt_ref, *rest, shards):
    out_ref = rest[-1]
    xt = xt_ref[...]
    shape = (out_ref.shape[0],) + out_ref.shape[2:]
    for at in range(0, shards, 2):
        g = jnp.concatenate([rest[at][...], rest[at + 1][...]], axis=1)
        got = jnp.dot(xt, g, preferred_element_type=jnp.float32).astype(jnp.bfloat16)
        out_ref[:, at] = got[:, :HEAD_DIM].reshape(shape)
        out_ref[:, at + 1] = got[:, HEAD_DIM:].reshape(shape)


def total_kernel(at_ref, got_ref, *rest, head, heads, order):
    out_ref = rest[-1]
    if len(rest) > 1:
        out_ref[...] = rest[0][...]
    me = at_ref[0]
    tp = len(order)
    for p in range(tp):
        acc = got_ref[0, p].astype(jnp.float32)
        for i in range(1, got_ref.shape[0]):
            acc = acc + got_ref[i, p].astype(jnp.float32)
        place = (me + order[p]) % tp
        first = pl.multiple_of((place * heads + head) * HEAD_DIM, HEAD_DIM)
        out_ref[:, pl.ds(first, HEAD_DIM)] = acc


def attend_kernel(me_ref, *refs, head, extra, merge, tiles, far):
    q_ref, g_ref, ko_ref, vo_ref, lse_ref, bias_ref, kv_ref = refs[:7]
    ahead_ref = refs[7] if merge else None
    rest = refs[7 + merge + extra :]
    gqf_ref, gq_ref, dko_ref, dvo_ref, back_ref = rest[:5]
    p_s, dp_s, ds_s, dk_s, dv_s, kt_s = rest[5:]
    step = pl.program_id(0)
    scale = HEAD_DIM**-0.5
    nkb = far // KB
    per = KB // (CAP * KEY_BLOCK)

    @pl.when(step == 0)
    def _():
        dk_s[...] = jnp.zeros_like(dk_s)
        dv_s[...] = jnp.zeros_like(dv_s)
        for i in range(nkb):
            keys = kv_ref[i * per : (i + 1) * per, 0:CAP].reshape(KB, HEAD_DIM)
            kt_s[:, i * KB : (i + 1) * KB] = keys.astype(jnp.float32).T.astype(jnp.bfloat16)

    q = q_ref[...]
    g = g_ref[...]
    lse = lse_ref[head : head + 1, :] * LOG2E
    nt = (((1,), (1,)), ((), ()))

    def ahead(i, dots):
        keys = kv_ref[pl.ds(i * per, per), 0:CAP].reshape(KB, HEAD_DIM)
        values = kv_ref[pl.ds(i * per, per), CAP : 2 * CAP].reshape(KB, HEAD_DIM)
        s = lax.dot_general(keys, q, nt, preferred_element_type=jnp.float32)
        dp = lax.dot_general(values, g, nt, preferred_element_type=jnp.float32)
        shift = bias_ref[pl.ds(i * per * CAP, per * CAP), :] - lse
        s = (s * (scale * LOG2E)).reshape(per * CAP, KEY_BLOCK, TQ) + shift[:, None, :]
        p = jnp.exp2(s).reshape(KB, TQ)
        rows = pl.ds(i * KB, KB)
        p_s[rows, :] = p
        dp_s[rows, :] = dp
        dv_s[rows, :] += jnp.dot(
            p.astype(jnp.bfloat16), g, preferred_element_type=jnp.float32
        )
        return dots + (p * dp).reshape(KB // 8, 8, TQ).sum(axis=0)

    dots = jnp.zeros((8, TQ), jnp.float32)
    for i in range(nkb):
        dots = ahead(i, dots)
    dots = jnp.sum(dots, axis=0, keepdims=True)
    key_at = lax.broadcasted_iota(jnp.int32, (128, 128), 0)
    row_at = lax.broadcasted_iota(jnp.int32, (128, 128), 1)
    near = (key_at // KEY_BLOCK == row_at // KEY_BLOCK) & (key_at <= row_at)
    own = []
    own_dots = []
    for t in range(TQ // 128):
        cut = slice(t * 128, (t + 1) * 128)
        s = lax.dot_general(ko_ref[cut, :], q[cut], nt, preferred_element_type=jnp.float32)
        dp = lax.dot_general(vo_ref[cut, :], g[cut], nt, preferred_element_type=jnp.float32)
        p = jnp.exp2(jnp.where(near, s * (scale * LOG2E) - lse[:, cut], NEG))
        own.append((p, dp))
        own_dots.append(jnp.sum(p * dp, axis=0, keepdims=True))
        dvo_ref[cut, :] = jnp.dot(
            p.astype(jnp.bfloat16), g[cut], preferred_element_type=jnp.float32
        )
    dots = dots + jnp.concatenate(own_dots, axis=1)

    def behind(i, carry):
        rows = pl.ds(i * KB, KB)
        ds = (p_s[rows, :] * (dp_s[rows, :] - dots)).astype(jnp.bfloat16)
        ds_s[rows, :] = ds
        dk_s[rows, :] += jnp.dot(ds, q, preferred_element_type=jnp.float32)
        part = jnp.dot(kt_s[:, rows], ds, preferred_element_type=jnp.float32)
        return part if carry is None else carry + part

    total = None
    for i in range(nkb):
        total = behind(i, total)
    for t in range(TQ // 128):
        cut = slice(t * 128, (t + 1) * 128)
        p, dp = own[t]
        ds = (p * (dp - dots[:, cut])).astype(jnp.bfloat16)
        dko_ref[cut, :] = scale * jnp.dot(ds, q[cut], preferred_element_type=jnp.float32)
        kt = ko_ref[cut, :].astype(jnp.float32).T.astype(jnp.bfloat16)
        part = total[:, cut] + jnp.dot(kt, ds, preferred_element_type=jnp.float32)
        out = (scale * part).T.astype(jnp.bfloat16)
        gq_ref[cut, :] = out
        gqf_ref[cut, :] = out

    @pl.when(step == tiles - 1)
    def _():
        shape = (far // (CAP * KEY_BLOCK), CAP, KEY_BLOCK, HEAD_DIM)
        dk = (scale * dk_s[...]).astype(jnp.bfloat16).reshape(shape)
        dv = dv_s[...].astype(jnp.bfloat16).reshape(shape)
        if merge:
            me = me_ref[0]
            for n in range(shape[0]):

                @pl.when(n < me)
                def _(n=n):
                    back_ref[n, 0:CAP] = dk[n]
                    back_ref[n, CAP : 2 * CAP] = dv[n]

                @pl.when(n >= me)
                def _(n=n):
                    back_ref[n] = ahead_ref[n]
        else:
            back_ref[:, 0:CAP] = dk
            back_ref[:, CAP : 2 * CAP] = dv


def land_kernel(me_ref, tab_ref, back_ref, dko_ref, dvo_ref, *rest, head, spans):
    gk_ref, gv_ref = rest[-2:]
    gk_ref[...] = dko_ref[...]
    gv_ref[...] = dvo_ref[...]
    me = me_ref[0]
    half = spans // 2

    def one(n, carry):
        at = head * half + n // 2
        odd = n % 2
        for c in range(CAP):

            @pl.when(tab_ref[4 + 2 * c + odd, at] > 0)
            def _(c=c):
                first = tab_ref[2 * c + odd, at] * KEY_BLOCK
                rows = pl.ds(pl.multiple_of(first, KEY_BLOCK), KEY_BLOCK)
                gk_ref[rows, :] += back_ref[n, c].astype(jnp.float32)
                gv_ref[rows, :] += back_ref[n, CAP + c].astype(jnp.float32)

        return carry

    lax.fori_loop(me + 1, spans, one, 0)


SMEM = pl.BlockSpec(memory_space=pltpu.SMEM)
VMEM = pl.BlockSpec(memory_space=pltpu.VMEM)
ANY = pl.BlockSpec(memory_space=pl.ANY)


def params(**more):
    return pltpu.CompilerParams(vmem_limit_bytes=60 * 1024 * 1024, **more)


def cost(flops, data=1 << 20):
    return pl.CostEstimate(flops=flops, transcendentals=0, bytes_accessed=data)


def five(spans, slots=1):
    return (spans, slots, 2 * CAP, KEY_BLOCK, HEAD_DIM)


def slotted(spans, slot):
    return pl.BlockSpec(
        (spans, None, 2 * CAP, KEY_BLOCK, HEAD_DIM), lambda i: (0, slot, 0, 0, 0)
    )


def pack_first(me, ids, key_blocks, value_blocks, heads, spans):
    blocks = key_blocks.shape[0]
    column = pl.BlockSpec((blocks, KEY_BLOCK, HEAD_DIM), lambda i: (0, 0, 0))
    return pl.pallas_call(
        functools.partial(first_kernel, heads=heads, spans=spans, blocks=blocks),
        grid=(1,),
        out_shape=[
            jax.ShapeDtypeStruct(five(spans), jnp.bfloat16),
            jax.ShapeDtypeStruct((8, 128), jnp.int32),
        ],
        in_specs=[SMEM, VMEM, column, column],
        out_specs=[slotted(spans, 0), VMEM],
        scratch_shapes=[
            pltpu.VMEM((heads * spans // 2, 128), jnp.int32),
            pltpu.VMEM((heads * spans // 2, 128), jnp.int32),
            pltpu.VMEM((8, 128), jnp.int32),
            pltpu.SMEM((8, 128), jnp.int32),
            pltpu.SemaphoreType.DMA,
        ],
        compiler_params=params(),
        cost_estimate=cost(1 << 26),
        name="first",
    )(me, ids, key_blocks, value_blocks)


def pack_rest(tab, key_blocks, value_blocks, heads, spans):
    return pl.pallas_call(
        functools.partial(pack_kernel, spans=spans),
        grid=(1,),
        out_shape=[jax.ShapeDtypeStruct(five(spans), jnp.bfloat16)] * (heads - 1),
        in_specs=[SMEM, VMEM, VMEM],
        out_specs=[slotted(spans, 0)] * (heads - 1),
        compiler_params=params(),
        cost_estimate=cost(1 << 26),
        name="pack",
    )(tab, key_blocks, value_blocks)


def mask(me, ids, spans, blocks):
    heads, picks, _ = ids.shape
    return pl.pallas_call(
        functools.partial(mask_kernel, heads=heads, spans=spans, blocks=blocks, picks=picks),
        out_shape=jax.ShapeDtypeStruct((heads, spans * CAP, blocks * KEY_BLOCK), jnp.float32),
        in_specs=[SMEM, VMEM],
        out_specs=VMEM,
        compiler_params=params(),
        cost_estimate=cost(1 << 26),
        name="mask",
    )(me, ids)


def turn(x):
    rows, cols = x.shape
    return pl.pallas_call(
        turn_kernel,
        grid=(cols // 256,),
        out_shape=jax.ShapeDtypeStruct((cols, rows), x.dtype),
        in_specs=[pl.BlockSpec((rows, 256), lambda i: (0, i))],
        out_specs=pl.BlockSpec((256, rows), lambda i: (i, 0)),
        compiler_params=params(),
        cost_estimate=cost(1 << 26),
        name="turn",
    )(x)


def attend(head, me, q, g, k, v, lse, bias, far_kv, gq_full, ahead, slots):
    rows, width = q.shape
    heads = lse.shape[0]
    tiles = rows // TQ
    spans = far_kv.shape[0]
    far = spans * CAP * KEY_BLOCK
    column = pl.BlockSpec((TQ, HEAD_DIM), lambda i: (i, head))
    alone = pl.BlockSpec((TQ, HEAD_DIM), lambda i: (i, 0))
    in_specs = [
        SMEM,
        column,
        column,
        column,
        column,
        pl.BlockSpec((heads, TQ), lambda i: (0, i)),
        pl.BlockSpec((None, spans * CAP, TQ), lambda i: (head, 0, i)),
        slotted(spans, 0),
    ]
    args = [me, q, g, k, v, lse, bias, far_kv]
    merge = ahead is not None
    if merge:
        in_specs.append(slotted(spans, 0))
        args.append(ahead)
    aliases = {}
    if gq_full is not None:
        aliases[len(args)] = 0
        in_specs.append(ANY)
        args.append(gq_full)
    return pl.pallas_call(
        functools.partial(
            attend_kernel, head=head, extra=len(aliases), merge=int(merge), tiles=tiles, far=far
        ),
        grid=(tiles,),
        in_specs=in_specs,
        out_specs=[column, alone, alone, alone, slotted(spans, 0)],
        out_shape=[
            jax.ShapeDtypeStruct((rows, width), jnp.bfloat16),
            jax.ShapeDtypeStruct((rows, HEAD_DIM), jnp.bfloat16),
            jax.ShapeDtypeStruct((rows, HEAD_DIM), jnp.float32),
            jax.ShapeDtypeStruct((rows, HEAD_DIM), jnp.float32),
            jax.ShapeDtypeStruct(five(spans, slots), jnp.bfloat16),
        ],
        scratch_shapes=[
            pltpu.VMEM((far, TQ), jnp.float32),
            pltpu.VMEM((far, TQ), jnp.float32),
            pltpu.VMEM((far, TQ), jnp.bfloat16),
            pltpu.VMEM((far, HEAD_DIM), jnp.float32),
            pltpu.VMEM((far, HEAD_DIM), jnp.float32),
            pltpu.VMEM((HEAD_DIM, far), jnp.bfloat16),
        ],
        input_output_aliases=aliases,
        cost_estimate=cost(10 * rows * far * HEAD_DIM, 8 << 20),
        compiler_params=params(dimension_semantics=("arbitrary",)),
    )(*args)


def weigh(xt, shards, buffer, spans, slot, slots):
    cols, rows = xt.shape
    tall = pl.BlockSpec((rows, HEAD_DIM), lambda i: (0, 0))
    tall_rows = 256
    in_specs = [pl.BlockSpec((tall_rows, rows), lambda i: (i, 0))] + [tall] * len(shards)
    args = [xt, *shards]
    aliases = {}
    if buffer is not None:
        aliases[len(args)] = 0
        in_specs.append(ANY)
        args.append(buffer)
    owned = cols // spans
    per = tall_rows // owned
    return pl.pallas_call(
        functools.partial(weight_kernel, shards=len(shards)),
        grid=(cols // tall_rows,),
        in_specs=in_specs,
        out_specs=pl.BlockSpec(
            (per, None, len(shards), owned, HEAD_DIM), lambda i: (i, slot, 0, 0, 0)
        ),
        out_shape=jax.ShapeDtypeStruct(five(spans, slots), jnp.bfloat16),
        input_output_aliases=aliases,
        compiler_params=params(),
        cost_estimate=cost(2 * cols * rows * len(shards) * HEAD_DIM, 8 << 20),
        name="weigh",
    )(*args)


def total(place, got, slot, buffer, head, heads, order):
    spans = got.shape[0]
    args = [place, got]
    in_specs = [SMEM, slotted(spans, slot)]
    aliases = {}
    if buffer is not None:
        aliases = {2: 0}
        in_specs.append(VMEM)
        args.append(buffer)
    return pl.pallas_call(
        functools.partial(total_kernel, head=head, heads=heads, order=order),
        grid=(1,),
        in_specs=in_specs,
        out_specs=VMEM,
        out_shape=jax.ShapeDtypeStruct(
            (KEY_BLOCK, len(order) * heads * HEAD_DIM), jnp.float32
        ),
        input_output_aliases=aliases,
        compiler_params=params(),
        cost_estimate=cost(1 << 24),
        name="total",
    )(*args)


def land(head, me, tab, home, dko, dvo, full, rows, width):
    spans = home.shape[0]
    column = pl.BlockSpec((rows, HEAD_DIM), lambda i: (0, head))
    alone = pl.BlockSpec((rows, HEAD_DIM), lambda i: (0, 0))
    in_specs = [SMEM, SMEM, slotted(spans, 0), alone, alone]
    args = [me, tab, home, dko, dvo]
    aliases = {}
    if full is not None:
        in_specs += [ANY, ANY]
        args += list(full)
        aliases = {5: 0, 6: 1}
    return pl.pallas_call(
        functools.partial(land_kernel, head=head, spans=spans),
        grid=(1,),
        in_specs=in_specs,
        out_specs=[column, column],
        out_shape=[jax.ShapeDtypeStruct((rows, width), jnp.float32)] * 2,
        input_output_aliases=aliases,
        compiler_params=params(),
        cost_estimate=cost(1 << 24),
    )(*args)


def exchange(x):
    return lax.all_to_all(x, "kv", split_axis=0, concat_axis=0, tiled=True)


def shift(x, by, tp):
    return lax.ppermute(x, "tp", [(i, (i + by) % tp) for i in range(tp)])


def program(query_rows, key_rows, value_rows, log_sums, cotangent, layer_input, chosen):
    spans = lax.axis_size("kv")
    tp = lax.axis_size("tp")
    heads = log_sums.shape[0]
    rows, width = query_rows.shape
    blocks = rows // KEY_BLOCK
    me = lax.axis_index("kv").astype(jnp.int32).reshape(1)
    place = lax.axis_index("tp").astype(jnp.int32).reshape(1)
    ids = jnp.transpose(chosen, (0, 2, 1))
    key_blocks = key_rows.reshape(blocks, KEY_BLOCK, width)
    value_blocks = value_rows.reshape(blocks, KEY_BLOCK, width)
    order = (0, 1, 3, 2)

    send0, tab = pack_first(me, ids, key_blocks, value_blocks, heads, spans)
    far0 = exchange(send0)
    send1, send2 = pack_rest(tab, key_blocks, value_blocks, heads, spans)
    xt = turn(layer_input)
    bias = mask(me, ids, spans, blocks)

    def attention(h, far, gq_full, ahead, slots):
        return attend(
            h, me, query_rows, cotangent, key_rows, value_rows, log_sums, bias, far,
            gq_full, ahead, slots,
        )

    def gathered(gq):
        right = shift(gq, -1, tp)
        left = shift(gq, 1, tp)
        across = shift(gq, 2, tp)
        return gq, right, left, across

    def product(shards, buffer, slot, slots):
        return weigh(xt, shards, buffer, spans, slot, slots)

    far1 = exchange(send1)
    gq_full, gq, *own0, out = attention(0, far0, None, send2, 1)
    shards0 = gathered(gq)
    far2 = exchange(out)
    gq_full, gq, *own1, out = attention(1, far1, gq_full, None, 2)
    shards1 = gathered(gq)
    home1 = exchange(product(shards0, out, 1, 2))
    gq_full, gq, *own2, out = attention(2, far2, gq_full, None, 2)
    shards2 = gathered(gq)
    home2 = exchange(product(shards1, out, 1, 2))
    last = exchange(product(shards2, None, 0, 1))

    full = None
    for h, (home, own) in enumerate(((far2, own0), (home1, own1), (home2, own2))):
        full = land(h, me, tab, home, *own, full, rows, width)
    grad_weight = None
    for h, (got, slot) in enumerate(((home1, 1), (home2, 1), (last, 0))):
        grad_weight = total(place, got, slot, grad_weight, h, heads, order)
    return gq_full, full[0], full[1], grad_weight


def solution(mesh):
    placed = (
        P("kv", "tp"),
        P("kv", "tp"),
        P("kv", "tp"),
        P("tp", "kv"),
        P("kv", "tp"),
        P("kv", "tp"),
        P("tp", None, None),
    )
    return jax.shard_map(
        program,
        mesh=mesh,
        in_specs=placed,
        out_specs=(P("kv", "tp"), P("kv", "tp"), P("kv", "tp"), P(("tp", "kv"), None)),
        check_vma=False,
    )
```

```python
import functools

import jax
import jax.numpy as jnp
from jax import lax
from jax.experimental import pallas as pl
from jax.experimental.pallas import tpu as pltpu
from jax.sharding import PartitionSpec as P


HEAD_DIM = 128
KEY_BLOCK = 32
CAP = 2
BIG = 1 << 20
LOG2E = 1.4426950408889634
NEG = -1.0e30
TQ = 512
VMEM_LIMIT = 60960 * 1024
WEIGH_ROWS = 512
KB = 256


def spread(column):
    wide = jnp.broadcast_to(column.astype(jnp.float32), (column.shape[0], 128))
    wide = jnp.concatenate([wide, jnp.zeros((128 - column.shape[0], 128), jnp.float32)], axis=0)
    return wide.T[0:1, :].astype(jnp.int32)


def copy_blocks(tab_s, k_ref, v_ref, send, h, half, lanes):
    def fill(m, carry):
        for odd in range(2):
            for c in range(CAP):
                b = tab_s[2 * c + odd, h * half + m]
                send[2 * m + odd, c] = k_ref[b, :, lanes]
                send[2 * m + odd, CAP + c] = v_ref[b, :, lanes]
        return carry

    lax.fori_loop(0, half, fill, 0, unroll=2)


def first_kernel(me_ref, chosen_ref, k_ref, v_ref, send, tab_ref, lo_s, hi_s, tab_v, tab_s, sem,
                 *, heads, spans, blocks):
    me = me_ref[0]
    half = spans // 2
    for h in range(heads):
        ids = chosen_ref[h]
        mine = (ids >> 6) == me
        lo = jnp.min(jnp.where(mine, ids, BIG), axis=0, keepdims=True)
        hi = jnp.max(jnp.where(mine, ids, -1), axis=0, keepdims=True)
        for m in range(half):
            lo_s[h * half + m : h * half + m + 1, :] = lo[:, m * 128 : (m + 1) * 128]
            hi_s[h * half + m : h * half + m + 1, :] = hi[:, m * 128 : (m + 1) * 128]
    lane = lax.broadcasted_iota(jnp.int32, (heads * half, 128), 1)
    tab_v[...] = jnp.zeros((8, 128), jnp.int32)
    for odd in range(2):
        ours = (lane // blocks) == odd
        lo = spread(jnp.min(jnp.where(ours, lo_s[...], BIG), axis=1, keepdims=True))
        hi = spread(jnp.max(jnp.where(ours, hi_s[...], -1), axis=1, keepdims=True))
        tab_v[odd : odd + 1, :] = lo & (blocks - 1)
        tab_v[2 + odd : 3 + odd, :] = jnp.maximum(hi, 0) & (blocks - 1)
        tab_v[4 + odd : 5 + odd, :] = (hi >= 0).astype(jnp.int32)
        tab_v[6 + odd : 7 + odd, :] = (hi > lo).astype(jnp.int32)
    tab_ref[...] = tab_v[...]
    copy = pltpu.make_async_copy(tab_v, tab_s, sem)
    copy.start()
    copy.wait()
    copy_blocks(tab_s, k_ref, v_ref, send, 0, half, slice(0, HEAD_DIM))


def pack_kernel(tab_ref, k_ref, v_ref, *sends, spans):
    for n, send in enumerate(sends):
        h = n + 1
        lanes = slice(h * HEAD_DIM, (h + 1) * HEAD_DIM)
        copy_blocks(tab_ref, k_ref, v_ref, send, h, spans // 2, lanes)


def mask_kernel(me_ref, chosen_ref, bias_ref, *, heads, spans, blocks, picks):
    me = me_ref[0]
    slots = spans * CAP
    slot = lax.broadcasted_iota(jnp.int32, (slots, 128), 0)
    lane = lax.broadcasted_iota(jnp.int32, (slots, 128), 1)
    ours = (lane // blocks) == (me % 2)
    place = lax.broadcasted_iota(jnp.int32, (128, blocks * KEY_BLOCK), 1) // KEY_BLOCK
    row = lax.broadcasted_iota(jnp.int32, (128, blocks * KEY_BLOCK), 0)
    expand = ((place + (me % 2) * blocks) == row).astype(jnp.bfloat16)
    start = pl.multiple_of((me // 2) * 128, 128)
    for h in range(heads):
        ids = chosen_ref[h, :, pl.ds(start, 128)]
        cols = [jnp.broadcast_to(ids[c : c + 1, :], (slots, 128)) for c in range(picks)]
        least = jnp.full((slots, 128), BIG, jnp.int32)
        most = jnp.full((slots, 128), -1, jnp.int32)
        for col in cols:
            hit = ((col >> 6) == (slot >> 1)) & ours
            least = jnp.minimum(least, jnp.where(hit, col, BIG))
            most = jnp.maximum(most, jnp.where(hit, col, -1))
        least = jnp.min(least, axis=1, keepdims=True)
        most = jnp.max(most, axis=1, keepdims=True)
        name = jnp.where(
            (slot & 1) == 0, least, jnp.where(most > least, most, -7)
        )
        named = cols[0] == name
        for col in cols[1:]:
            named = named | (col == name)
        hot = jnp.where(named, 1.0, 0.0).astype(jnp.bfloat16)
        full = jnp.dot(hot, expand, preferred_element_type=jnp.float32)
        bias_ref[h] = jnp.where(full > 0.5, 0.0, NEG)


def turn_kernel(x_ref, out_ref):
    rows = x_ref.shape[0]
    for i in range(rows // 256):
        cut = slice(i * 256, (i + 1) * 256)
        out_ref[:, cut] = x_ref[cut, :].T


def weight_kernel(me_ref, xt_ref, *rest, shards, steps, halves):
    span = xt_ref.shape[0] // steps
    xt = xt_ref[pl.ds(pl.multiple_of(pl.program_id(0) * span, span), span), :]
    core = me_ref[0] % 2
    shape = (span // KEY_BLOCK, KEY_BLOCK, HEAD_DIM)
    sums = []
    for at in range(0, shards, 2):
        g = jnp.concatenate([rest[at][...], rest[at + 1][...]], axis=1)
        got = jnp.dot(xt, g, preferred_element_type=jnp.float32).astype(jnp.bfloat16)
        sums += [got[:, :HEAD_DIM].reshape(shape), got[:, HEAD_DIM:].reshape(shape)]
    if halves:
        keep_ref, give_ref = rest[-2:]
        for p in range(2):
            keep_ref[:, p] = jnp.where(core == 0, sums[p], sums[2 + p])
            give_ref[:, p] = jnp.where(core == 0, sums[2 + p], sums[p])
    else:
        for p in range(shards):
            rest[-1][:, p] = sums[p]


def join_kernel(keep_ref, got_ref, *rest):
    out_ref = rest[-1]
    both = keep_ref[...].astype(jnp.float32) + got_ref[...].astype(jnp.float32)
    out_ref[...] = both.astype(jnp.bfloat16)


def put_sum(out_ref, got_ref, sources, column, first):
    acc = got_ref[sources[0], column].astype(jnp.float32)
    for i in sources[1:]:
        acc = acc + got_ref[i, column].astype(jnp.float32)
    out_ref[:, pl.ds(pl.multiple_of(first, HEAD_DIM), HEAD_DIM)] = acc


def total_kernel(at_ref, got_ref, out_ref, *, head, heads, order):
    tp = len(order)
    out_ref[...] = jnp.zeros_like(out_ref)
    for p in range(tp):
        place = (at_ref[0] + order[p]) % tp
        sources = range(got_ref.shape[0])
        put_sum(out_ref, got_ref, sources, p, (place * heads + head) * HEAD_DIM)


def pair_total_kernel(at_ref, *refs, first, heads, order):
    before_ref, out_ref = refs[-2:]
    tp = len(order)
    out_ref[...] = before_ref[...]
    for n, got_ref in enumerate(refs[:-2]):
        for p in range(tp):
            place = (at_ref[0] + order[p]) % tp
            sources = range(p // 2, got_ref.shape[0], 2)
            put_sum(out_ref, got_ref, sources, p % 2, (place * heads + first + n) * HEAD_DIM)


def attend_kernel(me_ref, *refs, head, extra, merge, tiles, far):
    q_ref, g_ref, ko_ref, vo_ref, lse_ref, bias_ref, kv_ref = refs[:7]
    ahead_ref = refs[7] if merge else None
    rest = refs[7 + merge + extra :]
    gqf_ref, gq_ref, dko_ref, dvo_ref, back_ref = rest[:5]
    p_s, dp_s, po_s, dpo_s, dots_s, dk_s, dv_s, kt_s, qq_s, kk_s = rest[5:]
    step = pl.program_id(0)
    scale = HEAD_DIM**-0.5
    nkb = far // KB
    per = KB // (CAP * KEY_BLOCK)
    parts = TQ // 128
    nt = (((1,), (1,)), ((), ()))

    def cut(t):
        return slice(t * 128, (t + 1) * 128)

    def ahead(first, behind):
        q = q_ref[...]
        g = g_ref[...]
        lse = lse_ref[head : head + 1, :] * LOG2E
        key_at = lax.broadcasted_iota(jnp.int32, (128, 128), 0)
        row_at = lax.broadcasted_iota(jnp.int32, (128, 128), 1)
        near = (key_at // KEY_BLOCK == row_at // KEY_BLOCK) & (key_at <= row_at)
        dots = jnp.zeros((8, TQ), jnp.float32)
        own_dots = []
        for i in range(nkb):
            rows = slice(i * KB, (i + 1) * KB)
            if behind is not None:
                behind(i)
            keys = kv_ref[i * per : (i + 1) * per, 0:CAP].reshape(KB, HEAD_DIM)
            values = kv_ref[i * per : (i + 1) * per, CAP : 2 * CAP].reshape(KB, HEAD_DIM)
            s = lax.dot_general(keys, q, nt, preferred_element_type=jnp.float32)
            dp = lax.dot_general(values, g, nt, preferred_element_type=jnp.float32)
            shift = bias_ref[i * per * CAP : (i + 1) * per * CAP, :] - lse
            s = (s * (scale * LOG2E)).reshape(per * CAP, KEY_BLOCK, TQ) + shift[:, None, :]
            p = jnp.exp2(s).reshape(KB, TQ)
            p_s[rows, :] = p
            dp_s[rows, :] = dp
            dv = jnp.dot(p.astype(jnp.bfloat16), g, preferred_element_type=jnp.float32)
            dv_s[rows, :] = dv if first else dv_s[rows, :] + dv
            dots = dots + (p * dp).reshape(KB // 8, 8, TQ).sum(axis=0)
            if i < parts:
                c = cut(i)
                s = lax.dot_general(ko_ref[c, :], q[c], nt, preferred_element_type=jnp.float32)
                dp = lax.dot_general(vo_ref[c, :], g[c], nt, preferred_element_type=jnp.float32)
                p = jnp.exp2(jnp.where(near, s * (scale * LOG2E) - lse[:, c], NEG))
                po_s[c, :] = p
                dpo_s[c, :] = dp
                own_dots.append(jnp.sum(p * dp, axis=0, keepdims=True))
                dvo_ref[c, :] = jnp.dot(
                    p.astype(jnp.bfloat16), g[c], preferred_element_type=jnp.float32
                )
        return jnp.sum(dots, axis=0, keepdims=True) + jnp.concatenate(own_dots, axis=1)

    def second_half(first):
        q = qq_s[...]
        dots = dots_s[...]
        held = []
        own = []

        def behind(i):
            rows = slice(i * KB, (i + 1) * KB)
            ds = (p_s[rows, :] * (dp_s[rows, :] - dots)).astype(jnp.bfloat16)
            dk = jnp.dot(ds, q, preferred_element_type=jnp.float32)
            dk_s[rows, :] = dk if first else dk_s[rows, :] + dk
            part = jnp.dot(kt_s[:, rows], ds, preferred_element_type=jnp.float32)
            held[:] = [held[0] + part] if held else [part]
            if i < parts:
                c = cut(i)
                ds = (po_s[c, :] * (dpo_s[c, :] - dots[:, c])).astype(jnp.bfloat16)
                dko_ref[c, :] = scale * jnp.dot(ds, q[c], preferred_element_type=jnp.float32)
                own.append(jnp.dot(kk_s[c, :].T, ds, preferred_element_type=jnp.float32))

        def finish():
            for t in range(parts):
                out = (scale * (held[0][:, cut(t)] + own[t])).T.astype(jnp.bfloat16)
                gq_ref[cut(t), :] = out
                gqf_ref[cut(t), :] = out

        return behind, finish

    def keep(dots):
        dots_s[...] = dots
        qq_s[...] = q_ref[...]
        kk_s[...] = ko_ref[...]

    @pl.when(step == 0)
    def _():
        for i in range(nkb):
            keys = kv_ref[i * per : (i + 1) * per, 0:CAP].reshape(KB, HEAD_DIM)
            kt_s[:, i * KB : (i + 1) * KB] = keys.T
        keep(ahead(True, None))
        dk_s[...] = jnp.zeros_like(dk_s)

    @pl.when((step > 0) & (step < tiles))
    def _():
        behind, finish = second_half(False)
        dots = ahead(False, behind)
        finish()
        keep(dots)

    @pl.when(step == tiles)
    def _():
        behind, finish = second_half(False)
        for i in range(nkb):
            behind(i)
        finish()
        shape = (far // (CAP * KEY_BLOCK), CAP, KEY_BLOCK, HEAD_DIM)
        dk = (scale * dk_s[...]).astype(jnp.bfloat16).reshape(shape)
        dv = dv_s[...].astype(jnp.bfloat16).reshape(shape)
        if merge:
            me = me_ref[0]
            for n in range(shape[0]):

                @pl.when(n < me)
                def _(n=n):
                    back_ref[n, 0:CAP] = dk[n]
                    back_ref[n, CAP : 2 * CAP] = dv[n]

                @pl.when(n >= me)
                def _(n=n):
                    back_ref[n] = ahead_ref[n]
        else:
            back_ref[:, 0:CAP] = dk
            back_ref[:, CAP : 2 * CAP] = dv


def land_kernel(me_ref, tab_ref, back_ref, dko_ref, dvo_ref, *rest, head, spans):
    gk_ref, gv_ref = rest[-2:]
    gk_ref[...] = dko_ref[...]
    gv_ref[...] = dvo_ref[...]
    me = me_ref[0]
    half = spans // 2

    def one(n, carry):
        at = head * half + n // 2
        odd = n % 2
        for c in range(CAP):

            @pl.when(tab_ref[4 + 2 * c + odd, at] > 0)
            def _(c=c):
                first = tab_ref[2 * c + odd, at] * KEY_BLOCK
                rows = pl.ds(pl.multiple_of(first, KEY_BLOCK), KEY_BLOCK)
                gk_ref[rows, :] += back_ref[n, c].astype(jnp.float32)
                gv_ref[rows, :] += back_ref[n, CAP + c].astype(jnp.float32)

        return carry

    lax.fori_loop(me + 1, spans, one, 0)


SMEM = pl.BlockSpec(memory_space=pltpu.SMEM)
VMEM = pl.BlockSpec(memory_space=pltpu.VMEM)
ANY = pl.BlockSpec(memory_space=pl.ANY)


def params(**more):
    return pltpu.CompilerParams(vmem_limit_bytes=VMEM_LIMIT, **more)


def cost(flops, data=1 << 20):
    return pl.CostEstimate(flops=flops, transcendentals=0, bytes_accessed=data)


def five(spans, slots=1):
    return (spans, slots, 2 * CAP, KEY_BLOCK, HEAD_DIM)


def slotted(spans, slot):
    return pl.BlockSpec(
        (spans, None, 2 * CAP, KEY_BLOCK, HEAD_DIM), lambda i: (0, slot, 0, 0, 0)
    )


def pack_first(me, ids, key_blocks, value_blocks, heads, spans):
    blocks = key_blocks.shape[0]
    column = pl.BlockSpec((blocks, KEY_BLOCK, HEAD_DIM), lambda i: (0, 0, 0))
    return pl.pallas_call(
        functools.partial(first_kernel, heads=heads, spans=spans, blocks=blocks),
        grid=(1,),
        out_shape=[
            jax.ShapeDtypeStruct(five(spans), jnp.bfloat16),
            jax.ShapeDtypeStruct((8, 128), jnp.int32),
        ],
        in_specs=[SMEM, VMEM, column, column],
        out_specs=[slotted(spans, 0), VMEM],
        scratch_shapes=[
            pltpu.VMEM((heads * spans // 2, 128), jnp.int32),
            pltpu.VMEM((heads * spans // 2, 128), jnp.int32),
            pltpu.VMEM((8, 128), jnp.int32),
            pltpu.SMEM((8, 128), jnp.int32),
            pltpu.SemaphoreType.DMA,
        ],
        compiler_params=params(),
        cost_estimate=cost(1 << 26),
        name="first",
    )(me, ids, key_blocks, value_blocks)


def pack_rest(tab, key_blocks, value_blocks, heads, spans):
    return pl.pallas_call(
        functools.partial(pack_kernel, spans=spans),
        grid=(1,),
        out_shape=[jax.ShapeDtypeStruct(five(spans), jnp.bfloat16)] * (heads - 1),
        in_specs=[SMEM, VMEM, VMEM],
        out_specs=[slotted(spans, 0)] * (heads - 1),
        compiler_params=params(),
        cost_estimate=cost(1 << 26),
        name="pack",
    )(tab, key_blocks, value_blocks)


def mask(me, ids, spans, blocks):
    heads, picks, _ = ids.shape
    return pl.pallas_call(
        functools.partial(mask_kernel, heads=heads, spans=spans, blocks=blocks, picks=picks),
        out_shape=jax.ShapeDtypeStruct((heads, spans * CAP, blocks * KEY_BLOCK), jnp.float32),
        in_specs=[SMEM, VMEM],
        out_specs=VMEM,
        compiler_params=params(),
        cost_estimate=cost(1 << 26),
        name="mask",
    )(me, ids)


def turn(x):
    rows, cols = x.shape
    return pl.pallas_call(
        turn_kernel,
        grid=(cols // 256,),
        out_shape=pltpu.VMEM((cols, rows), x.dtype),
        in_specs=[pl.BlockSpec((rows, 256), lambda i: (0, i))],
        out_specs=pl.BlockSpec((256, rows), lambda i: (i, 0)),
        compiler_params=params(),
        cost_estimate=cost(1 << 26),
        name="turn",
    )(x)


def attend(head, me, q, g, k, v, lse, bias, far_kv, gq_full, ahead, slots):
    rows, width = q.shape
    heads = lse.shape[0]
    tiles = rows // TQ
    spans = far_kv.shape[0]
    far = spans * CAP * KEY_BLOCK

    def now(i):
        return jnp.minimum(i, tiles - 1)

    def then(i):
        return jnp.maximum(i - 1, 0)

    column = pl.BlockSpec((TQ, HEAD_DIM), lambda i: (now(i), head))
    alone = pl.BlockSpec((TQ, HEAD_DIM), lambda i: (now(i), 0))
    late_column = pl.BlockSpec((TQ, HEAD_DIM), lambda i: (then(i), head))
    late = pl.BlockSpec((TQ, HEAD_DIM), lambda i: (then(i), 0))
    in_specs = [
        SMEM,
        column,
        column,
        column,
        column,
        pl.BlockSpec((heads, TQ), lambda i: (0, now(i))),
        pl.BlockSpec((None, spans * CAP, TQ), lambda i: (head, 0, now(i))),
        slotted(spans, 0),
    ]
    args = [me, q, g, k, v, lse, bias, far_kv]
    merge = ahead is not None
    if merge:
        in_specs.append(slotted(spans, 0))
        args.append(ahead)
    aliases = {}
    if gq_full is not None:
        aliases[len(args)] = 0
        in_specs.append(ANY)
        args.append(gq_full)
    return pl.pallas_call(
        functools.partial(
            attend_kernel, head=head, extra=len(aliases), merge=int(merge), tiles=tiles, far=far
        ),
        grid=(tiles + 1,),
        in_specs=in_specs,
        out_specs=[late_column, late, late, alone, slotted(spans, 0)],
        out_shape=[
            jax.ShapeDtypeStruct((rows, width), jnp.bfloat16),
            jax.ShapeDtypeStruct((rows, HEAD_DIM), jnp.bfloat16),
            jax.ShapeDtypeStruct((rows, HEAD_DIM), jnp.float32),
            jax.ShapeDtypeStruct((rows, HEAD_DIM), jnp.float32),
            jax.ShapeDtypeStruct(five(spans, slots), jnp.bfloat16),
        ],
        scratch_shapes=[
            pltpu.VMEM((far, TQ), jnp.float32),
            pltpu.VMEM((far, TQ), jnp.float32),
            pltpu.VMEM((TQ, 128), jnp.float32),
            pltpu.VMEM((TQ, 128), jnp.float32),
            pltpu.VMEM((1, TQ), jnp.float32),
            pltpu.VMEM((far, HEAD_DIM), jnp.float32),
            pltpu.VMEM((far, HEAD_DIM), jnp.float32),
            pltpu.VMEM((HEAD_DIM, far), jnp.bfloat16),
            pltpu.VMEM((TQ, HEAD_DIM), jnp.bfloat16),
            pltpu.VMEM((TQ, HEAD_DIM), jnp.bfloat16),
        ],
        input_output_aliases=aliases,
        cost_estimate=cost(10 * rows * far * HEAD_DIM, 8 << 20),
        compiler_params=params(dimension_semantics=("arbitrary",)),
    )(*args)


def weigh(me, xt, shards, buffer, spans, slot, slots, halves=False):
    cols, rows = xt.shape
    tall = pl.BlockSpec((rows, HEAD_DIM), lambda i: (0, 0))
    in_specs = [SMEM, VMEM] + [tall] * len(shards)
    args = [me, pltpu.with_memory_space_constraint(xt, pltpu.VMEM), *shards]
    aliases = {}
    if buffer is not None:
        aliases[len(args)] = 0
        in_specs.append(ANY)
        args.append(buffer)
    owned = cols // spans
    per = WEIGH_ROWS // owned
    if halves:
        shape = (spans, len(shards) // 2, owned, HEAD_DIM)
        out_spec = pl.BlockSpec((per,) + shape[1:], lambda i: (i, 0, 0, 0))
        out_specs = [out_spec] * 2
        out_shape = [jax.ShapeDtypeStruct(shape, jnp.bfloat16)] * 2
    else:
        out_specs = pl.BlockSpec(
            (per, None, len(shards), owned, HEAD_DIM), lambda i: (i, slot, 0, 0, 0)
        )
        out_shape = jax.ShapeDtypeStruct(five(spans, slots), jnp.bfloat16)
    return pl.pallas_call(
        functools.partial(
            weight_kernel, shards=len(shards), steps=cols // WEIGH_ROWS, halves=halves
        ),
        grid=(cols // WEIGH_ROWS,),
        in_specs=in_specs,
        out_specs=out_specs,
        out_shape=out_shape,
        input_output_aliases=aliases,
        compiler_params=params(),
        cost_estimate=cost(2 * cols * rows * len(shards) * HEAD_DIM, 8 << 20),
        name="weigh",
    )(*args)


def join(keep, got, buffer, slot, slots):
    spans = keep.shape[0]
    whole = pl.BlockSpec(keep.shape, lambda i: (0, 0, 0, 0))
    args, in_specs, aliases = [keep, got], [whole, whole], {}
    if buffer is not None:
        aliases = {2: 0}
        args.append(buffer)
        in_specs.append(ANY)
    return pl.pallas_call(
        join_kernel,
        grid=(1,),
        in_specs=in_specs,
        out_specs=pl.BlockSpec(
            (spans, None) + keep.shape[1:], lambda i: (0, slot, 0, 0, 0)
        ),
        out_shape=jax.ShapeDtypeStruct((spans, slots) + keep.shape[1:], jnp.bfloat16),
        input_output_aliases=aliases,
        compiler_params=params(),
        cost_estimate=cost(1 << 24),
        name="join",
    )(*args)


def total(place, got, slot, head, heads, order):
    return pl.pallas_call(
        functools.partial(total_kernel, head=head, heads=heads, order=order),
        grid=(1,),
        in_specs=[SMEM, slotted(got.shape[0], slot)],
        out_specs=VMEM,
        out_shape=jax.ShapeDtypeStruct(
            (KEY_BLOCK, len(order) * heads * HEAD_DIM), jnp.float32
        ),
        compiler_params=params(),
        cost_estimate=cost(1 << 24),
        name="total",
    )(place, got)


def pair_total(place, got, buffer, first, heads, order):
    spans, count = got.shape[:2]
    specs = [
        pl.BlockSpec((spans, None) + got.shape[2:], lambda i, n=n: (0, n, 0, 0, 0))
        for n in range(count)
    ]
    return pl.pallas_call(
        functools.partial(pair_total_kernel, first=first, heads=heads, order=order),
        grid=(1,),
        in_specs=[SMEM, *specs, VMEM],
        out_specs=VMEM,
        out_shape=jax.ShapeDtypeStruct(buffer.shape, buffer.dtype),
        input_output_aliases={1 + count: 0},
        compiler_params=params(),
        cost_estimate=cost(1 << 24),
        name="pairtotal",
    )(place, *[got] * count, buffer)


def land(head, me, tab, home, dko, dvo, full, rows, width):
    spans = home.shape[0]
    column = pl.BlockSpec((rows, HEAD_DIM), lambda i: (0, head))
    alone = pl.BlockSpec((rows, HEAD_DIM), lambda i: (0, 0))
    in_specs = [SMEM, SMEM, slotted(spans, 0), alone, alone]
    args = [me, tab, home, dko, dvo]
    aliases = {}
    if full is not None:
        in_specs += [ANY, ANY]
        args += list(full)
        aliases = {5: 0, 6: 1}
    return pl.pallas_call(
        functools.partial(land_kernel, head=head, spans=spans),
        grid=(1,),
        in_specs=in_specs,
        out_specs=[column, column],
        out_shape=[jax.ShapeDtypeStruct((rows, width), jnp.float32)] * 2,
        input_output_aliases=aliases,
        compiler_params=params(),
        cost_estimate=cost(1 << 24),
    )(*args)


def exchange(x):
    return lax.all_to_all(x, "kv", split_axis=0, concat_axis=0, tiled=True)


def shift(x, by, tp):
    return lax.ppermute(x, "tp", [(i, (i + by) % tp) for i in range(tp)])


def program(query_rows, key_rows, value_rows, log_sums, cotangent, layer_input, chosen):
    spans = lax.axis_size("kv")
    tp = lax.axis_size("tp")
    heads = log_sums.shape[0]
    rows, width = query_rows.shape
    blocks = rows // KEY_BLOCK
    me = lax.axis_index("kv").astype(jnp.int32).reshape(1)
    place = lax.axis_index("tp").astype(jnp.int32).reshape(1)
    ids = jnp.transpose(chosen, (0, 2, 1))
    key_blocks = key_rows.reshape(blocks, KEY_BLOCK, width)
    value_blocks = value_rows.reshape(blocks, KEY_BLOCK, width)
    order = (0, 1, 3, 2)

    send0, tab = pack_first(me, ids, key_blocks, value_blocks, heads, spans)
    far0 = exchange(send0)
    send1, send2 = pack_rest(tab, key_blocks, value_blocks, heads, spans)
    xt = turn(layer_input)
    bias = mask(me, ids, spans, blocks)

    def attention(h, far, gq_full, ahead, slots):
        return attend(
            h, me, query_rows, cotangent, key_rows, value_rows, log_sums, bias, far,
            gq_full, ahead, slots,
        )

    def gathered(gq):
        right = shift(gq, -1, tp)
        left = shift(gq, 1, tp)
        across = shift(gq, 2, tp)
        return gq, right, left, across

    def swapped(x):
        return lax.ppermute(x, "kv", [(i, i ^ 1) for i in range(spans)])

    far1 = exchange(send1)
    gq_full, gq, *own0, out = attention(0, far0, None, send2, 1)
    shards0 = gathered(gq)
    far2 = exchange(out)
    gq_full, gq, *own1, out = attention(1, far1, gq_full, None, 2)
    shards1 = gathered(gq)
    out = weigh(me, xt, shards0, out, spans, 1, 2)
    home1 = exchange(out)
    gq_full, gq, *own2, out = attention(2, far2, gq_full, None, 1)
    shards2 = gathered(gq)
    home2 = exchange(out)
    joined = None
    for h, shards in ((1, shards1), (2, shards2)):
        keep, give = weigh(me, xt, shards, None, spans, 0, 1, halves=True)
        got = swapped(give)
        joined = join(keep, got, joined, h - 1, heads - 1)
    last = exchange(joined)

    full = None
    for h, (home, own) in enumerate(((far2, own0), (home1, own1), (home2, own2))):
        full = land(h, me, tab, home, *own, full, rows, width)
    grad_weight = total(place, home1, 1, 0, heads, order)
    grad_weight = pair_total(place, last, grad_weight, 1, heads, order)
    return gq_full, full[0], full[1], grad_weight


def solution(mesh):
    placed = (
        P("kv", "tp"),
        P("kv", "tp"),
        P("kv", "tp"),
        P("tp", "kv"),
        P("kv", "tp"),
        P("kv", "tp"),
        P("tp", None, None),
    )
    return jax.shard_map(
        program,
        mesh=mesh,
        in_specs=placed,
        out_specs=(P("kv", "tp"), P("kv", "tp"), P("kv", "tp"), P(("tp", "kv"), None)),
        check_vma=False,
    )
```

```python
import functools

import jax
import jax.numpy as jnp
from jax import lax
from jax.experimental import pallas as pl
from jax.experimental.pallas import tpu as pltpu
from jax.sharding import PartitionSpec as P


HEAD_DIM = 128
KEY_BLOCK = 32
CAP = 2
BIG = 1 << 20
LOG2E = 1.4426950408889634
NEG = -1.0e30
TQ = 512
VMEM_LIMIT = 60960 * 1024
WEIGH_ROWS = 512
KB = 256


def spread(column):
    wide = jnp.broadcast_to(column.astype(jnp.float32), (column.shape[0], 128))
    wide = jnp.concatenate([wide, jnp.zeros((128 - column.shape[0], 128), jnp.float32)], axis=0)
    return wide.T[0:1, :].astype(jnp.int32)


def copy_blocks(tab_s, k_ref, v_ref, send, h, half, lanes):
    def fill(m, carry):
        for odd in range(2):
            for c in range(CAP):
                b = tab_s[2 * c + odd, h * half + m]
                send[2 * m + odd, c] = k_ref[b, :, lanes]
                send[2 * m + odd, CAP + c] = v_ref[b, :, lanes]
        return carry

    lax.fori_loop(0, half, fill, 0, unroll=2)


def first_kernel(me_ref, chosen_ref, k_ref, v_ref, send, tab_ref, lo_s, hi_s, tab_v, tab_s, sem,
                 *, heads, spans, blocks):
    me = me_ref[0]
    half = spans // 2
    for h in range(heads):
        ids = chosen_ref[h]
        mine = (ids >> 6) == me
        lo = jnp.min(jnp.where(mine, ids, BIG), axis=0, keepdims=True)
        hi = jnp.max(jnp.where(mine, ids, -1), axis=0, keepdims=True)
        for m in range(half):
            lo_s[h * half + m : h * half + m + 1, :] = lo[:, m * 128 : (m + 1) * 128]
            hi_s[h * half + m : h * half + m + 1, :] = hi[:, m * 128 : (m + 1) * 128]
    lane = lax.broadcasted_iota(jnp.int32, (heads * half, 128), 1)
    tab_v[...] = jnp.zeros((8, 128), jnp.int32)
    for odd in range(2):
        ours = (lane // blocks) == odd
        lo = spread(jnp.min(jnp.where(ours, lo_s[...], BIG), axis=1, keepdims=True))
        hi = spread(jnp.max(jnp.where(ours, hi_s[...], -1), axis=1, keepdims=True))
        tab_v[odd : odd + 1, :] = lo & (blocks - 1)
        tab_v[2 + odd : 3 + odd, :] = jnp.maximum(hi, 0) & (blocks - 1)
        tab_v[4 + odd : 5 + odd, :] = (hi >= 0).astype(jnp.int32)
        tab_v[6 + odd : 7 + odd, :] = (hi > lo).astype(jnp.int32)
    tab_ref[...] = tab_v[...]
    copy = pltpu.make_async_copy(tab_v, tab_s, sem)
    copy.start()
    copy.wait()
    copy_blocks(tab_s, k_ref, v_ref, send, 0, half, slice(0, HEAD_DIM))


def pack_kernel(tab_ref, k_ref, v_ref, *sends, spans):
    for n, send in enumerate(sends):
        h = n + 1
        lanes = slice(h * HEAD_DIM, (h + 1) * HEAD_DIM)
        copy_blocks(tab_ref, k_ref, v_ref, send, h, spans // 2, lanes)


def mask_kernel(me_ref, chosen_ref, bias_ref, *, heads, spans, blocks, picks):
    me = me_ref[0]
    slots = spans * CAP
    slot = lax.broadcasted_iota(jnp.int32, (slots, 128), 0)
    lane = lax.broadcasted_iota(jnp.int32, (slots, 128), 1)
    ours = (lane // blocks) == (me % 2)
    place = lax.broadcasted_iota(jnp.int32, (128, blocks * KEY_BLOCK), 1) // KEY_BLOCK
    row = lax.broadcasted_iota(jnp.int32, (128, blocks * KEY_BLOCK), 0)
    expand = ((place + (me % 2) * blocks) == row).astype(jnp.bfloat16)
    start = pl.multiple_of((me // 2) * 128, 128)
    for h in range(heads):
        ids = chosen_ref[h, :, pl.ds(start, 128)]
        cols = [jnp.broadcast_to(ids[c : c + 1, :], (slots, 128)) for c in range(picks)]
        least = jnp.full((slots, 128), BIG, jnp.int32)
        most = jnp.full((slots, 128), -1, jnp.int32)
        for col in cols:
            hit = ((col >> 6) == (slot >> 1)) & ours
            least = jnp.minimum(least, jnp.where(hit, col, BIG))
            most = jnp.maximum(most, jnp.where(hit, col, -1))
        least = jnp.min(least, axis=1, keepdims=True)
        most = jnp.max(most, axis=1, keepdims=True)
        name = jnp.where(
            (slot & 1) == 0, least, jnp.where(most > least, most, -7)
        )
        named = cols[0] == name
        for col in cols[1:]:
            named = named | (col == name)
        hot = jnp.where(named, 1.0, 0.0).astype(jnp.bfloat16)
        full = jnp.dot(hot, expand, preferred_element_type=jnp.float32)
        bias_ref[h] = jnp.where(full > 0.5, 0.0, NEG)


def turn_kernel(x_ref, out_ref):
    rows = x_ref.shape[0]
    for i in range(rows // 256):
        cut = slice(i * 256, (i + 1) * 256)
        out_ref[:, cut] = x_ref[cut, :].T


def weight_kernel(me_ref, xt_ref, *rest, shards, steps, halves):
    span = xt_ref.shape[0] // steps
    xt = xt_ref[pl.ds(pl.multiple_of(pl.program_id(0) * span, span), span), :]
    core = me_ref[0] % 2
    shape = (span // KEY_BLOCK, KEY_BLOCK, HEAD_DIM)
    sums = []
    for at in range(0, shards, 2):
        g = jnp.concatenate([rest[at][...], rest[at + 1][...]], axis=1)
        got = jnp.dot(xt, g, preferred_element_type=jnp.float32).astype(jnp.bfloat16)
        sums += [got[:, :HEAD_DIM].reshape(shape), got[:, HEAD_DIM:].reshape(shape)]
    if halves:
        keep_ref, give_ref = rest[-2:]
        for p in range(2):
            keep_ref[:, p] = jnp.where(core == 0, sums[p], sums[2 + p])
            give_ref[:, p] = jnp.where(core == 0, sums[2 + p], sums[p])
    else:
        for p in range(shards):
            rest[-1][:, p] = sums[p]


def join_kernel(keep_ref, got_ref, *rest):
    out_ref = rest[-1]
    both = keep_ref[...].astype(jnp.float32) + got_ref[...].astype(jnp.float32)
    out_ref[...] = both.astype(jnp.bfloat16)


def put_sum(out_ref, got_ref, sources, column, first):
    acc = got_ref[sources[0], column].astype(jnp.float32)
    for i in sources[1:]:
        acc = acc + got_ref[i, column].astype(jnp.float32)
    out_ref[:, pl.ds(pl.multiple_of(first, HEAD_DIM), HEAD_DIM)] = acc


def total_kernel(at_ref, got_ref, out_ref, *, head, heads, order):
    tp = len(order)
    out_ref[...] = jnp.zeros_like(out_ref)
    for p in range(tp):
        place = (at_ref[0] + order[p]) % tp
        sources = range(got_ref.shape[0])
        put_sum(out_ref, got_ref, sources, p, (place * heads + head) * HEAD_DIM)


def pair_total_kernel(at_ref, got_ref, before_ref, out_ref, *, head, heads, order):
    tp = len(order)
    out_ref[...] = before_ref[...]
    for p in range(tp):
        place = (at_ref[0] + order[p]) % tp
        sources = range(p // 2, got_ref.shape[0], 2)
        put_sum(out_ref, got_ref, sources, p % 2, (place * heads + head) * HEAD_DIM)


def attend_kernel(me_ref, *refs, head, extra, merge, tiles, far):
    q_ref, g_ref, ko_ref, vo_ref, lse_ref, bias_ref, kv_ref = refs[:7]
    ahead_ref = refs[7] if merge else None
    rest = refs[7 + merge + extra :]
    gqf_ref, gq_ref, dko_ref, dvo_ref, back_ref = rest[:5]
    p_s, dp_s, po_s, dpo_s, dots_s, dk_s, dv_s, kt_s, qq_s, kk_s = rest[5:]
    step = pl.program_id(0)
    scale = HEAD_DIM**-0.5
    nkb = far // KB
    per = KB // (CAP * KEY_BLOCK)
    parts = TQ // 128
    nt = (((1,), (1,)), ((), ()))

    def cut(t):
        return slice(t * 128, (t + 1) * 128)

    def ahead(first, behind):
        q = q_ref[...]
        g = g_ref[...]
        lse = lse_ref[head : head + 1, :] * LOG2E
        key_at = lax.broadcasted_iota(jnp.int32, (128, 128), 0)
        row_at = lax.broadcasted_iota(jnp.int32, (128, 128), 1)
        near = (key_at // KEY_BLOCK == row_at // KEY_BLOCK) & (key_at <= row_at)
        dots = jnp.zeros((8, TQ), jnp.float32)
        own_dots = []
        for i in range(nkb):
            rows = slice(i * KB, (i + 1) * KB)
            if behind is not None:
                behind(i)
            keys = kv_ref[i * per : (i + 1) * per, 0:CAP].reshape(KB, HEAD_DIM)
            values = kv_ref[i * per : (i + 1) * per, CAP : 2 * CAP].reshape(KB, HEAD_DIM)
            s = lax.dot_general(keys, q, nt, preferred_element_type=jnp.float32)
            dp = lax.dot_general(values, g, nt, preferred_element_type=jnp.float32)
            shift = bias_ref[i * per * CAP : (i + 1) * per * CAP, :] - lse
            s = (s * (scale * LOG2E)).reshape(per * CAP, KEY_BLOCK, TQ) + shift[:, None, :]
            p = jnp.exp2(s).reshape(KB, TQ)
            p_s[rows, :] = p
            dp_s[rows, :] = dp
            dv = jnp.dot(p.astype(jnp.bfloat16), g, preferred_element_type=jnp.float32)
            dv_s[rows, :] = dv if first else dv_s[rows, :] + dv
            dots = dots + (p * dp).reshape(KB // 8, 8, TQ).sum(axis=0)
            if i < parts:
                c = cut(i)
                s = lax.dot_general(ko_ref[c, :], q[c], nt, preferred_element_type=jnp.float32)
                dp = lax.dot_general(vo_ref[c, :], g[c], nt, preferred_element_type=jnp.float32)
                p = jnp.exp2(jnp.where(near, s * (scale * LOG2E) - lse[:, c], NEG))
                po_s[c, :] = p
                dpo_s[c, :] = dp
                own_dots.append(jnp.sum(p * dp, axis=0, keepdims=True))
                dvo_ref[c, :] = jnp.dot(
                    p.astype(jnp.bfloat16), g[c], preferred_element_type=jnp.float32
                )
        return jnp.sum(dots, axis=0, keepdims=True) + jnp.concatenate(own_dots, axis=1)

    def second_half(first):
        q = qq_s[...]
        dots = dots_s[...]
        held = []
        own = []

        def behind(i):
            rows = slice(i * KB, (i + 1) * KB)
            ds = (p_s[rows, :] * (dp_s[rows, :] - dots)).astype(jnp.bfloat16)
            dk = jnp.dot(ds, q, preferred_element_type=jnp.float32)
            dk_s[rows, :] = dk if first else dk_s[rows, :] + dk
            part = jnp.dot(kt_s[:, rows], ds, preferred_element_type=jnp.float32)
            held[:] = [held[0] + part] if held else [part]
            if i < parts:
                c = cut(i)
                ds = (po_s[c, :] * (dpo_s[c, :] - dots[:, c])).astype(jnp.bfloat16)
                dko_ref[c, :] = scale * jnp.dot(ds, q[c], preferred_element_type=jnp.float32)
                own.append(jnp.dot(kk_s[c, :].T, ds, preferred_element_type=jnp.float32))

        def finish():
            for t in range(parts):
                out = (scale * (held[0][:, cut(t)] + own[t])).T.astype(jnp.bfloat16)
                gq_ref[cut(t), :] = out
                gqf_ref[cut(t), :] = out

        return behind, finish

    def keep(dots):
        dots_s[...] = dots
        qq_s[...] = q_ref[...]
        kk_s[...] = ko_ref[...]

    @pl.when(step == 0)
    def _():
        for i in range(nkb):
            keys = kv_ref[i * per : (i + 1) * per, 0:CAP].reshape(KB, HEAD_DIM)
            kt_s[:, i * KB : (i + 1) * KB] = keys.T
        keep(ahead(True, None))
        dk_s[...] = jnp.zeros_like(dk_s)

    @pl.when((step > 0) & (step < tiles))
    def _():
        behind, finish = second_half(False)
        dots = ahead(False, behind)
        finish()
        keep(dots)

    @pl.when(step == tiles)
    def _():
        behind, finish = second_half(False)
        for i in range(nkb):
            behind(i)
        finish()
        shape = (far // (CAP * KEY_BLOCK), CAP, KEY_BLOCK, HEAD_DIM)
        dk = (scale * dk_s[...]).astype(jnp.bfloat16).reshape(shape)
        dv = dv_s[...].astype(jnp.bfloat16).reshape(shape)
        if merge:
            me = me_ref[0]
            for n in range(shape[0]):

                @pl.when(n < me)
                def _(n=n):
                    back_ref[n, 0:CAP] = dk[n]
                    back_ref[n, CAP : 2 * CAP] = dv[n]

                @pl.when(n >= me)
                def _(n=n):
                    back_ref[n] = ahead_ref[n]
        else:
            back_ref[:, 0:CAP] = dk
            back_ref[:, CAP : 2 * CAP] = dv


def land_kernel(me_ref, tab_ref, back_ref, dko_ref, dvo_ref, *rest, head, spans):
    gk_ref, gv_ref = rest[-2:]
    gk_ref[...] = dko_ref[...]
    gv_ref[...] = dvo_ref[...]
    me = me_ref[0]
    half = spans // 2

    def one(n, carry):
        at = head * half + n // 2
        odd = n % 2
        for c in range(CAP):

            @pl.when(tab_ref[4 + 2 * c + odd, at] > 0)
            def _(c=c):
                first = tab_ref[2 * c + odd, at] * KEY_BLOCK
                rows = pl.ds(pl.multiple_of(first, KEY_BLOCK), KEY_BLOCK)
                gk_ref[rows, :] += back_ref[n, c].astype(jnp.float32)
                gv_ref[rows, :] += back_ref[n, CAP + c].astype(jnp.float32)

        return carry

    lax.fori_loop(me + 1, spans, one, 0)


SMEM = pl.BlockSpec(memory_space=pltpu.SMEM)
VMEM = pl.BlockSpec(memory_space=pltpu.VMEM)
ANY = pl.BlockSpec(memory_space=pl.ANY)


def params(**more):
    return pltpu.CompilerParams(vmem_limit_bytes=VMEM_LIMIT, **more)


def cost(flops, data=1 << 20):
    return pl.CostEstimate(flops=flops, transcendentals=0, bytes_accessed=data)


def five(spans, slots=1):
    return (spans, slots, 2 * CAP, KEY_BLOCK, HEAD_DIM)


def slotted(spans, slot):
    return pl.BlockSpec(
        (spans, None, 2 * CAP, KEY_BLOCK, HEAD_DIM), lambda i: (0, slot, 0, 0, 0)
    )


def back_spec(spans, shape):
    return slotted(spans, 0) if len(shape) == 5 else tiles_of(spans, 2 * CAP, 0)


def pack_first(me, ids, key_blocks, value_blocks, heads, spans):
    blocks = key_blocks.shape[0]
    column = pl.BlockSpec((blocks, KEY_BLOCK, HEAD_DIM), lambda i: (0, 0, 0))
    return pl.pallas_call(
        functools.partial(first_kernel, heads=heads, spans=spans, blocks=blocks),
        grid=(1,),
        out_shape=[
            jax.ShapeDtypeStruct(five(spans), jnp.bfloat16),
            jax.ShapeDtypeStruct((8, 128), jnp.int32),
        ],
        in_specs=[SMEM, VMEM, column, column],
        out_specs=[slotted(spans, 0), VMEM],
        scratch_shapes=[
            pltpu.VMEM((heads * spans // 2, 128), jnp.int32),
            pltpu.VMEM((heads * spans // 2, 128), jnp.int32),
            pltpu.VMEM((8, 128), jnp.int32),
            pltpu.SMEM((8, 128), jnp.int32),
            pltpu.SemaphoreType.DMA,
        ],
        compiler_params=params(),
        cost_estimate=cost(1 << 26),
        name="first",
    )(me, ids, key_blocks, value_blocks)


def pack_rest(tab, key_blocks, value_blocks, heads, spans):
    return pl.pallas_call(
        functools.partial(pack_kernel, spans=spans),
        grid=(1,),
        out_shape=[jax.ShapeDtypeStruct(five(spans), jnp.bfloat16)] * (heads - 1),
        in_specs=[SMEM, VMEM, VMEM],
        out_specs=[slotted(spans, 0)] * (heads - 1),
        compiler_params=params(),
        cost_estimate=cost(1 << 26),
        name="pack",
    )(tab, key_blocks, value_blocks)


def mask(me, ids, spans, blocks):
    heads, picks, _ = ids.shape
    return pl.pallas_call(
        functools.partial(mask_kernel, heads=heads, spans=spans, blocks=blocks, picks=picks),
        out_shape=jax.ShapeDtypeStruct((heads, spans * CAP, blocks * KEY_BLOCK), jnp.float32),
        in_specs=[SMEM, VMEM],
        out_specs=VMEM,
        compiler_params=params(),
        cost_estimate=cost(1 << 26),
        name="mask",
    )(me, ids)


def turn(x):
    rows, cols = x.shape
    return pl.pallas_call(
        turn_kernel,
        grid=(cols // 256,),
        out_shape=pltpu.VMEM((cols, rows), x.dtype),
        in_specs=[pl.BlockSpec((rows, 256), lambda i: (0, i))],
        out_specs=pl.BlockSpec((256, rows), lambda i: (i, 0)),
        compiler_params=params(),
        cost_estimate=cost(1 << 26),
        name="turn",
    )(x)


def attend(head, me, q, g, k, v, lse, bias, far_kv, gq_full, ahead, back_shape):
    rows, width = q.shape
    heads = lse.shape[0]
    tiles = rows // TQ
    spans = far_kv.shape[0]
    far = spans * CAP * KEY_BLOCK

    def now(i):
        return jnp.minimum(i, tiles - 1)

    def then(i):
        return jnp.maximum(i - 1, 0)

    column = pl.BlockSpec((TQ, HEAD_DIM), lambda i: (now(i), head))
    alone = pl.BlockSpec((TQ, HEAD_DIM), lambda i: (now(i), 0))
    late_column = pl.BlockSpec((TQ, HEAD_DIM), lambda i: (then(i), head))
    late = pl.BlockSpec((TQ, HEAD_DIM), lambda i: (then(i), 0))
    in_specs = [
        SMEM,
        column,
        column,
        column,
        column,
        pl.BlockSpec((heads, TQ), lambda i: (0, now(i))),
        pl.BlockSpec((None, spans * CAP, TQ), lambda i: (head, 0, now(i))),
        slotted(spans, 0),
    ]
    args = [me, q, g, k, v, lse, bias, far_kv]
    merge = ahead is not None
    if merge:
        in_specs.append(slotted(spans, 0))
        args.append(ahead)
    aliases = {}
    if gq_full is not None:
        aliases[len(args)] = 0
        in_specs.append(ANY)
        args.append(gq_full)
    return pl.pallas_call(
        functools.partial(
            attend_kernel, head=head, extra=len(aliases), merge=int(merge), tiles=tiles, far=far
        ),
        grid=(tiles + 1,),
        in_specs=in_specs,
        out_specs=[late_column, late, late, alone, back_spec(spans, back_shape)],
        out_shape=[
            jax.ShapeDtypeStruct((rows, width), jnp.bfloat16),
            jax.ShapeDtypeStruct((rows, HEAD_DIM), jnp.bfloat16),
            jax.ShapeDtypeStruct((rows, HEAD_DIM), jnp.float32),
            jax.ShapeDtypeStruct((rows, HEAD_DIM), jnp.float32),
            jax.ShapeDtypeStruct(back_shape, jnp.bfloat16),
        ],
        scratch_shapes=[
            pltpu.VMEM((far, TQ), jnp.float32),
            pltpu.VMEM((far, TQ), jnp.float32),
            pltpu.VMEM((TQ, 128), jnp.float32),
            pltpu.VMEM((TQ, 128), jnp.float32),
            pltpu.VMEM((1, TQ), jnp.float32),
            pltpu.VMEM((far, HEAD_DIM), jnp.float32),
            pltpu.VMEM((far, HEAD_DIM), jnp.float32),
            pltpu.VMEM((HEAD_DIM, far), jnp.bfloat16),
            pltpu.VMEM((TQ, HEAD_DIM), jnp.bfloat16),
            pltpu.VMEM((TQ, HEAD_DIM), jnp.bfloat16),
        ],
        input_output_aliases=aliases,
        cost_estimate=cost(10 * rows * far * HEAD_DIM, 8 << 20),
        compiler_params=params(dimension_semantics=("arbitrary",)),
    )(*args)


def weigh(me, xt, shards, buffer, spans, slot, slots, halves=False):
    cols, rows = xt.shape
    tall = pl.BlockSpec((rows, HEAD_DIM), lambda i: (0, 0))
    in_specs = [SMEM, VMEM] + [tall] * len(shards)
    args = [me, pltpu.with_memory_space_constraint(xt, pltpu.VMEM), *shards]
    aliases = {}
    if buffer is not None:
        aliases[len(args)] = 0
        in_specs.append(ANY)
        args.append(buffer)
    owned = cols // spans
    per = WEIGH_ROWS // owned
    if halves:
        shape = (spans, len(shards) // 2, owned, HEAD_DIM)
        out_spec = pl.BlockSpec((per,) + shape[1:], lambda i: (i, 0, 0, 0))
        out_specs = [out_spec] * 2
        out_shape = [jax.ShapeDtypeStruct(shape, jnp.bfloat16)] * 2
    else:
        out_specs = pl.BlockSpec(
            (per, None, len(shards), owned, HEAD_DIM), lambda i: (i, slot, 0, 0, 0)
        )
        out_shape = jax.ShapeDtypeStruct(five(spans, slots), jnp.bfloat16)
    return pl.pallas_call(
        functools.partial(
            weight_kernel, shards=len(shards), steps=cols // WEIGH_ROWS, halves=halves
        ),
        grid=(cols // WEIGH_ROWS,),
        in_specs=in_specs,
        out_specs=out_specs,
        out_shape=out_shape,
        input_output_aliases=aliases,
        compiler_params=params(),
        cost_estimate=cost(2 * cols * rows * len(shards) * HEAD_DIM, 8 << 20),
        name="weigh",
    )(*args)


def tiles_of(spans, count, at):
    return pl.BlockSpec((spans, count, KEY_BLOCK, HEAD_DIM), lambda i: (0, at, 0, 0))


def join(keep, got, buffer, at):
    spans, count = keep.shape[:2]
    args, in_specs, aliases = [keep, got], [tiles_of(spans, count, 0)] * 2, {}
    out_shape = jax.ShapeDtypeStruct(keep.shape, keep.dtype)
    if buffer is not None:
        aliases = {2: 0}
        args.append(buffer)
        in_specs.append(ANY)
        out_shape = jax.ShapeDtypeStruct(buffer.shape, buffer.dtype)
    return pl.pallas_call(
        join_kernel,
        grid=(1,),
        in_specs=in_specs,
        out_specs=tiles_of(spans, count, at),
        out_shape=out_shape,
        input_output_aliases=aliases,
        compiler_params=params(),
        cost_estimate=cost(1 << 24),
        name="join",
    )(*args)


def total(place, got, slot, head, heads, order):
    return pl.pallas_call(
        functools.partial(total_kernel, head=head, heads=heads, order=order),
        grid=(1,),
        in_specs=[SMEM, slotted(got.shape[0], slot)],
        out_specs=VMEM,
        out_shape=jax.ShapeDtypeStruct(
            (KEY_BLOCK, len(order) * heads * HEAD_DIM), jnp.float32
        ),
        compiler_params=params(),
        cost_estimate=cost(1 << 24),
        name="total",
    )(place, got)


def pair_total(place, got, at, buffer, head, heads, order):
    return pl.pallas_call(
        functools.partial(pair_total_kernel, head=head, heads=heads, order=order),
        grid=(1,),
        in_specs=[SMEM, tiles_of(got.shape[0], len(order) // 2, at), VMEM],
        out_specs=VMEM,
        out_shape=jax.ShapeDtypeStruct(buffer.shape, buffer.dtype),
        input_output_aliases={2: 0},
        compiler_params=params(),
        cost_estimate=cost(1 << 24),
        name="pairtotal",
    )(place, got, buffer)


def land(head, me, tab, home, dko, dvo, full, rows, width):
    spans = home.shape[0]
    column = pl.BlockSpec((rows, HEAD_DIM), lambda i: (0, head))
    alone = pl.BlockSpec((rows, HEAD_DIM), lambda i: (0, 0))
    in_specs = [SMEM, SMEM, back_spec(spans, home.shape), alone, alone]
    args = [me, tab, home, dko, dvo]
    aliases = {}
    if full is not None:
        in_specs += [ANY, ANY]
        args += list(full)
        aliases = {5: 0, 6: 1}
    return pl.pallas_call(
        functools.partial(land_kernel, head=head, spans=spans),
        grid=(1,),
        in_specs=in_specs,
        out_specs=[column, column],
        out_shape=[jax.ShapeDtypeStruct((rows, width), jnp.float32)] * 2,
        input_output_aliases=aliases,
        compiler_params=params(),
        cost_estimate=cost(1 << 24),
    )(*args)


def exchange(x):
    return lax.all_to_all(x, "kv", split_axis=0, concat_axis=0, tiled=True)


def shift(x, by, tp):
    return lax.ppermute(x, "tp", [(i, (i + by) % tp) for i in range(tp)])


def program(query_rows, key_rows, value_rows, log_sums, cotangent, layer_input, chosen):
    spans = lax.axis_size("kv")
    tp = lax.axis_size("tp")
    heads = log_sums.shape[0]
    rows, width = query_rows.shape
    blocks = rows // KEY_BLOCK
    me = lax.axis_index("kv").astype(jnp.int32).reshape(1)
    place = lax.axis_index("tp").astype(jnp.int32).reshape(1)
    ids = jnp.transpose(chosen, (0, 2, 1))
    key_blocks = key_rows.reshape(blocks, KEY_BLOCK, width)
    value_blocks = value_rows.reshape(blocks, KEY_BLOCK, width)
    order = (0, 1, 3, 2)

    send0, tab = pack_first(me, ids, key_blocks, value_blocks, heads, spans)
    far0 = exchange(send0)
    send1, send2 = pack_rest(tab, key_blocks, value_blocks, heads, spans)
    xt = turn(layer_input)
    bias = mask(me, ids, spans, blocks)

    def attention(h, far, gq_full, ahead, back_shape):
        return attend(
            h, me, query_rows, cotangent, key_rows, value_rows, log_sums, bias, far,
            gq_full, ahead, back_shape,
        )

    def gathered(gq):
        right = shift(gq, -1, tp)
        left = shift(gq, 1, tp)
        across = shift(gq, 2, tp)
        return gq, right, left, across

    def swapped(x):
        return lax.ppermute(x, "kv", [(i, i ^ 1) for i in range(spans)])

    far1 = exchange(send1)
    gq_full, gq, *own0, out = attention(0, far0, None, send2, five(spans))
    shards0 = gathered(gq)
    far2 = exchange(out)
    gq_full, gq, *own1, out = attention(1, far1, gq_full, None, five(spans, 2))
    shards1 = gathered(gq)
    out = weigh(me, xt, shards0, out, spans, 1, 2)
    home1 = exchange(out)
    room = (spans, 2 * CAP + tp // 2, KEY_BLOCK, HEAD_DIM)
    gq_full, gq, *own2, out = attention(2, far2, gq_full, None, room)
    shards2 = gathered(gq)

    def shared(shards, buffer, at):
        keep, give = weigh(me, xt, shards, None, spans, 0, 1, halves=True)
        got = swapped(give)
        return join(keep, got, buffer, at)

    home2 = exchange(shared(shards1, out, 2))
    last = exchange(shared(shards2, None, 0))

    full = None
    for h, (home, own) in enumerate(((far2, own0), (home1, own1), (home2, own2))):
        full = land(h, me, tab, home, *own, full, rows, width)
    grad_weight = total(place, home1, 1, 0, heads, order)
    grad_weight = pair_total(place, home2, 2, grad_weight, 1, heads, order)
    grad_weight = pair_total(place, last, 0, grad_weight, 2, heads, order)
    return gq_full, full[0], full[1], grad_weight


def solution(mesh):
    placed = (
        P("kv", "tp"),
        P("kv", "tp"),
        P("kv", "tp"),
        P("tp", "kv"),
        P("kv", "tp"),
        P("kv", "tp"),
        P("tp", None, None),
    )
    return jax.shard_map(
        program,
        mesh=mesh,
        in_specs=placed,
        out_specs=(P("kv", "tp"), P("kv", "tp"), P("kv", "tp"), P(("tp", "kv"), None)),
        check_vma=False,
    )
```

```python
import functools

import jax
import jax.numpy as jnp
from jax import lax
from jax.experimental import pallas as pl
from jax.experimental.pallas import tpu as pltpu
from jax.sharding import PartitionSpec as P


HEAD_DIM = 128
KEY_BLOCK = 32
CAP = 2
BIG = 1 << 20
LOG2E = 1.4426950408889634
NEG = -1.0e30
TQ = 512
VMEM_LIMIT = 60960 * 1024
WEIGH_ROWS = 512
KB = 256


def spread(column):
    wide = jnp.broadcast_to(column.astype(jnp.float32), (column.shape[0], 128))
    wide = jnp.concatenate([wide, jnp.zeros((128 - column.shape[0], 128), jnp.float32)], axis=0)
    return wide.T[0:1, :].astype(jnp.int32)


def copy_blocks(tab_s, k_ref, v_ref, send, h, half, lanes):
    def fill(m, carry):
        for odd in range(2):
            for c in range(CAP):
                b = tab_s[2 * c + odd, h * half + m]
                send[2 * m + odd, c] = k_ref[b, :, lanes]
                send[2 * m + odd, CAP + c] = v_ref[b, :, lanes]
        return carry

    lax.fori_loop(0, half, fill, 0, unroll=2)


def first_kernel(me_ref, chosen_ref, k_ref, v_ref, send, tab_ref, lo_s, hi_s, tab_v, tab_s, sem,
                 *, heads, spans, blocks):
    me = me_ref[0]
    half = spans // 2
    for h in range(heads):
        ids = chosen_ref[h]
        mine = (ids >> 6) == me
        lo = jnp.min(jnp.where(mine, ids, BIG), axis=0, keepdims=True)
        hi = jnp.max(jnp.where(mine, ids, -1), axis=0, keepdims=True)
        for m in range(half):
            lo_s[h * half + m : h * half + m + 1, :] = lo[:, m * 128 : (m + 1) * 128]
            hi_s[h * half + m : h * half + m + 1, :] = hi[:, m * 128 : (m + 1) * 128]
    lane = lax.broadcasted_iota(jnp.int32, (heads * half, 128), 1)
    tab_v[...] = jnp.zeros((8, 128), jnp.int32)
    for odd in range(2):
        ours = (lane // blocks) == odd
        lo = spread(jnp.min(jnp.where(ours, lo_s[...], BIG), axis=1, keepdims=True))
        hi = spread(jnp.max(jnp.where(ours, hi_s[...], -1), axis=1, keepdims=True))
        tab_v[odd : odd + 1, :] = lo & (blocks - 1)
        tab_v[2 + odd : 3 + odd, :] = jnp.maximum(hi, 0) & (blocks - 1)
        tab_v[4 + odd : 5 + odd, :] = (hi >= 0).astype(jnp.int32)
        tab_v[6 + odd : 7 + odd, :] = (hi > lo).astype(jnp.int32)
    tab_ref[...] = tab_v[...]
    copy = pltpu.make_async_copy(tab_v, tab_s, sem)
    copy.start()
    copy.wait()
    copy_blocks(tab_s, k_ref, v_ref, send, 0, half, slice(0, HEAD_DIM))


def pack_kernel(tab_ref, k_ref, v_ref, *sends, spans):
    for n, send in enumerate(sends):
        h = n + 1
        lanes = slice(h * HEAD_DIM, (h + 1) * HEAD_DIM)
        copy_blocks(tab_ref, k_ref, v_ref, send, h, spans // 2, lanes)


def mask_kernel(me_ref, chosen_ref, bias_ref, *, heads, spans, blocks, picks):
    me = me_ref[0]
    slots = spans * CAP
    slot = lax.broadcasted_iota(jnp.int32, (slots, 128), 0)
    lane = lax.broadcasted_iota(jnp.int32, (slots, 128), 1)
    ours = (lane // blocks) == (me % 2)
    place = lax.broadcasted_iota(jnp.int32, (128, blocks * KEY_BLOCK), 1) // KEY_BLOCK
    row = lax.broadcasted_iota(jnp.int32, (128, blocks * KEY_BLOCK), 0)
    expand = ((place + (me % 2) * blocks) == row).astype(jnp.bfloat16)
    start = pl.multiple_of((me // 2) * 128, 128)
    for h in range(heads):
        ids = chosen_ref[h, :, pl.ds(start, 128)]
        cols = [jnp.broadcast_to(ids[c : c + 1, :], (slots, 128)) for c in range(picks)]
        least = jnp.full((slots, 128), BIG, jnp.int32)
        most = jnp.full((slots, 128), -1, jnp.int32)
        for col in cols:
            hit = ((col >> 6) == (slot >> 1)) & ours
            least = jnp.minimum(least, jnp.where(hit, col, BIG))
            most = jnp.maximum(most, jnp.where(hit, col, -1))
        least = jnp.min(least, axis=1, keepdims=True)
        most = jnp.max(most, axis=1, keepdims=True)
        name = jnp.where(
            (slot & 1) == 0, least, jnp.where(most > least, most, -7)
        )
        named = cols[0] == name
        for col in cols[1:]:
            named = named | (col == name)
        hot = jnp.where(named, 1.0, 0.0).astype(jnp.bfloat16)
        full = jnp.dot(hot, expand, preferred_element_type=jnp.float32)
        bias_ref[h] = jnp.where(full > 0.5, 0.0, NEG)


def turn_kernel(x_ref, out_ref):
    rows = x_ref.shape[0]
    for i in range(rows // 256):
        cut = slice(i * 256, (i + 1) * 256)
        out_ref[:, cut] = x_ref[cut, :].T


def weight_kernel(me_ref, xt_ref, *rest, extra, slot, halves):
    shards = rest[:4]
    outs = rest[4 + extra : -4]
    g_s, o_s, in_sem, out_sem = rest[-4:]
    copies = []
    for n, shard in enumerate(shards):
        lanes = pl.ds((n % 2) * HEAD_DIM, HEAD_DIM)
        copy = pltpu.make_async_copy(shard, g_s.at[n // 2, :, lanes], in_sem.at[n])
        copy.start()
        copies.append(copy)
    rows = xt_ref.shape[0]
    shape = (WEIGH_ROWS // KEY_BLOCK, KEY_BLOCK, HEAD_DIM)
    ends = []
    for pair in range(2):
        copies[2 * pair].wait()
        copies[2 * pair + 1].wait()
        g = g_s[pair]

        def some(b, carry, pair=pair, g=g):
            first = pl.multiple_of(b * WEIGH_ROWS, WEIGH_ROWS)
            xt = xt_ref[pl.ds(first, WEIGH_ROWS), :]
            got = jnp.dot(xt, g, preferred_element_type=jnp.float32).astype(jnp.bfloat16)
            owners = pl.ds(b * shape[0], shape[0])
            o_s[pair, owners, 0] = got[:, :HEAD_DIM].reshape(shape)
            o_s[pair, owners, 1] = got[:, HEAD_DIM:].reshape(shape)
            return carry

        lax.fori_loop(0, rows // WEIGH_ROWS, some, 0)
        if halves:
            core = me_ref[0] % 2
            for out, mine in ((outs[0], core == pair), (outs[1], core != pair)):
                copy = pltpu.make_async_copy(o_s.at[pair], out, out_sem.at[pair])
                pl.when(mine)(copy.start)
                ends.append((copy, mine))
        else:
            target = outs[0].at[:, slot, pl.ds(2 * pair, 2)]
            copy = pltpu.make_async_copy(o_s.at[pair], target, out_sem.at[pair])
            copy.start()
            ends.append((copy, None))
    for copy, mine in ends:
        if mine is None:
            copy.wait()
        else:
            pl.when(mine)(copy.wait)


def join_kernel(keep_ref, got_ref, *rest, at):
    out_ref, keep_s, got_s, sem = rest[-4:]
    one = pltpu.make_async_copy(keep_ref, keep_s, sem.at[0])
    two = pltpu.make_async_copy(got_ref, got_s, sem.at[1])
    one.start()
    two.start()
    one.wait()
    two.wait()
    both = keep_s[...].astype(jnp.float32) + got_s[...].astype(jnp.float32)
    got_s[...] = both.astype(jnp.bfloat16)
    count = keep_ref.shape[1]
    back = pltpu.make_async_copy(got_s, out_ref.at[:, pl.ds(at * count, count)], sem.at[2])
    back.start()
    back.wait()


def put_sum(out_ref, got_ref, sources, column, first):
    acc = got_ref[sources[0], column].astype(jnp.float32)
    for i in sources[1:]:
        acc = acc + got_ref[i, column].astype(jnp.float32)
    out_ref[:, pl.ds(pl.multiple_of(first, HEAD_DIM), HEAD_DIM)] = acc


def total_kernel(at_ref, got_ref, out_ref, *, head, heads, order):
    tp = len(order)
    out_ref[...] = jnp.zeros_like(out_ref)
    for p in range(tp):
        place = (at_ref[0] + order[p]) % tp
        sources = range(got_ref.shape[0])
        put_sum(out_ref, got_ref, sources, p, (place * heads + head) * HEAD_DIM)


def pair_total_kernel(at_ref, got_ref, before_ref, out_ref, got_s, sum_s, got_sem, sem,
                      *, at, head, heads, order):
    tp = len(order)
    got = pltpu.make_async_copy(got_ref.at[:, pl.ds(at * tp // 2, tp // 2)], got_s, got_sem)
    got.start()
    got.wait()
    copies = []
    for p in range(tp):
        place = (at_ref[0] + order[p]) % tp
        acc = got_s[p // 2, p % 2].astype(jnp.float32)
        for i in range(p // 2 + 2, got_s.shape[0], 2):
            acc = acc + got_s[i, p % 2].astype(jnp.float32)
        sum_s[p] = acc
        first = pl.multiple_of((place * heads + head) * HEAD_DIM, HEAD_DIM)
        copy = pltpu.make_async_copy(
            sum_s.at[p], out_ref.at[:, pl.ds(first, HEAD_DIM)], sem.at[p]
        )
        copy.start()
        copies.append(copy)
    for copy in copies:
        copy.wait()


def attend_kernel(me_ref, *refs, head, extra, merge, tiles, far):
    q_ref, g_ref, ko_ref, vo_ref, lse_ref, bias_ref, kv_ref = refs[:7]
    ahead_ref = refs[7] if merge else None
    rest = refs[7 + merge + extra :]
    gqf_ref, gq_ref, dko_ref, dvo_ref, back_ref = rest[:5]
    p_s, dp_s, po_s, dpo_s, dots_s, dk_s, dv_s, kt_s, qq_s, kk_s = rest[5:]
    step = pl.program_id(0)
    scale = HEAD_DIM**-0.5
    nkb = far // KB
    per = KB // (CAP * KEY_BLOCK)
    parts = TQ // 128
    nt = (((1,), (1,)), ((), ()))

    def cut(t):
        return slice(t * 128, (t + 1) * 128)

    def ahead(first, behind):
        q = q_ref[...]
        g = g_ref[...]
        lse = lse_ref[head : head + 1, :] * LOG2E
        key_at = lax.broadcasted_iota(jnp.int32, (128, 128), 0)
        row_at = lax.broadcasted_iota(jnp.int32, (128, 128), 1)
        near = (key_at // KEY_BLOCK == row_at // KEY_BLOCK) & (key_at <= row_at)
        dots = jnp.zeros((8, TQ), jnp.float32)
        own_dots = []
        for i in range(nkb):
            rows = slice(i * KB, (i + 1) * KB)
            if behind is not None:
                behind(i)
            keys = kv_ref[i * per : (i + 1) * per, 0:CAP].reshape(KB, HEAD_DIM)
            values = kv_ref[i * per : (i + 1) * per, CAP : 2 * CAP].reshape(KB, HEAD_DIM)
            s = lax.dot_general(keys, q, nt, preferred_element_type=jnp.float32)
            dp = lax.dot_general(values, g, nt, preferred_element_type=jnp.float32)
            shift = bias_ref[i * per * CAP : (i + 1) * per * CAP, :] - lse
            s = (s * (scale * LOG2E)).reshape(per * CAP, KEY_BLOCK, TQ) + shift[:, None, :]
            p = jnp.exp2(s).reshape(KB, TQ)
            p_s[rows, :] = p
            dp_s[rows, :] = dp
            dv = jnp.dot(p.astype(jnp.bfloat16), g, preferred_element_type=jnp.float32)
            dv_s[rows, :] = dv if first else dv_s[rows, :] + dv
            dots = dots + (p * dp).reshape(KB // 8, 8, TQ).sum(axis=0)
            if i < parts:
                c = cut(i)
                s = lax.dot_general(ko_ref[c, :], q[c], nt, preferred_element_type=jnp.float32)
                dp = lax.dot_general(vo_ref[c, :], g[c], nt, preferred_element_type=jnp.float32)
                p = jnp.exp2(jnp.where(near, s * (scale * LOG2E) - lse[:, c], NEG))
                po_s[c, :] = p
                dpo_s[c, :] = dp
                own_dots.append(jnp.sum(p * dp, axis=0, keepdims=True))
                dvo_ref[c, :] = jnp.dot(
                    p.astype(jnp.bfloat16), g[c], preferred_element_type=jnp.float32
                )
        return jnp.sum(dots, axis=0, keepdims=True) + jnp.concatenate(own_dots, axis=1)

    def second_half(first):
        q = qq_s[...]
        dots = dots_s[...]
        held = []
        own = []

        def behind(i):
            rows = slice(i * KB, (i + 1) * KB)
            ds = (p_s[rows, :] * (dp_s[rows, :] - dots)).astype(jnp.bfloat16)
            dk = jnp.dot(ds, q, preferred_element_type=jnp.float32)
            dk_s[rows, :] = dk if first else dk_s[rows, :] + dk
            part = jnp.dot(kt_s[:, rows], ds, preferred_element_type=jnp.float32)
            held[:] = [held[0] + part] if held else [part]
            if i < parts:
                c = cut(i)
                ds = (po_s[c, :] * (dpo_s[c, :] - dots[:, c])).astype(jnp.bfloat16)
                dko_ref[c, :] = scale * jnp.dot(ds, q[c], preferred_element_type=jnp.float32)
                own.append(jnp.dot(kk_s[c, :].T, ds, preferred_element_type=jnp.float32))

        def finish():
            for t in range(parts):
                out = (scale * (held[0][:, cut(t)] + own[t])).T.astype(jnp.bfloat16)
                gq_ref[cut(t), :] = out
                gqf_ref[cut(t), :] = out

        return behind, finish

    def keep(dots):
        dots_s[...] = dots
        qq_s[...] = q_ref[...]
        kk_s[...] = ko_ref[...]

    @pl.when(step == 0)
    def _():
        for i in range(nkb):
            keys = kv_ref[i * per : (i + 1) * per, 0:CAP].reshape(KB, HEAD_DIM)
            kt_s[:, i * KB : (i + 1) * KB] = keys.T
        keep(ahead(True, None))
        dk_s[...] = jnp.zeros_like(dk_s)

    @pl.when((step > 0) & (step < tiles))
    def _():
        behind, finish = second_half(False)
        dots = ahead(False, behind)
        finish()
        keep(dots)

    @pl.when(step == tiles)
    def _():
        behind, finish = second_half(False)
        for i in range(nkb):
            behind(i)
        finish()
        shape = (far // (CAP * KEY_BLOCK), CAP, KEY_BLOCK, HEAD_DIM)
        dk = (scale * dk_s[...]).astype(jnp.bfloat16).reshape(shape)
        dv = dv_s[...].astype(jnp.bfloat16).reshape(shape)
        if merge:
            me = me_ref[0]
            for n in range(shape[0]):

                @pl.when(n < me)
                def _(n=n):
                    back_ref[n, 0:CAP] = dk[n]
                    back_ref[n, CAP : 2 * CAP] = dv[n]

                @pl.when(n >= me)
                def _(n=n):
                    back_ref[n] = ahead_ref[n]
        else:
            back_ref[:, 0:CAP] = dk
            back_ref[:, CAP : 2 * CAP] = dv


def land_kernel(me_ref, tab_ref, back_ref, dko_ref, dvo_ref, *rest, head, spans):
    gk_ref, gv_ref = rest[-2:]
    gk_ref[...] = dko_ref[...]
    gv_ref[...] = dvo_ref[...]
    me = me_ref[0]
    half = spans // 2

    def one(n, carry):
        at = head * half + n // 2
        odd = n % 2
        for c in range(CAP):
            named = tab_ref[4 + 2 * c + odd, at] > 0
            first = tab_ref[2 * c + odd, at] * KEY_BLOCK
            rows = pl.ds(pl.multiple_of(first, KEY_BLOCK), KEY_BLOCK)
            gk_ref[rows, :] += jnp.where(named, back_ref[n, c].astype(jnp.float32), 0.0)
            gv_ref[rows, :] += jnp.where(named, back_ref[n, CAP + c].astype(jnp.float32), 0.0)

        return carry

    lax.fori_loop(me + 1, spans, one, 0)


SMEM = pl.BlockSpec(memory_space=pltpu.SMEM)
VMEM = pl.BlockSpec(memory_space=pltpu.VMEM)
ANY = pl.BlockSpec(memory_space=pl.ANY)


def params(**more):
    return pltpu.CompilerParams(vmem_limit_bytes=VMEM_LIMIT, **more)


def cost(flops, data=1 << 20):
    return pl.CostEstimate(flops=flops, transcendentals=0, bytes_accessed=data)


def five(spans, slots=1):
    return (spans, slots, 2 * CAP, KEY_BLOCK, HEAD_DIM)


def slotted(spans, slot):
    return pl.BlockSpec(
        (spans, None, 2 * CAP, KEY_BLOCK, HEAD_DIM), lambda i: (0, slot, 0, 0, 0)
    )


def back_spec(spans, shape):
    return slotted(spans, 0) if len(shape) == 5 else tiles_of(spans, 2 * CAP, 0)


def pack_first(me, ids, key_blocks, value_blocks, heads, spans):
    blocks = key_blocks.shape[0]
    column = pl.BlockSpec((blocks, KEY_BLOCK, HEAD_DIM), lambda i: (0, 0, 0))
    return pl.pallas_call(
        functools.partial(first_kernel, heads=heads, spans=spans, blocks=blocks),
        grid=(1,),
        out_shape=[
            jax.ShapeDtypeStruct(five(spans), jnp.bfloat16),
            jax.ShapeDtypeStruct((8, 128), jnp.int32),
        ],
        in_specs=[SMEM, VMEM, column, column],
        out_specs=[slotted(spans, 0), VMEM],
        scratch_shapes=[
            pltpu.VMEM((heads * spans // 2, 128), jnp.int32),
            pltpu.VMEM((heads * spans // 2, 128), jnp.int32),
            pltpu.VMEM((8, 128), jnp.int32),
            pltpu.SMEM((8, 128), jnp.int32),
            pltpu.SemaphoreType.DMA,
        ],
        compiler_params=params(),
        cost_estimate=cost(1 << 26),
        name="first",
    )(me, ids, key_blocks, value_blocks)


def pack_rest(tab, key_blocks, value_blocks, heads, spans):
    return pl.pallas_call(
        functools.partial(pack_kernel, spans=spans),
        grid=(1,),
        out_shape=[jax.ShapeDtypeStruct(five(spans), jnp.bfloat16)] * (heads - 1),
        in_specs=[SMEM, VMEM, VMEM],
        out_specs=[slotted(spans, 0)] * (heads - 1),
        compiler_params=params(),
        cost_estimate=cost(1 << 26),
        name="pack",
    )(tab, key_blocks, value_blocks)


def mask(me, ids, spans, blocks):
    heads, picks, _ = ids.shape
    return pl.pallas_call(
        functools.partial(mask_kernel, heads=heads, spans=spans, blocks=blocks, picks=picks),
        out_shape=jax.ShapeDtypeStruct((heads, spans * CAP, blocks * KEY_BLOCK), jnp.float32),
        in_specs=[SMEM, VMEM],
        out_specs=VMEM,
        compiler_params=params(),
        cost_estimate=cost(1 << 26),
        name="mask",
    )(me, ids)


def turn(x):
    rows, cols = x.shape
    return pl.pallas_call(
        turn_kernel,
        grid=(cols // 256,),
        out_shape=pltpu.VMEM((cols, rows), x.dtype),
        in_specs=[pl.BlockSpec((rows, 256), lambda i: (0, i))],
        out_specs=pl.BlockSpec((256, rows), lambda i: (i, 0)),
        compiler_params=params(),
        cost_estimate=cost(1 << 26),
        name="turn",
    )(x)


def attend(head, me, q, g, k, v, lse, bias, far_kv, gq_full, ahead, back_shape):
    rows, width = q.shape
    heads = lse.shape[0]
    tiles = rows // TQ
    spans = far_kv.shape[0]
    far = spans * CAP * KEY_BLOCK

    def now(i):
        return jnp.minimum(i, tiles - 1)

    def then(i):
        return jnp.maximum(i - 1, 0)

    column = pl.BlockSpec((TQ, HEAD_DIM), lambda i: (now(i), head))
    alone = pl.BlockSpec((TQ, HEAD_DIM), lambda i: (now(i), 0))
    late_column = pl.BlockSpec((TQ, HEAD_DIM), lambda i: (then(i), head))
    late = pl.BlockSpec((TQ, HEAD_DIM), lambda i: (then(i), 0))
    in_specs = [
        SMEM,
        column,
        column,
        column,
        column,
        pl.BlockSpec((heads, TQ), lambda i: (0, now(i))),
        pl.BlockSpec((None, spans * CAP, TQ), lambda i: (head, 0, now(i))),
        slotted(spans, 0),
    ]
    args = [me, q, g, k, v, lse, bias, far_kv]
    merge = ahead is not None
    if merge:
        in_specs.append(slotted(spans, 0))
        args.append(ahead)
    aliases = {}
    if gq_full is not None:
        aliases[len(args)] = 0
        in_specs.append(ANY)
        args.append(gq_full)
    return pl.pallas_call(
        functools.partial(
            attend_kernel, head=head, extra=len(aliases), merge=int(merge), tiles=tiles, far=far
        ),
        grid=(tiles + 1,),
        in_specs=in_specs,
        out_specs=[late_column, late, late, alone, back_spec(spans, back_shape)],
        out_shape=[
            jax.ShapeDtypeStruct((rows, width), jnp.bfloat16),
            jax.ShapeDtypeStruct((rows, HEAD_DIM), jnp.bfloat16),
            jax.ShapeDtypeStruct((rows, HEAD_DIM), jnp.float32),
            jax.ShapeDtypeStruct((rows, HEAD_DIM), jnp.float32),
            jax.ShapeDtypeStruct(back_shape, jnp.bfloat16),
        ],
        scratch_shapes=[
            pltpu.VMEM((far, TQ), jnp.float32),
            pltpu.VMEM((far, TQ), jnp.float32),
            pltpu.VMEM((TQ, 128), jnp.float32),
            pltpu.VMEM((TQ, 128), jnp.float32),
            pltpu.VMEM((1, TQ), jnp.float32),
            pltpu.VMEM((far, HEAD_DIM), jnp.float32),
            pltpu.VMEM((far, HEAD_DIM), jnp.float32),
            pltpu.VMEM((HEAD_DIM, far), jnp.bfloat16),
            pltpu.VMEM((TQ, HEAD_DIM), jnp.bfloat16),
            pltpu.VMEM((TQ, HEAD_DIM), jnp.bfloat16),
        ],
        input_output_aliases=aliases,
        cost_estimate=cost(10 * rows * far * HEAD_DIM, 8 << 20),
        compiler_params=params(dimension_semantics=("arbitrary",)),
    )(*args)


def weigh(me, xt, shards, buffer, spans, slot, slots, halves=False):
    cols, rows = xt.shape
    in_specs = [SMEM, VMEM] + [ANY] * len(shards)
    args = [me, pltpu.with_memory_space_constraint(xt, pltpu.VMEM), *shards]
    aliases = {}
    if buffer is not None:
        aliases[len(args)] = 0
        in_specs.append(ANY)
        args.append(buffer)
    half = (spans, len(shards) // 2, cols // spans, HEAD_DIM)
    if halves:
        out_specs = [ANY, ANY]
        out_shape = [jax.ShapeDtypeStruct(half, jnp.bfloat16)] * 2
    else:
        out_specs = ANY
        out_shape = jax.ShapeDtypeStruct(five(spans, slots), jnp.bfloat16)
    return pl.pallas_call(
        functools.partial(weight_kernel, extra=len(aliases), slot=slot, halves=halves),
        in_specs=in_specs,
        out_specs=out_specs,
        out_shape=out_shape,
        scratch_shapes=[
            pltpu.VMEM((2, rows, 2 * HEAD_DIM), jnp.bfloat16),
            pltpu.VMEM((2,) + half, jnp.bfloat16),
            pltpu.SemaphoreType.DMA((4,)),
            pltpu.SemaphoreType.DMA((2,)),
        ],
        input_output_aliases=aliases,
        compiler_params=params(),
        cost_estimate=cost(2 * cols * rows * len(shards) * HEAD_DIM, 8 << 20),
        name="weigh",
    )(*args)


def tiles_of(spans, count, at):
    return pl.BlockSpec((spans, count, KEY_BLOCK, HEAD_DIM), lambda i: (0, at, 0, 0))


def join(keep, got, buffer, at):
    args, aliases = [keep, got], {}
    out_shape = jax.ShapeDtypeStruct(keep.shape, keep.dtype)
    if buffer is not None:
        aliases = {2: 0}
        args.append(buffer)
        out_shape = jax.ShapeDtypeStruct(buffer.shape, buffer.dtype)
    return pl.pallas_call(
        functools.partial(join_kernel, at=at),
        in_specs=[ANY] * len(args),
        out_specs=ANY,
        out_shape=out_shape,
        scratch_shapes=[
            pltpu.VMEM(keep.shape, keep.dtype),
            pltpu.VMEM(keep.shape, keep.dtype),
            pltpu.SemaphoreType.DMA((3,)),
        ],
        input_output_aliases=aliases,
        compiler_params=params(),
        cost_estimate=cost(1 << 24),
        name="join",
    )(*args)


def total(place, got, slot, head, heads, order):
    return pl.pallas_call(
        functools.partial(total_kernel, head=head, heads=heads, order=order),
        grid=(1,),
        in_specs=[SMEM, slotted(got.shape[0], slot)],
        out_specs=VMEM,
        out_shape=jax.ShapeDtypeStruct(
            (KEY_BLOCK, len(order) * heads * HEAD_DIM), jnp.float32
        ),
        compiler_params=params(),
        cost_estimate=cost(1 << 24),
        name="total",
    )(place, got)


def pair_total(place, got, at, buffer, head, heads, order):
    half = (got.shape[0], len(order) // 2, KEY_BLOCK, HEAD_DIM)
    return pl.pallas_call(
        functools.partial(pair_total_kernel, at=at, head=head, heads=heads, order=order),
        in_specs=[SMEM, ANY, ANY],
        out_specs=ANY,
        out_shape=jax.ShapeDtypeStruct(buffer.shape, buffer.dtype),
        scratch_shapes=[
            pltpu.VMEM(half, got.dtype),
            pltpu.VMEM((len(order), KEY_BLOCK, HEAD_DIM), jnp.float32),
            pltpu.SemaphoreType.DMA,
            pltpu.SemaphoreType.DMA((len(order),)),
        ],
        input_output_aliases={2: 0},
        compiler_params=params(),
        cost_estimate=cost(1 << 24),
        name="pairtotal",
    )(place, got, buffer)


def land(head, me, tab, home, dko, dvo, full, rows, width):
    spans = home.shape[0]
    column = pl.BlockSpec((rows, HEAD_DIM), lambda i: (0, head))
    alone = pl.BlockSpec((rows, HEAD_DIM), lambda i: (0, 0))
    in_specs = [SMEM, SMEM, back_spec(spans, home.shape), alone, alone]
    args = [me, tab, home, dko, dvo]
    aliases = {}
    if full is not None:
        in_specs += [ANY, ANY]
        args += list(full)
        aliases = {5: 0, 6: 1}
    return pl.pallas_call(
        functools.partial(land_kernel, head=head, spans=spans),
        grid=(1,),
        in_specs=in_specs,
        out_specs=[column, column],
        out_shape=[jax.ShapeDtypeStruct((rows, width), jnp.float32)] * 2,
        input_output_aliases=aliases,
        compiler_params=pltpu.CompilerParams(vmem_limit_bytes=32 * 1024 * 1024),
        cost_estimate=cost(1 << 24),
    )(*args)


def exchange(x):
    return lax.all_to_all(x, "kv", split_axis=0, concat_axis=0, tiled=True)


def shift(x, by, tp):
    return lax.ppermute(x, "tp", [(i, (i + by) % tp) for i in range(tp)])


def program(query_rows, key_rows, value_rows, log_sums, cotangent, layer_input, chosen):
    spans = lax.axis_size("kv")
    tp = lax.axis_size("tp")
    heads = log_sums.shape[0]
    rows, width = query_rows.shape
    blocks = rows // KEY_BLOCK
    me = lax.axis_index("kv").astype(jnp.int32).reshape(1)
    place = lax.axis_index("tp").astype(jnp.int32).reshape(1)
    ids = jnp.transpose(chosen, (0, 2, 1))
    key_blocks = key_rows.reshape(blocks, KEY_BLOCK, width)
    value_blocks = value_rows.reshape(blocks, KEY_BLOCK, width)
    order = (0, 1, 3, 2)

    send0, tab = pack_first(me, ids, key_blocks, value_blocks, heads, spans)
    far0 = exchange(send0)
    send1, send2 = pack_rest(tab, key_blocks, value_blocks, heads, spans)
    xt = turn(layer_input)
    bias = mask(me, ids, spans, blocks)

    def attention(h, far, gq_full, ahead, back_shape):
        return attend(
            h, me, query_rows, cotangent, key_rows, value_rows, log_sums, bias, far,
            gq_full, ahead, back_shape,
        )

    def gathered(gq):
        right = shift(gq, -1, tp)
        left = shift(gq, 1, tp)
        across = shift(gq, 2, tp)
        return gq, right, left, across

    def swapped(x):
        return lax.ppermute(x, "kv", [(i, i ^ 1) for i in range(spans)])

    far1 = exchange(send1)
    gq_full, gq, *own0, out = attention(0, far0, None, send2, five(spans))
    shards0 = gathered(gq)
    far2 = exchange(out)
    gq_full, gq, *own1, out = attention(1, far1, gq_full, None, five(spans, 2))
    shards1 = gathered(gq)
    out = weigh(me, xt, shards0, out, spans, 1, 2)
    home1 = exchange(out)
    room = (spans, 2 * CAP + tp // 2, KEY_BLOCK, HEAD_DIM)
    gq_full, gq, *own2, out = attention(2, far2, gq_full, None, room)
    shards2 = gathered(gq)

    def shared(shards, buffer, at):
        keep, give = weigh(me, xt, shards, None, spans, 0, 1, halves=True)
        got = swapped(give)
        return join(keep, got, buffer, at)

    home2 = exchange(shared(shards1, out, 2))
    last = exchange(shared(shards2, None, 0))

    full = None
    for h, (home, own) in enumerate(((far2, own0), (home1, own1), (home2, own2))):
        full = land(h, me, tab, home, *own, full, rows, width)
    grad_weight = total(place, home1, 1, 0, heads, order)
    grad_weight = pair_total(place, home2, 2, grad_weight, 1, heads, order)
    grad_weight = pair_total(place, last, 0, grad_weight, 2, heads, order)
    return gq_full, full[0], full[1], grad_weight


def solution(mesh):
    placed = (
        P("kv", "tp"),
        P("kv", "tp"),
        P("kv", "tp"),
        P("tp", "kv"),
        P("kv", "tp"),
        P("kv", "tp"),
        P("tp", None, None),
    )
    return jax.shard_map(
        program,
        mesh=mesh,
        in_specs=placed,
        out_specs=(P("kv", "tp"), P("kv", "tp"), P("kv", "tp"), P(("tp", "kv"), None)),
        check_vma=False,
    )
```

```python
import functools

import jax
import jax.numpy as jnp
from jax import lax
from jax.experimental import pallas as pl
from jax.experimental.pallas import tpu as pltpu
from jax.sharding import PartitionSpec as P


HEAD_DIM = 128
KEY_BLOCK = 32
CAP = 2
BIG = 1 << 20
LOG2E = 1.4426950408889634
NEG = -1.0e30
TQ = 512
VMEM_LIMIT = 60960 * 1024
WEIGH_ROWS = 512
KB = 256


def spread(column):
    wide = jnp.broadcast_to(column.astype(jnp.float32), (column.shape[0], 128))
    wide = jnp.concatenate([wide, jnp.zeros((128 - column.shape[0], 128), jnp.float32)], axis=0)
    return wide.T[0:1, :].astype(jnp.int32)


def copy_blocks(tab_s, k_ref, v_ref, send, h, half, lanes):
    def fill(m, carry):
        for odd in range(2):
            for c in range(CAP):
                b = tab_s[2 * c + odd, h * half + m]
                send[2 * m + odd, c] = k_ref[b, :, lanes]
                send[2 * m + odd, CAP + c] = v_ref[b, :, lanes]
        return carry

    lax.fori_loop(0, half, fill, 0)


def first_kernel(me_ref, chosen_ref, k_ref, v_ref, send, tab_ref, lo_s, hi_s, tab_v, tab_s, sem,
                 *, heads, spans, blocks):
    me = me_ref[0]
    half = spans // 2
    for h in range(heads):
        ids = chosen_ref[h]
        mine = (ids >> 6) == me
        lo = jnp.min(jnp.where(mine, ids, BIG), axis=0, keepdims=True)
        hi = jnp.max(jnp.where(mine, ids, -1), axis=0, keepdims=True)
        for m in range(half):
            lo_s[h * half + m : h * half + m + 1, :] = lo[:, m * 128 : (m + 1) * 128]
            hi_s[h * half + m : h * half + m + 1, :] = hi[:, m * 128 : (m + 1) * 128]
    lane = lax.broadcasted_iota(jnp.int32, (heads * half, 128), 1)
    tab_v[...] = jnp.zeros((8, 128), jnp.int32)
    for odd in range(2):
        ours = (lane // blocks) == odd
        lo = spread(jnp.min(jnp.where(ours, lo_s[...], BIG), axis=1, keepdims=True))
        hi = spread(jnp.max(jnp.where(ours, hi_s[...], -1), axis=1, keepdims=True))
        tab_v[odd : odd + 1, :] = lo & (blocks - 1)
        tab_v[2 + odd : 3 + odd, :] = jnp.maximum(hi, 0) & (blocks - 1)
        tab_v[4 + odd : 5 + odd, :] = (hi >= 0).astype(jnp.int32)
        tab_v[6 + odd : 7 + odd, :] = (hi > lo).astype(jnp.int32)
    tab_ref[...] = tab_v[...]
    copy = pltpu.make_async_copy(tab_v, tab_s, sem)
    copy.start()
    copy.wait()
    copy_blocks(tab_s, k_ref, v_ref, send, 0, half, slice(0, HEAD_DIM))


def pack_kernel(tab_ref, k_ref, v_ref, *sends, spans):
    for n, send in enumerate(sends):
        h = n + 1
        lanes = slice(h * HEAD_DIM, (h + 1) * HEAD_DIM)
        copy_blocks(tab_ref, k_ref, v_ref, send, h, spans // 2, lanes)


def mask_kernel(me_ref, chosen_ref, bias_ref, *, heads, spans, blocks, picks):
    me = me_ref[0]
    slots = spans * CAP
    slot = lax.broadcasted_iota(jnp.int32, (slots, 128), 0)
    lane = lax.broadcasted_iota(jnp.int32, (slots, 128), 1)
    ours = (lane // blocks) == (me % 2)
    place = lax.broadcasted_iota(jnp.int32, (128, blocks * KEY_BLOCK), 1) // KEY_BLOCK
    row = lax.broadcasted_iota(jnp.int32, (128, blocks * KEY_BLOCK), 0)
    expand = ((place + (me % 2) * blocks) == row).astype(jnp.bfloat16)
    start = pl.multiple_of((me // 2) * 128, 128)

    def one(h, carry):
        ids = chosen_ref[h, :, pl.ds(start, 128)]
        cols = [jnp.broadcast_to(ids[c : c + 1, :], (slots, 128)) for c in range(picks)]
        least = jnp.full((slots, 128), BIG, jnp.int32)
        most = jnp.full((slots, 128), -1, jnp.int32)
        for col in cols:
            hit = ((col >> 6) == (slot >> 1)) & ours
            least = jnp.minimum(least, jnp.where(hit, col, BIG))
            most = jnp.maximum(most, jnp.where(hit, col, -1))
        least = jnp.min(least, axis=1, keepdims=True)
        most = jnp.max(most, axis=1, keepdims=True)
        name = jnp.where(
            (slot & 1) == 0, least, jnp.where(most > least, most, -7)
        )
        named = cols[0] == name
        for col in cols[1:]:
            named = named | (col == name)
        hot = jnp.where(named, 1.0, 0.0).astype(jnp.bfloat16)
        full = jnp.dot(hot, expand, preferred_element_type=jnp.float32)
        bias_ref[h] = jnp.where(full > 0.5, 0.0, NEG)
        return carry

    lax.fori_loop(0, heads, one, 0)


def turn_kernel(x_ref, out_ref):
    rows = x_ref.shape[0]
    for i in range(rows // 256):
        cut = slice(i * 256, (i + 1) * 256)
        out_ref[:, cut] = x_ref[cut, :].T


def weight_kernel(me_ref, xt_ref, *rest, extra, slot, halves):
    shards = rest[:4]
    outs = rest[4 + extra : -4]
    g_s, o_s, in_sem, out_sem = rest[-4:]
    copies = []
    for n, shard in enumerate(shards):
        lanes = pl.ds((n % 2) * HEAD_DIM, HEAD_DIM)
        copy = pltpu.make_async_copy(shard, g_s.at[n // 2, :, lanes], in_sem.at[n])
        copy.start()
        copies.append(copy)
    rows = xt_ref.shape[0]
    shape = (WEIGH_ROWS // KEY_BLOCK, KEY_BLOCK, HEAD_DIM)
    ends = []
    for pair in range(2):
        copies[2 * pair].wait()
        copies[2 * pair + 1].wait()
        g = g_s[pair]

        def some(b, carry, pair=pair, g=g):
            first = pl.multiple_of(b * WEIGH_ROWS, WEIGH_ROWS)
            xt = xt_ref[pl.ds(first, WEIGH_ROWS), :]
            got = jnp.dot(xt, g, preferred_element_type=jnp.float32).astype(jnp.bfloat16)
            owners = pl.ds(b * shape[0], shape[0])
            o_s[pair, owners, 0] = got[:, :HEAD_DIM].reshape(shape)
            o_s[pair, owners, 1] = got[:, HEAD_DIM:].reshape(shape)
            return carry

        lax.fori_loop(0, rows // WEIGH_ROWS, some, 0, unroll=not halves)
        if halves:
            core = me_ref[0] % 2
            for out, mine in ((outs[0], core == pair), (outs[1], core != pair)):
                copy = pltpu.make_async_copy(o_s.at[pair], out, out_sem.at[pair])
                pl.when(mine)(copy.start)
                ends.append((copy, mine))
        else:
            target = outs[0].at[:, slot, pl.ds(2 * pair, 2)]
            copy = pltpu.make_async_copy(o_s.at[pair], target, out_sem.at[pair])
            copy.start()
            ends.append((copy, None))
    for copy, mine in ends:
        if mine is None:
            copy.wait()
        else:
            pl.when(mine)(copy.wait)


def join_kernel(keep_ref, got_ref, *rest, at):
    out_ref, keep_s, got_s, sem = rest[-4:]
    one = pltpu.make_async_copy(keep_ref, keep_s, sem.at[0])
    two = pltpu.make_async_copy(got_ref, got_s, sem.at[1])
    one.start()
    two.start()
    one.wait()
    two.wait()
    both = keep_s[...].astype(jnp.float32) + got_s[...].astype(jnp.float32)
    got_s[...] = both.astype(jnp.bfloat16)
    count = keep_ref.shape[1]
    back = pltpu.make_async_copy(got_s, out_ref.at[:, pl.ds(at * count, count)], sem.at[2])
    back.start()
    back.wait()


def put_sum(out_ref, got_ref, sources, column, first):
    acc = got_ref[sources[0], column].astype(jnp.float32)
    for i in sources[1:]:
        acc = acc + got_ref[i, column].astype(jnp.float32)
    out_ref[:, pl.ds(pl.multiple_of(first, HEAD_DIM), HEAD_DIM)] = acc


def total_kernel(at_ref, got_ref, out_ref, *, head, heads, order):
    tp = len(order)
    out_ref[...] = jnp.zeros_like(out_ref)
    for p in range(tp):
        place = (at_ref[0] + order[p]) % tp
        sources = range(got_ref.shape[0])
        put_sum(out_ref, got_ref, sources, p, (place * heads + head) * HEAD_DIM)


def pair_total_kernel(at_ref, got_ref, before_ref, out_ref, got_s, sum_s, got_sem, sem,
                      *, at, head, heads, order):
    tp = len(order)
    got = pltpu.make_async_copy(got_ref.at[:, pl.ds(at * tp // 2, tp // 2)], got_s, got_sem)
    got.start()
    got.wait()
    copies = []
    for p in range(tp):
        place = (at_ref[0] + order[p]) % tp
        acc = got_s[p // 2, p % 2].astype(jnp.float32)
        for i in range(p // 2 + 2, got_s.shape[0], 2):
            acc = acc + got_s[i, p % 2].astype(jnp.float32)
        sum_s[p] = acc
        first = pl.multiple_of((place * heads + head) * HEAD_DIM, HEAD_DIM)
        copy = pltpu.make_async_copy(
            sum_s.at[p], out_ref.at[:, pl.ds(first, HEAD_DIM)], sem.at[p]
        )
        copy.start()
        copies.append(copy)
    for copy in copies:
        copy.wait()


def attend_kernel(me_ref, *refs, head, extra, merge, tiles, far):
    q_ref, g_ref, ko_ref, vo_ref, lse_ref, bias_ref, kv_ref = refs[:7]
    ahead_ref = refs[7] if merge else None
    rest = refs[7 + merge + extra :]
    gqf_ref, gq_ref, dko_ref, dvo_ref, back_ref = rest[:5]
    p_s, dp_s, po_s, dpo_s, dots_s, dk_s, dv_s, kt_s, qq_s, kk_s = rest[5:]
    step = pl.program_id(0)
    scale = HEAD_DIM**-0.5
    nkb = far // KB
    per = KB // (CAP * KEY_BLOCK)
    parts = TQ // 128
    nt = (((1,), (1,)), ((), ()))

    def cut(t):
        return slice(t * 128, (t + 1) * 128)

    def ahead(first, behind):
        q = q_ref[...]
        g = g_ref[...]
        lse = lse_ref[head : head + 1, :] * LOG2E
        key_at = lax.broadcasted_iota(jnp.int32, (128, 128), 0)
        row_at = lax.broadcasted_iota(jnp.int32, (128, 128), 1)
        near = (key_at // KEY_BLOCK == row_at // KEY_BLOCK) & (key_at <= row_at)
        dots = jnp.zeros((8, TQ), jnp.float32)
        own_dots = []
        for i in range(nkb):
            rows = slice(i * KB, (i + 1) * KB)
            if behind is not None:
                behind(i)
            keys = kv_ref[i * per : (i + 1) * per, 0:CAP].reshape(KB, HEAD_DIM)
            values = kv_ref[i * per : (i + 1) * per, CAP : 2 * CAP].reshape(KB, HEAD_DIM)
            s = lax.dot_general(keys, q, nt, preferred_element_type=jnp.float32)
            dp = lax.dot_general(values, g, nt, preferred_element_type=jnp.float32)
            shift = bias_ref[i * per * CAP : (i + 1) * per * CAP, :] - lse
            s = (s * (scale * LOG2E)).reshape(per * CAP, KEY_BLOCK, TQ) + shift[:, None, :]
            p = jnp.exp2(s).reshape(KB, TQ)
            p_s[rows, :] = p
            dp_s[rows, :] = dp
            dv = jnp.dot(p.astype(jnp.bfloat16), g, preferred_element_type=jnp.float32)
            dv_s[rows, :] = dv if first else dv_s[rows, :] + dv
            dots = dots + (p * dp).reshape(KB // 8, 8, TQ).sum(axis=0)
            if i < parts:
                c = cut(i)
                s = lax.dot_general(ko_ref[c, :], q[c], nt, preferred_element_type=jnp.float32)
                dp = lax.dot_general(vo_ref[c, :], g[c], nt, preferred_element_type=jnp.float32)
                p = jnp.exp2(jnp.where(near, s * (scale * LOG2E) - lse[:, c], NEG))
                po_s[c, :] = p
                dpo_s[c, :] = dp
                own_dots.append(jnp.sum(p * dp, axis=0, keepdims=True))
                dvo_ref[c, :] = jnp.dot(
                    p.astype(jnp.bfloat16), g[c], preferred_element_type=jnp.float32
                )
        return jnp.sum(dots, axis=0, keepdims=True) + jnp.concatenate(own_dots, axis=1)

    def second_half(first):
        q = qq_s[...]
        dots = dots_s[...]
        held = []
        own = []

        def behind(i):
            rows = slice(i * KB, (i + 1) * KB)
            ds = (p_s[rows, :] * (dp_s[rows, :] - dots)).astype(jnp.bfloat16)
            dk = jnp.dot(ds, q, preferred_element_type=jnp.float32)
            dk_s[rows, :] = dk if first else dk_s[rows, :] + dk
            part = jnp.dot(kt_s[:, rows], ds, preferred_element_type=jnp.float32)
            held[:] = [held[0] + part] if held else [part]
            if i < parts:
                c = cut(i)
                ds = (po_s[c, :] * (dpo_s[c, :] - dots[:, c])).astype(jnp.bfloat16)
                dko_ref[c, :] = scale * jnp.dot(ds, q[c], preferred_element_type=jnp.float32)
                own.append(jnp.dot(kk_s[c, :].T, ds, preferred_element_type=jnp.float32))

        def finish():
            for t in range(parts):
                out = (scale * (held[0][:, cut(t)] + own[t])).T.astype(jnp.bfloat16)
                gq_ref[cut(t), :] = out
                gqf_ref[cut(t), :] = out

        return behind, finish

    def keep(dots):
        dots_s[...] = dots
        qq_s[...] = q_ref[...]
        kk_s[...] = ko_ref[...]

    @pl.when(step == 0)
    def _():
        for i in range(nkb):
            keys = kv_ref[i * per : (i + 1) * per, 0:CAP].reshape(KB, HEAD_DIM)
            kt_s[:, i * KB : (i + 1) * KB] = keys.T
        keep(ahead(True, None))
        dk_s[...] = jnp.zeros_like(dk_s)

    @pl.when((step > 0) & (step < tiles))
    def _():
        behind, finish = second_half(False)
        dots = ahead(False, behind)
        finish()
        keep(dots)

    @pl.when(step == tiles)
    def _():
        behind, finish = second_half(False)
        for i in range(nkb):
            behind(i)
        finish()
        shape = (far // (CAP * KEY_BLOCK), CAP, KEY_BLOCK, HEAD_DIM)
        dk = (scale * dk_s[...]).astype(jnp.bfloat16).reshape(shape)
        dv = dv_s[...].astype(jnp.bfloat16).reshape(shape)
        if merge:
            me = me_ref[0]
            for n in range(shape[0]):
                back_ref[n, 0:CAP] = jnp.where(n < me, dk[n], ahead_ref[n, 0:CAP])
                back_ref[n, CAP : 2 * CAP] = jnp.where(
                    n < me, dv[n], ahead_ref[n, CAP : 2 * CAP]
                )
        else:
            back_ref[:, 0:CAP] = dk
            back_ref[:, CAP : 2 * CAP] = dv


def land_kernel(me_ref, tab_ref, back_ref, dko_ref, dvo_ref, *rest, head, spans):
    gk_ref, gv_ref = rest[-2:]
    gk_ref[...] = dko_ref[...]
    gv_ref[...] = dvo_ref[...]
    me = me_ref[0]
    half = spans // 2

    def one(n, carry):
        at = head * half + n // 2
        odd = n % 2
        for c in range(CAP):
            named = tab_ref[4 + 2 * c + odd, at] > 0
            first = tab_ref[2 * c + odd, at] * KEY_BLOCK
            rows = pl.ds(pl.multiple_of(first, KEY_BLOCK), KEY_BLOCK)
            gk_ref[rows, :] += jnp.where(named, back_ref[n, c].astype(jnp.float32), 0.0)
            gv_ref[rows, :] += jnp.where(named, back_ref[n, CAP + c].astype(jnp.float32), 0.0)

        return carry

    lax.fori_loop(me + 1, spans, one, 0)


SMEM = pl.BlockSpec(memory_space=pltpu.SMEM)
VMEM = pl.BlockSpec(memory_space=pltpu.VMEM)
ANY = pl.BlockSpec(memory_space=pl.ANY)


def params(**more):
    return pltpu.CompilerParams(vmem_limit_bytes=VMEM_LIMIT, **more)


def cost(flops, data=1 << 20):
    return pl.CostEstimate(flops=flops, transcendentals=0, bytes_accessed=data)


def five(spans, slots=1):
    return (spans, slots, 2 * CAP, KEY_BLOCK, HEAD_DIM)


def slotted(spans, slot):
    return pl.BlockSpec(
        (spans, None, 2 * CAP, KEY_BLOCK, HEAD_DIM), lambda i: (0, slot, 0, 0, 0)
    )


def back_spec(spans, shape):
    return slotted(spans, 0) if len(shape) == 5 else tiles_of(spans, 2 * CAP, 0)


def pack_first(me, ids, key_blocks, value_blocks, heads, spans):
    blocks = key_blocks.shape[0]
    column = pl.BlockSpec((blocks, KEY_BLOCK, HEAD_DIM), lambda i: (0, 0, 0))
    return pl.pallas_call(
        functools.partial(first_kernel, heads=heads, spans=spans, blocks=blocks),
        grid=(1,),
        out_shape=[
            jax.ShapeDtypeStruct(five(spans), jnp.bfloat16),
            jax.ShapeDtypeStruct((8, 128), jnp.int32),
        ],
        in_specs=[SMEM, VMEM, column, column],
        out_specs=[slotted(spans, 0), VMEM],
        scratch_shapes=[
            pltpu.VMEM((heads * spans // 2, 128), jnp.int32),
            pltpu.VMEM((heads * spans // 2, 128), jnp.int32),
            pltpu.VMEM((8, 128), jnp.int32),
            pltpu.SMEM((8, 128), jnp.int32),
            pltpu.SemaphoreType.DMA,
        ],
        compiler_params=params(),
        cost_estimate=cost(1 << 26),
        name="first",
    )(me, ids, key_blocks, value_blocks)


def pack_rest(tab, key_blocks, value_blocks, heads, spans):
    return pl.pallas_call(
        functools.partial(pack_kernel, spans=spans),
        grid=(1,),
        out_shape=[jax.ShapeDtypeStruct(five(spans), jnp.bfloat16)] * (heads - 1),
        in_specs=[SMEM, VMEM, VMEM],
        out_specs=[slotted(spans, 0)] * (heads - 1),
        compiler_params=params(),
        cost_estimate=cost(1 << 26),
        name="pack",
    )(tab, key_blocks, value_blocks)


def mask(me, ids, spans, blocks):
    heads, picks, _ = ids.shape
    return pl.pallas_call(
        functools.partial(mask_kernel, heads=heads, spans=spans, blocks=blocks, picks=picks),
        out_shape=jax.ShapeDtypeStruct((heads, spans * CAP, blocks * KEY_BLOCK), jnp.float32),
        in_specs=[SMEM, VMEM],
        out_specs=VMEM,
        compiler_params=params(),
        cost_estimate=cost(1 << 26),
        name="mask",
    )(me, ids)


def turn(x):
    rows, cols = x.shape
    return pl.pallas_call(
        turn_kernel,
        grid=(cols // 256,),
        out_shape=pltpu.VMEM((cols, rows), x.dtype),
        in_specs=[pl.BlockSpec((rows, 256), lambda i: (0, i))],
        out_specs=pl.BlockSpec((256, rows), lambda i: (i, 0)),
        compiler_params=params(),
        cost_estimate=cost(1 << 26),
        name="turn",
    )(x)


def attend(head, me, q, g, k, v, lse, bias, far_kv, gq_full, ahead, back_shape):
    rows, width = q.shape
    heads = lse.shape[0]
    tiles = rows // TQ
    spans = far_kv.shape[0]
    far = spans * CAP * KEY_BLOCK

    def now(i):
        return jnp.minimum(i, tiles - 1)

    def then(i):
        return jnp.maximum(i - 1, 0)

    column = pl.BlockSpec((TQ, HEAD_DIM), lambda i: (now(i), head))
    alone = pl.BlockSpec((TQ, HEAD_DIM), lambda i: (now(i), 0))
    late_column = pl.BlockSpec((TQ, HEAD_DIM), lambda i: (then(i), head))
    late = pl.BlockSpec((TQ, HEAD_DIM), lambda i: (then(i), 0))
    in_specs = [
        SMEM,
        column,
        column,
        column,
        column,
        pl.BlockSpec((heads, TQ), lambda i: (0, now(i))),
        pl.BlockSpec((None, spans * CAP, TQ), lambda i: (head, 0, now(i))),
        slotted(spans, 0),
    ]
    args = [me, q, g, k, v, lse, bias, far_kv]
    merge = ahead is not None
    if merge:
        in_specs.append(slotted(spans, 0))
        args.append(ahead)
    aliases = {}
    if gq_full is not None:
        aliases[len(args)] = 0
        in_specs.append(ANY)
        args.append(gq_full)
    return pl.pallas_call(
        functools.partial(
            attend_kernel, head=head, extra=len(aliases), merge=int(merge), tiles=tiles, far=far
        ),
        grid=(tiles + 1,),
        in_specs=in_specs,
        out_specs=[late_column, late, late, alone, back_spec(spans, back_shape)],
        out_shape=[
            jax.ShapeDtypeStruct((rows, width), jnp.bfloat16),
            jax.ShapeDtypeStruct((rows, HEAD_DIM), jnp.bfloat16),
            jax.ShapeDtypeStruct((rows, HEAD_DIM), jnp.float32),
            jax.ShapeDtypeStruct((rows, HEAD_DIM), jnp.float32),
            jax.ShapeDtypeStruct(back_shape, jnp.bfloat16),
        ],
        scratch_shapes=[
            pltpu.VMEM((far, TQ), jnp.float32),
            pltpu.VMEM((far, TQ), jnp.float32),
            pltpu.VMEM((TQ, 128), jnp.float32),
            pltpu.VMEM((TQ, 128), jnp.float32),
            pltpu.VMEM((1, TQ), jnp.float32),
            pltpu.VMEM((far, HEAD_DIM), jnp.float32),
            pltpu.VMEM((far, HEAD_DIM), jnp.float32),
            pltpu.VMEM((HEAD_DIM, far), jnp.bfloat16),
            pltpu.VMEM((TQ, HEAD_DIM), jnp.bfloat16),
            pltpu.VMEM((TQ, HEAD_DIM), jnp.bfloat16),
        ],
        input_output_aliases=aliases,
        cost_estimate=cost(10 * rows * far * HEAD_DIM, 8 << 20),
        compiler_params=params(dimension_semantics=("arbitrary",)),
    )(*args)


def weigh(me, xt, shards, buffer, spans, slot, slots, halves=False):
    cols, rows = xt.shape
    in_specs = [SMEM, VMEM] + [ANY] * len(shards)
    args = [me, pltpu.with_memory_space_constraint(xt, pltpu.VMEM), *shards]
    aliases = {}
    if buffer is not None:
        aliases[len(args)] = 0
        in_specs.append(ANY)
        args.append(buffer)
    half = (spans, len(shards) // 2, cols // spans, HEAD_DIM)
    if halves:
        out_specs = [ANY, ANY]
        out_shape = [jax.ShapeDtypeStruct(half, jnp.bfloat16)] * 2
    else:
        out_specs = ANY
        out_shape = jax.ShapeDtypeStruct(five(spans, slots), jnp.bfloat16)
    return pl.pallas_call(
        functools.partial(weight_kernel, extra=len(aliases), slot=slot, halves=halves),
        in_specs=in_specs,
        out_specs=out_specs,
        out_shape=out_shape,
        scratch_shapes=[
            pltpu.VMEM((2, rows, 2 * HEAD_DIM), jnp.bfloat16),
            pltpu.VMEM((2,) + half, jnp.bfloat16),
            pltpu.SemaphoreType.DMA((4,)),
            pltpu.SemaphoreType.DMA((2,)),
        ],
        input_output_aliases=aliases,
        compiler_params=params(),
        cost_estimate=cost(2 * cols * rows * len(shards) * HEAD_DIM, 8 << 20),
        name="weigh",
    )(*args)


def tiles_of(spans, count, at):
    return pl.BlockSpec((spans, count, KEY_BLOCK, HEAD_DIM), lambda i: (0, at, 0, 0))


def join(keep, got, buffer, at):
    args, aliases = [keep, got], {}
    out_shape = jax.ShapeDtypeStruct(keep.shape, keep.dtype)
    if buffer is not None:
        aliases = {2: 0}
        args.append(buffer)
        out_shape = jax.ShapeDtypeStruct(buffer.shape, buffer.dtype)
    return pl.pallas_call(
        functools.partial(join_kernel, at=at),
        in_specs=[ANY] * len(args),
        out_specs=ANY,
        out_shape=out_shape,
        scratch_shapes=[
            pltpu.VMEM(keep.shape, keep.dtype),
            pltpu.VMEM(keep.shape, keep.dtype),
            pltpu.SemaphoreType.DMA((3,)),
        ],
        input_output_aliases=aliases,
        compiler_params=params(),
        cost_estimate=cost(1 << 24),
        name="join",
    )(*args)


def total(place, got, slot, head, heads, order):
    return pl.pallas_call(
        functools.partial(total_kernel, head=head, heads=heads, order=order),
        grid=(1,),
        in_specs=[SMEM, slotted(got.shape[0], slot)],
        out_specs=VMEM,
        out_shape=jax.ShapeDtypeStruct(
            (KEY_BLOCK, len(order) * heads * HEAD_DIM), jnp.float32
        ),
        compiler_params=params(),
        cost_estimate=cost(1 << 24),
        name="total",
    )(place, got)


def pair_total(place, got, at, buffer, head, heads, order):
    half = (got.shape[0], len(order) // 2, KEY_BLOCK, HEAD_DIM)
    return pl.pallas_call(
        functools.partial(pair_total_kernel, at=at, head=head, heads=heads, order=order),
        in_specs=[SMEM, ANY, ANY],
        out_specs=ANY,
        out_shape=jax.ShapeDtypeStruct(buffer.shape, buffer.dtype),
        scratch_shapes=[
            pltpu.VMEM(half, got.dtype),
            pltpu.VMEM((len(order), KEY_BLOCK, HEAD_DIM), jnp.float32),
            pltpu.SemaphoreType.DMA,
            pltpu.SemaphoreType.DMA((len(order),)),
        ],
        input_output_aliases={2: 0},
        compiler_params=params(),
        cost_estimate=cost(1 << 24),
        name="pairtotal",
    )(place, got, buffer)


def land(head, me, tab, home, dko, dvo, full, rows, width):
    spans = home.shape[0]
    column = pl.BlockSpec((rows, HEAD_DIM), lambda i: (0, head))
    alone = pl.BlockSpec((rows, HEAD_DIM), lambda i: (0, 0))
    in_specs = [SMEM, SMEM, back_spec(spans, home.shape), alone, alone]
    args = [me, tab, home, dko, dvo]
    aliases = {}
    if full is not None:
        in_specs += [ANY, ANY]
        args += list(full)
        aliases = {5: 0, 6: 1}
    return pl.pallas_call(
        functools.partial(land_kernel, head=head, spans=spans),
        grid=(1,),
        in_specs=in_specs,
        out_specs=[column, column],
        out_shape=[jax.ShapeDtypeStruct((rows, width), jnp.float32)] * 2,
        input_output_aliases=aliases,
        compiler_params=pltpu.CompilerParams(vmem_limit_bytes=32 * 1024 * 1024),
        cost_estimate=cost(1 << 24),
    )(*args)


def exchange(x):
    return lax.all_to_all(x, "kv", split_axis=0, concat_axis=0, tiled=True)


def shift(x, by, tp):
    return lax.ppermute(x, "tp", [(i, (i + by) % tp) for i in range(tp)])


def program(query_rows, key_rows, value_rows, log_sums, cotangent, layer_input, chosen):
    spans = lax.axis_size("kv")
    tp = lax.axis_size("tp")
    heads = log_sums.shape[0]
    rows, width = query_rows.shape
    blocks = rows // KEY_BLOCK
    me = lax.axis_index("kv").astype(jnp.int32).reshape(1)
    place = lax.axis_index("tp").astype(jnp.int32).reshape(1)
    ids = jnp.transpose(chosen, (0, 2, 1))
    key_blocks = key_rows.reshape(blocks, KEY_BLOCK, width)
    value_blocks = value_rows.reshape(blocks, KEY_BLOCK, width)
    order = (0, 1, 3, 2)

    send0, tab = pack_first(me, ids, key_blocks, value_blocks, heads, spans)
    far0 = exchange(send0)
    send1, send2 = pack_rest(tab, key_blocks, value_blocks, heads, spans)
    xt = turn(layer_input)
    bias = mask(me, ids, spans, blocks)

    def attention(h, far, gq_full, ahead, back_shape):
        return attend(
            h, me, query_rows, cotangent, key_rows, value_rows, log_sums, bias, far,
            gq_full, ahead, back_shape,
        )

    def gathered(gq):
        right = shift(gq, -1, tp)
        left = shift(gq, 1, tp)
        across = shift(gq, 2, tp)
        return gq, right, left, across

    def swapped(x):
        return lax.ppermute(x, "kv", [(i, i ^ 1) for i in range(spans)])

    far1 = exchange(send1)
    gq_full, gq, *own0, out = attention(0, far0, None, send2, five(spans))
    shards0 = gathered(gq)
    far2 = exchange(out)
    gq_full, gq, *own1, out = attention(1, far1, gq_full, None, five(spans, 2))
    shards1 = gathered(gq)
    out = weigh(me, xt, shards0, out, spans, 1, 2)
    home1 = exchange(out)
    room = (spans, 2 * CAP + tp // 2, KEY_BLOCK, HEAD_DIM)
    gq_full, gq, *own2, out = attention(2, far2, gq_full, None, room)
    shards2 = gathered(gq)

    def shared(shards, buffer, at):
        keep, give = weigh(me, xt, shards, None, spans, 0, 1, halves=True)
        got = swapped(give)
        return join(keep, got, buffer, at)

    home2 = exchange(shared(shards1, out, 2))
    last = exchange(shared(shards2, None, 0))

    full = None
    for h, (home, own) in enumerate(((far2, own0), (home1, own1), (home2, own2))):
        full = land(h, me, tab, home, *own, full, rows, width)
    grad_weight = total(place, home1, 1, 0, heads, order)
    grad_weight = pair_total(place, home2, 2, grad_weight, 1, heads, order)
    grad_weight = pair_total(place, last, 0, grad_weight, 2, heads, order)
    return gq_full, full[0], full[1], grad_weight


def solution(mesh):
    placed = (
        P("kv", "tp"),
        P("kv", "tp"),
        P("kv", "tp"),
        P("tp", "kv"),
        P("kv", "tp"),
        P("kv", "tp"),
        P("tp", None, None),
    )
    return jax.shard_map(
        program,
        mesh=mesh,
        in_specs=placed,
        out_specs=(P("kv", "tp"), P("kv", "tp"), P("kv", "tp"), P(("tp", "kv"), None)),
        check_vma=False,
    )
```

```python
import functools

import jax
import jax.numpy as jnp
from jax import lax
from jax.experimental import pallas as pl
from jax.experimental.pallas import tpu as pltpu
from jax.sharding import PartitionSpec as P


HEAD_DIM = 128
KEY_BLOCK = 32
CAP = 2
BIG = 1 << 20
LOG2E = 1.4426950408889634
NEG = -1.0e30
TQ = 512
VMEM_LIMIT = 60960 * 1024
WEIGH_ROWS = 512
KB = 256


def spread(column):
    wide = jnp.broadcast_to(column.astype(jnp.float32), (column.shape[0], 128))
    wide = jnp.concatenate([wide, jnp.zeros((128 - column.shape[0], 128), jnp.float32)], axis=0)
    return wide.T[0:1, :].astype(jnp.int32)


def copy_blocks(tab_s, k_ref, v_ref, send, h, half, lanes):
    def fill(m, carry):
        for odd in range(2):
            for c in range(CAP):
                b = tab_s[2 * c + odd, h * half + m]
                send[2 * m + odd, c] = k_ref[b, :, lanes]
                send[2 * m + odd, CAP + c] = v_ref[b, :, lanes]
        return carry

    lax.fori_loop(0, half, fill, 0)


def first_kernel(me_ref, chosen_ref, k_ref, v_ref, send, tab_ref, lo_s, hi_s, tab_v, tab_s, sem,
                 *, heads, spans, blocks):
    me = me_ref[0]
    half = spans // 2
    for h in range(heads):
        ids = chosen_ref[h]
        mine = (ids >> 6) == me
        lo = jnp.min(jnp.where(mine, ids, BIG), axis=0, keepdims=True)
        hi = jnp.max(jnp.where(mine, ids, -1), axis=0, keepdims=True)
        for m in range(half):
            lo_s[h * half + m : h * half + m + 1, :] = lo[:, m * 128 : (m + 1) * 128]
            hi_s[h * half + m : h * half + m + 1, :] = hi[:, m * 128 : (m + 1) * 128]
    lane = lax.broadcasted_iota(jnp.int32, (heads * half, 128), 1)
    tab_v[...] = jnp.zeros((8, 128), jnp.int32)
    for odd in range(2):
        ours = (lane // blocks) == odd
        lo = spread(jnp.min(jnp.where(ours, lo_s[...], BIG), axis=1, keepdims=True))
        hi = spread(jnp.max(jnp.where(ours, hi_s[...], -1), axis=1, keepdims=True))
        tab_v[odd : odd + 1, :] = lo & (blocks - 1)
        tab_v[2 + odd : 3 + odd, :] = jnp.maximum(hi, 0) & (blocks - 1)
        tab_v[4 + odd : 5 + odd, :] = (hi >= 0).astype(jnp.int32)
        tab_v[6 + odd : 7 + odd, :] = (hi > lo).astype(jnp.int32)
    tab_ref[...] = tab_v[...]
    copy = pltpu.make_async_copy(tab_v, tab_s, sem)
    copy.start()
    copy.wait()
    copy_blocks(tab_s, k_ref, v_ref, send, 0, half, slice(0, HEAD_DIM))


def pack_kernel(tab_ref, k_ref, v_ref, *sends, spans):
    for n, send in enumerate(sends):
        h = n + 1
        lanes = slice(h * HEAD_DIM, (h + 1) * HEAD_DIM)
        copy_blocks(tab_ref, k_ref, v_ref, send, h, spans // 2, lanes)


def mask_kernel(me_ref, chosen_ref, bias_ref, *, heads, spans, blocks, picks):
    me = me_ref[0]
    slots = spans * CAP
    slot = lax.broadcasted_iota(jnp.int32, (slots, 128), 0)
    lane = lax.broadcasted_iota(jnp.int32, (slots, 128), 1)
    ours = (lane // blocks) == (me % 2)
    place = lax.broadcasted_iota(jnp.int32, (128, blocks * KEY_BLOCK), 1) // KEY_BLOCK
    row = lax.broadcasted_iota(jnp.int32, (128, blocks * KEY_BLOCK), 0)
    expand = ((place + (me % 2) * blocks) == row).astype(jnp.bfloat16)
    start = pl.multiple_of((me // 2) * 128, 128)

    def one(h, carry):
        ids = chosen_ref[h, :, pl.ds(start, 128)]
        cols = [jnp.broadcast_to(ids[c : c + 1, :], (slots, 128)) for c in range(picks)]
        least = jnp.full((slots, 128), BIG, jnp.int32)
        most = jnp.full((slots, 128), -1, jnp.int32)
        for col in cols:
            hit = ((col >> 6) == (slot >> 1)) & ours
            least = jnp.minimum(least, jnp.where(hit, col, BIG))
            most = jnp.maximum(most, jnp.where(hit, col, -1))
        least = jnp.min(least, axis=1, keepdims=True)
        most = jnp.max(most, axis=1, keepdims=True)
        name = jnp.where(
            (slot & 1) == 0, least, jnp.where(most > least, most, -7)
        )
        named = cols[0] == name
        for col in cols[1:]:
            named = named | (col == name)
        hot = jnp.where(named, 1.0, 0.0).astype(jnp.bfloat16)
        full = jnp.dot(hot, expand, preferred_element_type=jnp.float32)
        bias_ref[h] = jnp.where(full > 0.5, 0.0, NEG)
        return carry

    lax.fori_loop(0, heads, one, 0)


def turn_kernel(x_ref, out_ref):
    def some(i, carry):
        cut = pl.ds(pl.multiple_of(i * 512, 512), 512)
        out_ref[:, cut] = x_ref[cut, :].T
        return carry

    lax.fori_loop(0, x_ref.shape[0] // 512, some, 0)


def weight_kernel(me_ref, xt_ref, *rest, extra, slot, halves):
    shards = rest[:4]
    outs = rest[4 + extra : -4]
    g_s, o_s, in_sem, out_sem = rest[-4:]
    copies = []
    for n, shard in enumerate(shards):
        lanes = pl.ds((n % 2) * HEAD_DIM, HEAD_DIM)
        copy = pltpu.make_async_copy(shard, g_s.at[n // 2, :, lanes], in_sem.at[n])
        copy.start()
        copies.append(copy)
    rows = xt_ref.shape[0]
    shape = (WEIGH_ROWS // KEY_BLOCK, KEY_BLOCK, HEAD_DIM)
    ends = []
    for pair in range(2):
        copies[2 * pair].wait()
        copies[2 * pair + 1].wait()
        g = g_s[pair]

        def some(b, carry, pair=pair, g=g):
            first = pl.multiple_of(b * WEIGH_ROWS, WEIGH_ROWS)
            xt = xt_ref[pl.ds(first, WEIGH_ROWS), :]
            got = jnp.dot(xt, g, preferred_element_type=jnp.float32).astype(jnp.bfloat16)
            owners = pl.ds(b * shape[0], shape[0])
            o_s[pair, owners, 0] = got[:, :HEAD_DIM].reshape(shape)
            o_s[pair, owners, 1] = got[:, HEAD_DIM:].reshape(shape)
            return carry

        lax.fori_loop(0, rows // WEIGH_ROWS, some, 0, unroll=halves)
        if halves:
            core = me_ref[0] % 2
            for out, mine in ((outs[0], core == pair), (outs[1], core != pair)):
                copy = pltpu.make_async_copy(o_s.at[pair], out, out_sem.at[pair])
                pl.when(mine)(copy.start)
                ends.append((copy, mine))
        else:
            target = outs[0].at[:, slot, pl.ds(2 * pair, 2)]
            copy = pltpu.make_async_copy(o_s.at[pair], target, out_sem.at[pair])
            copy.start()
            ends.append((copy, None))
    for copy, mine in ends:
        if mine is None:
            copy.wait()
        else:
            pl.when(mine)(copy.wait)


def join_kernel(keep_ref, got_ref, *rest, at):
    out_ref, keep_s, got_s, sem = rest[-4:]
    one = pltpu.make_async_copy(keep_ref, keep_s, sem.at[0])
    two = pltpu.make_async_copy(got_ref, got_s, sem.at[1])
    one.start()
    two.start()
    one.wait()
    two.wait()
    both = keep_s[...].astype(jnp.float32) + got_s[...].astype(jnp.float32)
    got_s[...] = both.astype(jnp.bfloat16)
    count = keep_ref.shape[1]
    back = pltpu.make_async_copy(got_s, out_ref.at[:, pl.ds(at * count, count)], sem.at[2])
    back.start()
    back.wait()


def put_sum(out_ref, got_ref, sources, column, first):
    acc = got_ref[sources[0], column].astype(jnp.float32)
    for i in sources[1:]:
        acc = acc + got_ref[i, column].astype(jnp.float32)
    out_ref[:, pl.ds(pl.multiple_of(first, HEAD_DIM), HEAD_DIM)] = acc


def total_kernel(at_ref, got_ref, out_ref, *, head, heads, order):
    tp = len(order)
    out_ref[...] = jnp.zeros_like(out_ref)
    for p in range(tp):
        place = (at_ref[0] + order[p]) % tp
        sources = range(got_ref.shape[0])
        put_sum(out_ref, got_ref, sources, p, (place * heads + head) * HEAD_DIM)


def pair_total_kernel(at_ref, got_ref, before_ref, out_ref, got_s, sum_s, got_sem, sem,
                      *, at, head, heads, order):
    tp = len(order)
    got = pltpu.make_async_copy(got_ref.at[:, pl.ds(at * tp // 2, tp // 2)], got_s, got_sem)
    got.start()
    got.wait()
    copies = []
    for p in range(tp):
        place = (at_ref[0] + order[p]) % tp
        acc = got_s[p // 2, p % 2].astype(jnp.float32)
        for i in range(p // 2 + 2, got_s.shape[0], 2):
            acc = acc + got_s[i, p % 2].astype(jnp.float32)
        sum_s[p] = acc
        first = pl.multiple_of((place * heads + head) * HEAD_DIM, HEAD_DIM)
        copy = pltpu.make_async_copy(
            sum_s.at[p], out_ref.at[:, pl.ds(first, HEAD_DIM)], sem.at[p]
        )
        copy.start()
        copies.append(copy)
    for copy in copies:
        copy.wait()


def attend_kernel(me_ref, *refs, head, extra, merge, tiles, far):
    q_ref, g_ref, ko_ref, vo_ref, lse_ref, bias_ref, kv_ref = refs[:7]
    ahead_ref = refs[7] if merge else None
    rest = refs[7 + merge + extra :]
    gqf_ref, gq_ref, dko_ref, dvo_ref, back_ref = rest[:5]
    p_s, dp_s, po_s, dpo_s, dots_s, dk_s, dv_s, kt_s, qq_s, kk_s = rest[5:]
    step = pl.program_id(0)
    scale = HEAD_DIM**-0.5
    nkb = far // KB
    per = KB // (CAP * KEY_BLOCK)
    parts = TQ // 128
    nt = (((1,), (1,)), ((), ()))

    def cut(t):
        return slice(t * 128, (t + 1) * 128)

    def ahead(first, behind):
        q = q_ref[...]
        g = g_ref[...]
        lse = lse_ref[head : head + 1, :] * LOG2E
        key_at = lax.broadcasted_iota(jnp.int32, (128, 128), 0)
        row_at = lax.broadcasted_iota(jnp.int32, (128, 128), 1)
        near = (key_at // KEY_BLOCK == row_at // KEY_BLOCK) & (key_at <= row_at)
        dots = jnp.zeros((8, TQ), jnp.float32)
        own_dots = []
        for i in range(nkb):
            rows = slice(i * KB, (i + 1) * KB)
            if behind is not None:
                behind(i)
            keys = kv_ref[i * per : (i + 1) * per, 0:CAP].reshape(KB, HEAD_DIM)
            values = kv_ref[i * per : (i + 1) * per, CAP : 2 * CAP].reshape(KB, HEAD_DIM)
            s = lax.dot_general(keys, q, nt, preferred_element_type=jnp.float32)
            dp = lax.dot_general(values, g, nt, preferred_element_type=jnp.float32)
            shift = bias_ref[i * per * CAP : (i + 1) * per * CAP, :] - lse
            s = (s * (scale * LOG2E)).reshape(per * CAP, KEY_BLOCK, TQ) + shift[:, None, :]
            p = jnp.exp2(s).reshape(KB, TQ)
            p_s[rows, :] = p
            dp_s[rows, :] = dp
            dv = jnp.dot(p.astype(jnp.bfloat16), g, preferred_element_type=jnp.float32)
            dv_s[rows, :] = dv if first else dv_s[rows, :] + dv
            dots = dots + (p * dp).reshape(KB // 8, 8, TQ).sum(axis=0)
            if i < parts:
                c = cut(i)
                s = lax.dot_general(ko_ref[c, :], q[c], nt, preferred_element_type=jnp.float32)
                dp = lax.dot_general(vo_ref[c, :], g[c], nt, preferred_element_type=jnp.float32)
                p = jnp.exp2(jnp.where(near, s * (scale * LOG2E) - lse[:, c], NEG))
                po_s[c, :] = p
                dpo_s[c, :] = dp
                own_dots.append(jnp.sum(p * dp, axis=0, keepdims=True))
                dvo_ref[c, :] = jnp.dot(
                    p.astype(jnp.bfloat16), g[c], preferred_element_type=jnp.float32
                )
        return jnp.sum(dots, axis=0, keepdims=True) + jnp.concatenate(own_dots, axis=1)

    def second_half(first):
        q = qq_s[...]
        dots = dots_s[...]
        held = []
        own = []

        def behind(i):
            rows = slice(i * KB, (i + 1) * KB)
            ds = (p_s[rows, :] * (dp_s[rows, :] - dots)).astype(jnp.bfloat16)
            dk = jnp.dot(ds, q, preferred_element_type=jnp.float32)
            dk_s[rows, :] = dk if first else dk_s[rows, :] + dk
            part = jnp.dot(kt_s[:, rows], ds, preferred_element_type=jnp.float32)
            held[:] = [held[0] + part] if held else [part]
            if i < parts:
                c = cut(i)
                ds = (po_s[c, :] * (dpo_s[c, :] - dots[:, c])).astype(jnp.bfloat16)
                dko_ref[c, :] = scale * jnp.dot(ds, q[c], preferred_element_type=jnp.float32)
                own.append(jnp.dot(kk_s[c, :].T, ds, preferred_element_type=jnp.float32))

        def finish():
            for t in range(parts):
                out = (scale * (held[0][:, cut(t)] + own[t])).T.astype(jnp.bfloat16)
                gq_ref[cut(t), :] = out
                gqf_ref[cut(t), :] = out

        return behind, finish

    def keep(dots):
        dots_s[...] = dots
        qq_s[...] = q_ref[...]
        kk_s[...] = ko_ref[...]

    @pl.when(step == 0)
    def _():
        for i in range(nkb):
            keys = kv_ref[i * per : (i + 1) * per, 0:CAP].reshape(KB, HEAD_DIM)
            kt_s[:, i * KB : (i + 1) * KB] = keys.T
        keep(ahead(True, None))
        dk_s[...] = jnp.zeros_like(dk_s)

    @pl.when((step > 0) & (step < tiles))
    def _():
        behind, finish = second_half(False)
        dots = ahead(False, behind)
        finish()
        keep(dots)

    @pl.when(step == tiles)
    def _():
        behind, finish = second_half(False)
        for i in range(nkb):
            behind(i)
        finish()
        shape = (far // (CAP * KEY_BLOCK), CAP, KEY_BLOCK, HEAD_DIM)
        dk = (scale * dk_s[...]).astype(jnp.bfloat16).reshape(shape)
        dv = dv_s[...].astype(jnp.bfloat16).reshape(shape)
        if merge:
            me = me_ref[0]
            for n in range(shape[0]):
                back_ref[n, 0:CAP] = jnp.where(n < me, dk[n], ahead_ref[n, 0:CAP])
                back_ref[n, CAP : 2 * CAP] = jnp.where(
                    n < me, dv[n], ahead_ref[n, CAP : 2 * CAP]
                )
        else:
            back_ref[:, 0:CAP] = dk
            back_ref[:, CAP : 2 * CAP] = dv


def land_kernel(me_ref, tab_ref, back_ref, dko_ref, dvo_ref, *rest, head, spans):
    gk_ref, gv_ref = rest[-2:]
    gk_ref[...] = dko_ref[...]
    gv_ref[...] = dvo_ref[...]
    me = me_ref[0]
    half = spans // 2

    def one(n, carry):
        at = head * half + n // 2
        odd = n % 2
        for c in range(CAP):
            named = tab_ref[4 + 2 * c + odd, at] > 0
            first = tab_ref[2 * c + odd, at] * KEY_BLOCK
            rows = pl.ds(pl.multiple_of(first, KEY_BLOCK), KEY_BLOCK)
            gk_ref[rows, :] += jnp.where(named, back_ref[n, c].astype(jnp.float32), 0.0)
            gv_ref[rows, :] += jnp.where(named, back_ref[n, CAP + c].astype(jnp.float32), 0.0)

        return carry

    lax.fori_loop(me + 1, spans, one, 0)


SMEM = pl.BlockSpec(memory_space=pltpu.SMEM)
VMEM = pl.BlockSpec(memory_space=pltpu.VMEM)
ANY = pl.BlockSpec(memory_space=pl.ANY)


def params(**more):
    return pltpu.CompilerParams(vmem_limit_bytes=VMEM_LIMIT, **more)


def cost(flops, data=1 << 20):
    return pl.CostEstimate(flops=flops, transcendentals=0, bytes_accessed=data)


def five(spans, slots=1):
    return (spans, slots, 2 * CAP, KEY_BLOCK, HEAD_DIM)


def slotted(spans, slot):
    return pl.BlockSpec(
        (spans, None, 2 * CAP, KEY_BLOCK, HEAD_DIM), lambda i: (0, slot, 0, 0, 0)
    )


def back_spec(spans, shape):
    return slotted(spans, 0) if len(shape) == 5 else tiles_of(spans, 2 * CAP, 0)


def pack_first(me, ids, key_blocks, value_blocks, heads, spans):
    blocks = key_blocks.shape[0]
    column = pl.BlockSpec((blocks, KEY_BLOCK, HEAD_DIM), lambda i: (0, 0, 0))
    return pl.pallas_call(
        functools.partial(first_kernel, heads=heads, spans=spans, blocks=blocks),
        grid=(1,),
        out_shape=[
            jax.ShapeDtypeStruct(five(spans), jnp.bfloat16),
            jax.ShapeDtypeStruct((8, 128), jnp.int32),
        ],
        in_specs=[SMEM, VMEM, column, column],
        out_specs=[slotted(spans, 0), VMEM],
        scratch_shapes=[
            pltpu.VMEM((heads * spans // 2, 128), jnp.int32),
            pltpu.VMEM((heads * spans // 2, 128), jnp.int32),
            pltpu.VMEM((8, 128), jnp.int32),
            pltpu.SMEM((8, 128), jnp.int32),
            pltpu.SemaphoreType.DMA,
        ],
        compiler_params=params(),
        cost_estimate=cost(1 << 26),
        name="first",
    )(me, ids, key_blocks, value_blocks)


def pack_rest(tab, key_blocks, value_blocks, heads, spans):
    return pl.pallas_call(
        functools.partial(pack_kernel, spans=spans),
        grid=(1,),
        out_shape=[jax.ShapeDtypeStruct(five(spans), jnp.bfloat16)] * (heads - 1),
        in_specs=[SMEM, VMEM, VMEM],
        out_specs=[slotted(spans, 0)] * (heads - 1),
        compiler_params=params(),
        cost_estimate=cost(1 << 26),
        name="pack",
    )(tab, key_blocks, value_blocks)


def mask(me, ids, spans, blocks):
    heads, picks, _ = ids.shape
    return pl.pallas_call(
        functools.partial(mask_kernel, heads=heads, spans=spans, blocks=blocks, picks=picks),
        out_shape=jax.ShapeDtypeStruct((heads, spans * CAP, blocks * KEY_BLOCK), jnp.float32),
        in_specs=[SMEM, VMEM],
        out_specs=VMEM,
        compiler_params=params(),
        cost_estimate=cost(1 << 26),
        name="mask",
    )(me, ids)


def turn(x):
    rows, cols = x.shape
    return pl.pallas_call(
        turn_kernel,
        grid=(cols // 256,),
        out_shape=pltpu.VMEM((cols, rows), x.dtype),
        in_specs=[pl.BlockSpec((rows, 256), lambda i: (0, i))],
        out_specs=pl.BlockSpec((256, rows), lambda i: (i, 0)),
        compiler_params=params(),
        cost_estimate=cost(1 << 26),
        name="turn",
    )(x)


def attend(head, me, q, g, k, v, lse, bias, far_kv, gq_full, ahead, back_shape):
    rows, width = q.shape
    heads = lse.shape[0]
    tiles = rows // TQ
    spans = far_kv.shape[0]
    far = spans * CAP * KEY_BLOCK

    def now(i):
        return jnp.minimum(i, tiles - 1)

    def then(i):
        return jnp.maximum(i - 1, 0)

    column = pl.BlockSpec((TQ, HEAD_DIM), lambda i: (now(i), head))
    alone = pl.BlockSpec((TQ, HEAD_DIM), lambda i: (now(i), 0))
    late_column = pl.BlockSpec((TQ, HEAD_DIM), lambda i: (then(i), head))
    late = pl.BlockSpec((TQ, HEAD_DIM), lambda i: (then(i), 0))
    in_specs = [
        SMEM,
        column,
        column,
        column,
        column,
        pl.BlockSpec((heads, TQ), lambda i: (0, now(i))),
        pl.BlockSpec((None, spans * CAP, TQ), lambda i: (head, 0, now(i))),
        slotted(spans, 0),
    ]
    args = [me, q, g, k, v, lse, bias, far_kv]
    merge = ahead is not None
    if merge:
        in_specs.append(slotted(spans, 0))
        args.append(ahead)
    aliases = {}
    if gq_full is not None:
        aliases[len(args)] = 0
        in_specs.append(ANY)
        args.append(gq_full)
    return pl.pallas_call(
        functools.partial(
            attend_kernel, head=head, extra=len(aliases), merge=int(merge), tiles=tiles, far=far
        ),
        grid=(tiles + 1,),
        in_specs=in_specs,
        out_specs=[late_column, late, late, alone, back_spec(spans, back_shape)],
        out_shape=[
            jax.ShapeDtypeStruct((rows, width), jnp.bfloat16),
            jax.ShapeDtypeStruct((rows, HEAD_DIM), jnp.bfloat16),
            jax.ShapeDtypeStruct((rows, HEAD_DIM), jnp.float32),
            jax.ShapeDtypeStruct((rows, HEAD_DIM), jnp.float32),
            jax.ShapeDtypeStruct(back_shape, jnp.bfloat16),
        ],
        scratch_shapes=[
            pltpu.VMEM((far, TQ), jnp.float32),
            pltpu.VMEM((far, TQ), jnp.float32),
            pltpu.VMEM((TQ, 128), jnp.float32),
            pltpu.VMEM((TQ, 128), jnp.float32),
            pltpu.VMEM((1, TQ), jnp.float32),
            pltpu.VMEM((far, HEAD_DIM), jnp.float32),
            pltpu.VMEM((far, HEAD_DIM), jnp.float32),
            pltpu.VMEM((HEAD_DIM, far), jnp.bfloat16),
            pltpu.VMEM((TQ, HEAD_DIM), jnp.bfloat16),
            pltpu.VMEM((TQ, HEAD_DIM), jnp.bfloat16),
        ],
        input_output_aliases=aliases,
        cost_estimate=cost(10 * rows * far * HEAD_DIM, 8 << 20),
        compiler_params=params(dimension_semantics=("arbitrary",)),
    )(*args)


def weigh(me, xt, shards, buffer, spans, slot, slots, halves=False):
    cols, rows = xt.shape
    in_specs = [SMEM, VMEM] + [ANY] * len(shards)
    args = [me, pltpu.with_memory_space_constraint(xt, pltpu.VMEM), *shards]
    aliases = {}
    if buffer is not None:
        aliases[len(args)] = 0
        in_specs.append(ANY)
        args.append(buffer)
    half = (spans, len(shards) // 2, cols // spans, HEAD_DIM)
    if halves:
        out_specs = [ANY, ANY]
        out_shape = [jax.ShapeDtypeStruct(half, jnp.bfloat16)] * 2
    else:
        out_specs = ANY
        out_shape = jax.ShapeDtypeStruct(five(spans, slots), jnp.bfloat16)
    return pl.pallas_call(
        functools.partial(weight_kernel, extra=len(aliases), slot=slot, halves=halves),
        in_specs=in_specs,
        out_specs=out_specs,
        out_shape=out_shape,
        scratch_shapes=[
            pltpu.VMEM((2, rows, 2 * HEAD_DIM), jnp.bfloat16),
            pltpu.VMEM((2,) + half, jnp.bfloat16),
            pltpu.SemaphoreType.DMA((4,)),
            pltpu.SemaphoreType.DMA((2,)),
        ],
        input_output_aliases=aliases,
        compiler_params=params(),
        cost_estimate=cost(2 * cols * rows * len(shards) * HEAD_DIM, 8 << 20),
        name="weigh",
    )(*args)


def tiles_of(spans, count, at):
    return pl.BlockSpec((spans, count, KEY_BLOCK, HEAD_DIM), lambda i: (0, at, 0, 0))


def join(keep, got, buffer, at):
    args, aliases = [keep, got], {}
    out_shape = jax.ShapeDtypeStruct(keep.shape, keep.dtype)
    if buffer is not None:
        aliases = {2: 0}
        args.append(buffer)
        out_shape = jax.ShapeDtypeStruct(buffer.shape, buffer.dtype)
    return pl.pallas_call(
        functools.partial(join_kernel, at=at),
        in_specs=[ANY] * len(args),
        out_specs=ANY,
        out_shape=out_shape,
        scratch_shapes=[
            pltpu.VMEM(keep.shape, keep.dtype),
            pltpu.VMEM(keep.shape, keep.dtype),
            pltpu.SemaphoreType.DMA((3,)),
        ],
        input_output_aliases=aliases,
        compiler_params=params(),
        cost_estimate=cost(1 << 24),
        name="join",
    )(*args)


def total(place, got, slot, head, heads, order):
    return pl.pallas_call(
        functools.partial(total_kernel, head=head, heads=heads, order=order),
        grid=(1,),
        in_specs=[SMEM, slotted(got.shape[0], slot)],
        out_specs=VMEM,
        out_shape=jax.ShapeDtypeStruct(
            (KEY_BLOCK, len(order) * heads * HEAD_DIM), jnp.float32
        ),
        compiler_params=params(),
        cost_estimate=cost(1 << 24),
        name="total",
    )(place, got)


def pair_total(place, got, at, buffer, head, heads, order):
    half = (got.shape[0], len(order) // 2, KEY_BLOCK, HEAD_DIM)
    return pl.pallas_call(
        functools.partial(pair_total_kernel, at=at, head=head, heads=heads, order=order),
        in_specs=[SMEM, ANY, ANY],
        out_specs=ANY,
        out_shape=jax.ShapeDtypeStruct(buffer.shape, buffer.dtype),
        scratch_shapes=[
            pltpu.VMEM(half, got.dtype),
            pltpu.VMEM((len(order), KEY_BLOCK, HEAD_DIM), jnp.float32),
            pltpu.SemaphoreType.DMA,
            pltpu.SemaphoreType.DMA((len(order),)),
        ],
        input_output_aliases={2: 0},
        compiler_params=params(),
        cost_estimate=cost(1 << 24),
        name="pairtotal",
    )(place, got, buffer)


def land(head, me, tab, home, dko, dvo, full, rows, width):
    spans = home.shape[0]
    column = pl.BlockSpec((rows, HEAD_DIM), lambda i: (0, head))
    alone = pl.BlockSpec((rows, HEAD_DIM), lambda i: (0, 0))
    in_specs = [SMEM, SMEM, back_spec(spans, home.shape), alone, alone]
    args = [me, tab, home, dko, dvo]
    aliases = {}
    if full is not None:
        in_specs += [ANY, ANY]
        args += list(full)
        aliases = {5: 0, 6: 1}
    return pl.pallas_call(
        functools.partial(land_kernel, head=head, spans=spans),
        grid=(1,),
        in_specs=in_specs,
        out_specs=[column, column],
        out_shape=[jax.ShapeDtypeStruct((rows, width), jnp.float32)] * 2,
        input_output_aliases=aliases,
        compiler_params=pltpu.CompilerParams(vmem_limit_bytes=32 * 1024 * 1024),
        cost_estimate=cost(1 << 24),
    )(*args)


def exchange(x):
    return lax.all_to_all(x, "kv", split_axis=0, concat_axis=0, tiled=True)


def shift(x, by, tp):
    return lax.ppermute(x, "tp", [(i, (i + by) % tp) for i in range(tp)])


def program(query_rows, key_rows, value_rows, log_sums, cotangent, layer_input, chosen):
    spans = lax.axis_size("kv")
    tp = lax.axis_size("tp")
    heads = log_sums.shape[0]
    rows, width = query_rows.shape
    blocks = rows // KEY_BLOCK
    me = lax.axis_index("kv").astype(jnp.int32).reshape(1)
    place = lax.axis_index("tp").astype(jnp.int32).reshape(1)
    ids = jnp.transpose(chosen, (0, 2, 1))
    key_blocks = key_rows.reshape(blocks, KEY_BLOCK, width)
    value_blocks = value_rows.reshape(blocks, KEY_BLOCK, width)
    order = (0, 1, 3, 2)

    send0, tab = pack_first(me, ids, key_blocks, value_blocks, heads, spans)
    far0 = exchange(send0)
    send1, send2 = pack_rest(tab, key_blocks, value_blocks, heads, spans)
    xt = turn(layer_input)
    bias = mask(me, ids, spans, blocks)

    def attention(h, far, gq_full, ahead, back_shape):
        return attend(
            h, me, query_rows, cotangent, key_rows, value_rows, log_sums, bias, far,
            gq_full, ahead, back_shape,
        )

    def gathered(gq):
        right = shift(gq, -1, tp)
        left = shift(gq, 1, tp)
        across = shift(gq, 2, tp)
        return gq, right, left, across

    def swapped(x):
        return lax.ppermute(x, "kv", [(i, i ^ 1) for i in range(spans)])

    far1 = exchange(send1)
    gq_full, gq, *own0, out = attention(0, far0, None, send2, five(spans))
    shards0 = gathered(gq)
    far2 = exchange(out)
    gq_full, gq, *own1, out = attention(1, far1, gq_full, None, five(spans, 2))
    shards1 = gathered(gq)
    out = weigh(me, xt, shards0, out, spans, 1, 2)
    home1 = exchange(out)
    room = (spans, 2 * CAP + tp // 2, KEY_BLOCK, HEAD_DIM)
    gq_full, gq, *own2, out = attention(2, far2, gq_full, None, room)
    shards2 = gathered(gq)

    def shared(shards, buffer, at):
        keep, give = weigh(me, xt, shards, None, spans, 0, 1, halves=True)
        got = swapped(give)
        return join(keep, got, buffer, at)

    home2 = exchange(shared(shards1, out, 2))
    last = exchange(shared(shards2, None, 0))

    full = None
    for h, (home, own) in enumerate(((far2, own0), (home1, own1), (home2, own2))):
        full = land(h, me, tab, home, *own, full, rows, width)
    grad_weight = total(place, home1, 1, 0, heads, order)
    grad_weight = pair_total(place, home2, 2, grad_weight, 1, heads, order)
    grad_weight = pair_total(place, last, 0, grad_weight, 2, heads, order)
    return gq_full, full[0], full[1], grad_weight


def solution(mesh):
    placed = (
        P("kv", "tp"),
        P("kv", "tp"),
        P("kv", "tp"),
        P("tp", "kv"),
        P("kv", "tp"),
        P("kv", "tp"),
        P("tp", None, None),
    )
    return jax.shard_map(
        program,
        mesh=mesh,
        in_specs=placed,
        out_specs=(P("kv", "tp"), P("kv", "tp"), P("kv", "tp"), P(("tp", "kv"), None)),
        check_vma=False,
    )
```
